32 devices in a mesh: fs: 8 (over z, y), tp: 4 (over x, core).
Axes of the slice: x: 2, y: 2, z: 4, core: 2. Of those that a mesh axis runs over, the one named last changes fastest.
Arguments:
- tokens: bfloat16 [3072, 2048], P('fs'), may hold values from -6 to 6
- norm_gain: float32 [2048], replicated, may hold values from 0.1 to 1.9
- w_gate: bfloat16 [2048, 4096], P('fs', 'tp'), may hold values from -0.125 to 0.125
- w_up: bfloat16 [2048, 4096], P('fs', 'tp'), may hold values from -0.125 to 0.125
- w_down: bfloat16 [4096, 2048], P('tp', 'fs'), may hold values from -0.09375 to 0.09375
- cotangent: bfloat16 [3072, 2048], P('fs'), may hold values from -6 to 6
Outputs:
- grad_tokens: bfloat16 [3072, 2048], P('fs')
- grad_down: float32 [4096, 2048], P('tp', 'fs')
- down_norms: float32 [4096], P('tp')
The draws below stay inside these ranges and needn't reach their ends.
All inputs are finite; a program needn't handle non-finite values.
Results may differ from the reference program's by a relative error of at most 0.018.
Values may be sent and summed in bfloat16 or wider, within the bound.
A program may use at most 64 MiB of HBM per device.

```python
import jax
import jax.numpy as jnp
from jax import lax

D = 2048
FF = 4096
TOKENS = 3072
N_TP = 4


def spiked(drawn, rng, source, target, blocks, factor):
    def block_of(position):
        return (jnp.arange(drawn.shape[position]) // (drawn.shape[position] // blocks)).reshape((-1,) + (1,) * (drawn.ndim - 1 - position))

    first = jax.random.permutation(rng, blocks)[block_of(target)]
    other_side = (block_of(target) + blocks // 2) % blocks
    return jnp.where((block_of(source) == first) | (block_of(source) == other_side), factor * drawn, drawn)


def steps_of(key, extent, cuts, least, largest):
    level = 1.0
    for position, blocks in cuts:
        heights = jax.random.uniform(jax.random.fold_in(jax.random.fold_in(key, 6), position), (blocks,), jnp.float32, least / len(cuts), largest / len(cuts))
        level = level * jnp.repeat(jnp.exp(heights), extent[position] // blocks).reshape((-1,) + (1,) * (len(extent) - 1 - position))
    return level


def noise(stream_key, shape, scale, limit, pieces=(), kind=jnp.bfloat16):
    loudness = steps_of(stream_key, shape, pieces, -0.22, 0.18) if pieces else 1.0
    array = jax.random.normal(stream_key, shape, jnp.float32) * scale * loudness
    return jnp.minimum(jnp.maximum(array, -limit), limit).astype(kind)


def bell_draw_with(own_key, extent, scale, bound, cuts, heavy, held_as=jnp.bfloat16):
    values = scale * jax.random.normal(own_key, extent, jnp.float32)
    if cuts:
        values = values * steps_of(own_key, extent, cuts, -0.22, 0.18)
    return jnp.clip(spiked(values, jax.random.fold_in(own_key, 3), *heavy), -bound, bound).astype(held_as)


def setup_inputs(seed: int = 0) -> dict:
    key_list = jax.random.split(jax.random.key(seed), 7)
    tokens = noise(key_list[0], (TOKENS, D), 1.0, 6.0, ((0, 8),))
    norm_gain = jnp.clip(1.0 + 0.18 * jax.random.normal(key_list[1], (D,), jnp.float32), 0.1, 1.9)
    w_gate = noise(key_list[2], (D, FF), D ** -0.5, 0.125, ((0, 8), (1, 4)))
    w_up = noise(key_list[3], (D, FF), D ** -0.5, 0.125, ((0, 8), (1, 4)))
    w_down = noise(key_list[4], (FF, D), FF ** -0.5, 0.09375, ((0, 4), (1, 8)))
    cotangent = bell_draw_with(key_list[5], (TOKENS, D), 1.0, 6.0, ((0, 8),), (0, 1, 8, 2.0))
    return dict(tokens=tokens, norm_gain=norm_gain, w_gate=w_gate, w_up=w_up, w_down=w_down, cotangent=cotangent)


EPS = 1e-06

def reference(tokens, norm_gain, w_gate, w_up, w_down, cotangent):
    xf = tokens.astype(jnp.float32)
    inv = lax.rsqrt(lax.optimization_barrier(jnp.mean(xf * xf, axis=-1, keepdims=True)) + EPS)
    scaled = xf * inv
    normed = (scaled * norm_gain).astype(jnp.bfloat16)
    gate = jnp.dot(normed, w_gate, preferred_element_type=jnp.float32)
    up = jnp.dot(normed, w_up, preferred_element_type=jnp.float32)
    sig = jax.nn.sigmoid(gate)
    act = gate * sig
    hidden = (act * up).astype(jnp.bfloat16)
    d_hidden = 0.5 * lax.dot_general(cotangent, w_down, (((1,), (1,)), ((), ())), preferred_element_type=jnp.float32)
    grad_down = 0.5 * lax.dot_general(hidden, cotangent, (((0,), (0,)), ((), ())), preferred_element_type=jnp.float32)
    down_norms = lax.optimization_barrier(jnp.sum(grad_down * grad_down, axis=1))
    d_gate = (d_hidden * up * sig * (1.0 + gate * (1.0 - sig))).astype(jnp.bfloat16)
    d_up = (d_hidden * act).astype(jnp.bfloat16)
    width = FF // N_TP

    def block(total, index):
        start = (index * width).astype(jnp.int32)
        gate_part = lax.dynamic_slice_in_dim(d_gate, start, width, 1)
        up_part = lax.dynamic_slice_in_dim(d_up, start, width, 1)
        gate_rows = lax.dynamic_slice_in_dim(w_gate, start, width, 1)
        up_rows = lax.dynamic_slice_in_dim(w_up, start, width, 1)
        part = lax.dot_general(gate_part, gate_rows, (((1,), (1,)), ((), ())), preferred_element_type=jnp.float32)
        part = part + lax.dot_general(up_part, up_rows, (((1,), (1,)), ((), ())), preferred_element_type=jnp.float32)
        rounded = lax.optimization_barrier(part.astype(jnp.bfloat16))
        return (total + rounded.astype(jnp.float32), None)
    start_total = jnp.zeros(tokens.shape, jnp.float32)
    d_normed, unused = lax.scan(block, start_total, jnp.arange(N_TP, dtype=jnp.int32))
    d_scaled = d_normed * norm_gain
    inner = lax.optimization_barrier(jnp.mean(d_scaled * scaled, axis=-1, keepdims=True))
    grad_tokens = (inv * (d_scaled - scaled * inner)).astype(jnp.bfloat16)
    return (grad_tokens, grad_down, down_norms)
```

```python
import functools

import jax
import jax.numpy as jnp
from jax import lax
from jax.experimental import pallas as pl
from jax.experimental.pallas import tpu as pltpu
from jax.sharding import PartitionSpec as P

EPS = 1e-06
BF16 = jnp.bfloat16
F32 = jnp.float32


def place(pieces, count):
    first = pieces[0][1]
    held = jnp.zeros((count,) + first.shape, first.dtype)
    for position, piece in pieces:
        held = lax.dynamic_update_slice_in_dim(held, piece[None], position, 0)
    return held


def take(array, position, axis=0):
    return lax.dynamic_index_in_dim(array, position, axis, keepdims=False)


def gather_kernel(n_z, n_y, n_x, own_gu, own_dn, other_gu, other_dn, mine, w_gu, w_dn, got,
                  z_send, z_recv, y_send, y_recv, x_send, x_recv, c_send, c_recv, local):
    f, t = lax.axis_index("fs"), lax.axis_index("tp")
    z, y, x, c = lax.div(f, n_y), lax.rem(f, n_y), lax.div(t, 2), lax.rem(t, 2)
    n_tp = 2 * n_x
    sources = ((own_gu, other_gu), (own_dn, other_dn))
    held = (w_gu, w_dn)

    def at_z(s):
        return {"fs": lax.rem(z + s, n_z) * n_y + y}

    def at_y(r):
        return {"fs": z * n_y + lax.rem(y + r, n_y)}

    def at_x(s):
        return {"tp": lax.rem(t + 2 * s, n_tp)}

    twin = {"fs": (z + 1 - 2 * lax.rem(z, 2)) * n_y + y}
    core = {"tp": t + 1 - 2 * c}

    barrier = pltpu.get_barrier_semaphore()
    friends = [at_z(s) for s in range(1, n_z)] + [at_y(r) for r in range(1, n_y)]
    friends += [at_x(s) for s in range(1, n_x)] + [core]
    for friend in friends:
        pl.semaphore_signal(barrier, inc=1, device_id=friend, device_id_type=pl.DeviceIdType.MESH)
    pl.semaphore_wait(barrier, len(friends))

    started = []

    def send(src, dst, out_sem, in_sem, to):
        copy = pltpu.make_async_remote_copy(
            src_ref=src, dst_ref=dst, send_sem=out_sem, recv_sem=in_sem,
            device_id=to, device_id_type=pl.DeviceIdType.MESH,
        )
        copy.start()
        started.append(copy)
        return copy

    order = sorted(range(1, n_z), key=lambda s: min(s, n_z - s))
    from_z = {}

    def start_z(k):
        for s in order:
            from_z[k, s] = send(
                sources[k][s % 2], held[k].at[f], z_send.at[k, s], z_recv.at[k, s], at_z(s)
            )

    late = []

    def forward(k, s):
        if s == 0:
            src = sources[k][0]
            slot = f
        else:
            from_z[k, s].wait_recv()
            slot = lax.rem(z + n_z - s, n_z) * n_y + y
            src = held[k].at[slot]
        for r in range(1, n_y):
            late.append(send(
                src, held[k].at[slot], y_send.at[k, s, r], y_recv.at[k, s, r], at_y(r)
            ))

    start_z(0)
    forward(0, 0)
    tokens = send(mine, got.at[:, x, c], x_send.at[0], x_recv.at[0], twin)
    start_z(1)
    forward(1, 0)
    stays = [pltpu.make_async_copy(sources[k][0], held[k].at[f], local.at[k]) for k in range(2)]
    for copy in stays:
        copy.start()
    for s in order:
        forward(0, s)
    tokens.wait_recv()
    across = [
        send(got.at[:, x, c], got.at[:, x, c], x_send.at[s], x_recv.at[s], at_x(s))
        for s in range(1, n_x)
    ]
    for s in order[:-1]:
        forward(1, s)
    for copy in across:
        copy.wait_recv()
    late.append(send(got.at[:, :, c], got.at[:, :, c], c_send, c_recv, core))
    forward(1, order[-1])
    for copy in late:
        copy.wait_recv()
    for copy in started:
        copy.wait_send()
    for copy in stays:
        copy.wait()


def gather_all(n_z, n_y, n_x, own, other, mine):
    n_fs = n_z * n_y
    dma = pltpu.SemaphoreType.DMA
    anywhere = pl.BlockSpec(memory_space=pl.ANY)
    return pl.pallas_call(
        functools.partial(gather_kernel, n_z, n_y, n_x),
        out_shape=[jax.ShapeDtypeStruct((n_fs,) + a.shape, a.dtype) for a in own]
        + [jax.ShapeDtypeStruct((2, n_x, 2) + mine.shape[1:], mine.dtype)],
        in_specs=[anywhere] * 5,
        out_specs=[anywhere] * 3,
        scratch_shapes=[
            dma((2, n_z)), dma((2, n_z)), dma((2, n_z, n_y)), dma((2, n_z, n_y)),
            dma((n_x,)), dma((n_x,)), dma, dma, dma((2,)),
        ],
        compiler_params=pltpu.CompilerParams(collective_id=0, has_side_effects=True),
    )(*own, *other, mine)


def tile_of(extent, most):
    return max(n for n in range(16, most + 1, 16) if extent % n == 0)


def dot(a, b, contract):
    return lax.dot_general(a, b, (contract, ((), ())), preferred_element_type=F32)


def rows_at(start, count):
    return pl.ds(pl.multiple_of(start, 16), count)


def cols_at(start, count):
    return pl.ds(pl.multiple_of(start, 128), count)


def fused_kernel(n_z, n_y, n_x, tokens, cotangent, gain, w_gate, w_up, w_down,
                 o_grad, o_down, o_norms,
                 tok, cot, normed, wg, wu, wd, gate, up, d_hid, hid_t, d_gate, d_up,
                 own_share, y_out, y_in, q_out, q_in, t_out, t_in, kept, n_own, n_over_y, n_over_z,
                 part, c_out, c_in, m_out, m_in, x_all, grad,
                 z_send, z_recv, f_send, f_recv, tt_send, tt_recv, tx_send, tx_recv, tc_send, tc_recv,
                 y_send, y_recv, q_send, q_recv, t_send, t_recv, ny_send, ny_recv, nz_send, nz_recv,
                 c_send, c_recv, m_send, m_recv, x_send, x_recv, g_send, g_recv, local):
    f, t = lax.axis_index("fs"), lax.axis_index("tp")
    z, y, x, c = lax.div(f, n_y), lax.rem(f, n_y), lax.div(t, 2), lax.rem(t, 2)
    q, h = lax.div(z, 2), lax.rem(z, 2)
    n_tp, n_q = 2 * n_x, n_z // 2
    rows, d_model = tokens.shape
    depth, half = wg.shape[1], wg.shape[2]
    piece = rows // n_tp
    chunks = c_out.shape[1]
    side = rows // 2
    chunk = side // chunks

    def at_z(s):
        return {"fs": lax.rem(z + s, n_z) * n_y + y}

    def at_y(r):
        return {"fs": z * n_y + lax.rem(y + r, n_y)}

    def at_x(s):
        return {"tp": lax.rem(t + 2 * s, n_tp)}

    twin = {"fs": (z + 1 - 2 * h) * n_y + y}
    core = {"tp": t + 1 - 2 * c}

    started, kept_local = [], []

    def send(src, dst, out_sem, in_sem, to):
        copy = pltpu.make_async_remote_copy(
            src_ref=src, dst_ref=dst, send_sem=out_sem, recv_sem=in_sem,
            device_id=to, device_id_type=pl.DeviceIdType.MESH,
        )
        copy.start()
        started.append(copy)
        return copy

    def bring(src, dst, sem):
        copy = pltpu.make_async_copy(src, dst, sem)
        copy.start()
        return copy

    held = (wg, wu, wd)

    def source(k, which):
        if k == 2:
            return w_down.at[rows_at(which * half, half), :]
        return (w_gate, w_up)[k].at[:, cols_at(which * half, half)]

    bring_tok = bring(tokens, tok.at[pl.ds(0, rows)], local.at[0])
    bring_cot = bring(cotangent, cot.at[pl.ds(0, rows)], local.at[1])
    stays = [bring(source(k, h), held[k].at[f], local.at[2 + k]) for k in range(3)]

    barrier = pltpu.get_barrier_semaphore()
    friends = [at_z(s) for s in range(1, n_z)] + [at_y(r) for r in range(1, n_y)]
    friends += [at_x(s) for s in range(1, n_x)] + [core]
    for friend in friends:
        pl.semaphore_signal(barrier, inc=1, device_id=friend, device_id_type=pl.DeviceIdType.MESH)
    pl.semaphore_wait(barrier, len(friends))

    order = sorted(range(1, n_z), key=lambda s: min(s, n_z - s))
    from_z, over_y = {}, {}

    def start_z(k):
        for s in order:
            which = h if s % 2 == 0 else 1 - h
            from_z[k, s] = send(
                source(k, which), held[k].at[f], z_send.at[k, s], z_recv.at[k, s], at_z(s)
            )

    def slot(s, r):
        return lax.rem(z + n_z - s, n_z) * n_y + lax.rem(y + n_y - r, n_y)

    def forward(k, s):
        if s == 0:
            src = source(k, h)
        else:
            from_z[k, s].wait_recv()
            src = held[k].at[slot(s, 0)]
        for r in range(1, n_y):
            over_y[k, s, r] = send(
                src, held[k].at[slot(s, 0)], f_send.at[k, s, r], f_recv.at[k, s, r], at_y(r)
            )

    mine = rows_at(rows + t * piece, piece)
    raw, both = (tokens, cotangent), (tok, cot)
    to_twin = [
        send(raw[a].at[rows_at(t * piece, piece)], both[a].at[mine], tt_send.at[a], tt_recv.at[a], twin)
        for a in range(2)
    ]
    start_z(0)
    start_z(1)
    forward(0, 0)
    forward(1, 0)
    start_z(2)
    forward(2, 0)

    norm_tile = tile_of(rows, 32)

    def normalize(first):
        @pl.loop(0, rows // norm_tile)
        def _(i):
            at = rows_at(first + i * norm_tile, norm_tile)
            xf = tok[at, :].astype(F32)
            inv = lax.rsqrt(jnp.mean(xf * xf, axis=-1, keepdims=True) + EPS)
            normed[at, :] = (xf * inv * gain[...]).astype(BF16)

    bring_tok.wait()
    normalize(0)

    m_tile = tile_of(2 * rows, 256)

    def add_gate_up(s, r):
        if s == 0 and r == 0:
            stays[0].wait()
            stays[1].wait()
        elif r > 0:
            over_y[0, s, r].wait_recv()
            over_y[1, s, r].wait_recv()
        at_slot = slot(s, r)

        @pl.loop(0, 2 * rows // m_tile)
        def _(i):
            at = rows_at(i * m_tile, m_tile)
            a = normed[at, cols_at(at_slot * depth, depth)]
            for total, w in ((gate, wg), (up, wu)):
                term = dot(a, w[at_slot], ((1,), (0,)))
                total[at, :] = term if s == 0 and r == 0 else total[at, :] + term

    def add_d_hidden(s, r):
        if s == 0 and r == 0:
            stays[2].wait()
        elif r > 0:
            over_y[2, s, r].wait_recv()
        at_slot = slot(s, r)

        @pl.loop(0, 2 * rows // m_tile)
        def _(i):
            at = rows_at(i * m_tile, m_tile)
            term = dot(cot[at, cols_at(at_slot * depth, depth)], wd[at_slot], ((1,), (1,)))
            d_hid[at, :] = term if s == 0 and r == 0 else d_hid[at, :] + term

    for copy in to_twin:
        copy.wait_recv()
    across = [
        [send(b.at[mine], b.at[mine], tx_send.at[a, s], tx_recv.at[a, s], at_x(s)) for s in range(1, n_x)]
        for a, b in enumerate(both)
    ]
    forward(0, order[0])
    forward(1, order[0])
    for a, b in enumerate(both):
        for copy in across[a]:
            copy.wait_recv()
    met = []
    for a, b in enumerate(both):
        for k in range(n_x):
            at = rows_at(rows + (2 * k + c) * piece, piece)
            met.append(send(b.at[at], b.at[at], tc_send.at[a, k], tc_recv.at[a, k], core))
    for s in order[1:-1]:
        forward(0, s)
        forward(1, s)
    bring_cot.wait()
    for copy in met:
        copy.wait_recv()
    normalize(rows)
    for r in range(n_y):
        add_gate_up(0, r)
    for s in order[:-1]:
        add_gate_up(s, 0)
    forward(0, order[-1])
    forward(1, order[-1])
    for s in order[:-1]:
        for r in range(1, n_y):
            add_gate_up(s, r)
    add_gate_up(order[-1], 0)
    forward(2, order[0])
    for r in range(1, n_y):
        add_gate_up(order[-1], r)

    e_tile = tile_of(2 * rows, 128)

    @pl.loop(0, 2 * rows // e_tile)
    def _(i):
        at = rows_at(i * e_tile, e_tile)
        g, u = gate[at, :], up[at, :]
        sig = jax.nn.sigmoid(g)
        act = g * sig
        hid_t[:, cols_at(i * e_tile, e_tile)] = (act * u).T.astype(BF16)
        gate[at, :] = 0.5 * (u * sig * (1.0 + g * (1.0 - sig)))
        up[at, :] = 0.5 * act

    s_tile = tile_of(half, 128)

    def share(block, put):
        @pl.loop(0, half // s_tile)
        def _(i):
            at = rows_at(i * s_tile, s_tile)
            put(at, 0.5 * dot(hid_t[at, :], cot[:, cols_at(block * depth, depth)], ((1,), (0,))))

    def block_of(step, rel, r):
        column = 2 * lax.rem(q + step, n_q) + (h if rel == 0 else 1 - h)
        return column * n_y + lax.rem(y + r, n_y)

    y_copies = {}

    def send_share(step, rel):
        for r in range(1, n_y):
            out = y_out.at[step, rel, r]

            def put(at, value):
                out[at, :] = value.astype(BF16)

            share(block_of(step, rel, r), put)
            y_copies[step, rel, r] = send(
                out, y_in.at[step, rel, r], y_send.at[step, rel, r], y_recv.at[step, rel, r], at_y(r)
            )

    def own_block(step, rel):
        out = own_share.at[step, rel]

        def put(at, value):
            out[at, :] = value

        share(block_of(step, rel, 0), put)

    q_copies = {}

    def cross(step, rel):
        for r in range(1, n_y):
            y_copies[step, rel, r].wait_recv()

        @pl.loop(0, half // s_tile)
        def _(i):
            at = rows_at(i * s_tile, s_tile)
            total = own_share[step, rel, at, :]
            for r in range(1, n_y):
                total = total + y_in[step, rel, r, at, :].astype(F32)
            q_out[step, rel, at, :] = total.astype(BF16)

        q_copies[step, rel] = send(
            q_out.at[step, rel], q_in.at[step, rel], q_send.at[step, rel], q_recv.at[step, rel],
            at_z(2 * step),
        )

    for step in range(1, n_q):
        for rel in (1, 0):
            send_share(step, rel)
    for step in range(1, n_q):
        for rel in (1, 0):
            own_block(step, rel)
    for s in order[1:-1]:
        forward(2, s)
    add_d_hidden(0, 0)
    for r in range(1, n_y):
        add_d_hidden(0, r)
    for s in order[:-1]:
        add_d_hidden(s, 0)
    for step in range(1, n_q):
        for rel in (1, 0):
            cross(step, rel)
    for s in order[:-1]:
        for r in range(1, n_y):
            add_d_hidden(s, r)
    forward(2, order[-1])
    for rel in (1, 0):
        send_share(0, rel)
    for rel in (1, 0):
        own_block(0, rel)
    add_d_hidden(order[-1], 0)
    for r in range(1, n_y):
        add_d_hidden(order[-1], r)

    @pl.loop(0, 2 * rows // e_tile)
    def _(i):
        at = rows_at(i * e_tile, e_tile)
        d = d_hid[at, :]
        d_gate[at, :] = (d * gate[at, :]).astype(BF16)
        d_up[at, :] = (d * up[at, :]).astype(BF16)

    def partial(group, core_side, put):
        first = group * rows + core_side * side

        @pl.loop(0, n_z * n_y)
        def _(k):
            at = rows_at(first, side)
            put(cols_at(k * depth, depth),
                dot(d_gate[at, :], wg[k], ((1,), (1,))) + dot(d_up[at, :], wu[k], ((1,), (1,))))

    c_copies = {}

    def to_core(group):
        def put(at, value):
            for j in range(chunks):
                c_out[group, j, :, at] = value[j * chunk:(j + 1) * chunk].astype(BF16)

        partial(group, 1 - c, put)
        for j in range(chunks):
            c_copies[group, j] = send(
                c_out.at[group, j], c_in.at[group, j], c_send.at[group, j], c_recv.at[group, j], core
            )

    def keep(group):
        def put(at, value):
            for j in range(chunks):
                part[group, j, :, at] = value[j * chunk:(j + 1) * chunk]

        partial(group, c, put)

    l_tile = tile_of(chunk, 32)

    def each(body):
        @pl.loop(0, chunk // l_tile)
        def _(i):
            body(rows_at(i * l_tile, l_tile))

    to_core(1)
    keep(1)
    m_copies = []
    for j in range(chunks):
        c_copies[1, j].wait_recv()

        def fold(at):
            m_out[j, at, :] = (part[1, j, at, :] + c_in[1, j, at, :].astype(F32)).astype(BF16)

        each(fold)
        m_copies.append(send(m_out.at[j], m_in.at[j], m_send.at[j], m_recv.at[j], twin))
    to_core(0)
    keep(0)
    x_copies = {}
    for j in range(chunks):
        c_copies[0, j].wait_recv()
        m_copies[j].wait_recv()

        def fold(at):
            x_all[j, x, at, :] = (
                part[0, j, at, :] + c_in[0, j, at, :].astype(F32) + m_in[j, at, :].astype(F32)
            ).astype(BF16)

        each(fold)
        for s in range(1, n_x):
            x_copies[j, s] = send(
                x_all.at[j, x], x_all.at[j, x], x_send.at[j, s], x_recv.at[j, s], at_x(s)
            )

    def finish(j):
        for s in range(1, n_x):
            x_copies[j, s].wait_recv()
        first = c * side + j * chunk

        @pl.loop(0, chunk // l_tile)
        def _(i):
            at = rows_at(i * l_tile, l_tile)
            to = rows_at(first + i * l_tile, l_tile)
            xf = tok[to, :].astype(F32)
            inv = lax.rsqrt(jnp.mean(xf * xf, axis=-1, keepdims=True) + EPS)
            scaled = xf * inv
            d_normed = x_all[j, 0, at, :].astype(F32)
            for k in range(1, n_x):
                d_normed = d_normed + x_all[j, k, at, :].astype(F32)
            d_scaled = d_normed * gain[...]
            inner = jnp.mean(d_scaled * scaled, axis=-1, keepdims=True)
            grad[j, at, :] = (inv * (d_scaled - scaled * inner)).astype(BF16)

        place_at = o_grad.at[rows_at(first, chunk)]
        kept_local.append(bring(grad.at[j], place_at, local.at[5 + j]))
        return send(grad.at[j], place_at, g_send.at[j], g_recv.at[j], core)

    shared = [finish(j) for j in range(chunks - 1)]

    def collect(rel, put):
        for r in range(1, n_y):
            y_copies[0, rel, r].wait_recv()
        for step in range(1, n_q):
            q_copies[step, rel].wait_recv()

        @pl.loop(0, half // s_tile)
        def _(i):
            at = rows_at(i * s_tile, s_tile)
            total = own_share[0, rel, at, :]
            for r in range(1, n_y):
                total = total + y_in[0, rel, r, at, :].astype(F32)
            for step in range(1, n_q):
                total = total + q_in[step, rel, at, :].astype(F32)
            put(i * s_tile, at, total)

    def put_twin(start, at, value):
        t_out[at, :] = value.astype(BF16)

    def put_kept(start, at, value):
        kept[rows_at(h * half + start, s_tile), :] = value

    collect(1, put_twin)
    swapped = send(t_out, t_in, t_send, t_recv, twin)
    collect(0, put_kept)
    shared.append(finish(chunks - 1))
    swapped.wait_recv()

    @pl.loop(0, half // s_tile)
    def _(i):
        at = rows_at(i * s_tile, s_tile)
        kept[rows_at((1 - h) * half + i * s_tile, s_tile), :] = t_in[at, :].astype(F32)

    kept_local.append(bring(kept, o_down, local.at[5 + chunks]))

    for i in range(2 * half // s_tile):
        g = kept[i * s_tile:(i + 1) * s_tile, :]
        squares = g * g
        folded = squares[:, :128]
        for k in range(1, depth // 128):
            folded = folded + squares[:, k * 128:(k + 1) * 128]
        n_over_y[y, :, i * s_tile:(i + 1) * s_tile] = jnp.sum(folded.T, axis=0, keepdims=True)
    exchange = [
        send(n_over_y.at[y], n_over_y.at[y], ny_send.at[r], ny_recv.at[r], at_y(r)) for r in range(1, n_y)
    ]
    for copy in exchange:
        copy.wait_recv()
    total = n_over_y[0]
    for k in range(1, n_y):
        total = total + n_over_y[k]
    n_over_z[z] = total
    exchange = [
        send(n_over_z.at[z], n_over_z.at[z], nz_send.at[s], nz_recv.at[s], at_z(s)) for s in range(1, n_z)
    ]
    for copy in exchange:
        copy.wait_recv()
    total = n_over_z[0]
    for k in range(1, n_z):
        total = total + n_over_z[k]
    o_norms[...] = total

    for copy in shared:
        copy.wait_recv()
    for copy in started:
        copy.wait_send()
    for copy in kept_local:
        copy.wait()


def fused(n_z, n_y, n_x, tokens, norm_gain, w_gate, w_up, w_down, cotangent):
    n_fs, n_tp, n_q = n_z * n_y, 2 * n_x, n_z // 2
    rows, d_model = tokens.shape
    depth, half = w_gate.shape[0], w_gate.shape[1] // 2
    chunks = 2
    chunk = rows // 2 // chunks
    dma, vmem = pltpu.SemaphoreType.DMA, pltpu.VMEM
    anywhere = pl.BlockSpec(memory_space=pl.ANY)
    inside = pl.BlockSpec(memory_space=pltpu.VMEM)
    block = (half, depth)
    scratch = [
        vmem((2 * rows, d_model), BF16), vmem((2 * rows, d_model), BF16), vmem((2 * rows, d_model), BF16),
        vmem((n_fs, depth, half), BF16), vmem((n_fs, depth, half), BF16), vmem((n_fs, half, depth), BF16),
        vmem((2 * rows, half), F32), vmem((2 * rows, half), F32), vmem((2 * rows, half), F32),
        vmem((half, 2 * rows), BF16), vmem((2 * rows, half), BF16), vmem((2 * rows, half), BF16),
        vmem((n_q, 2) + block, F32), vmem((n_q, 2, n_y) + block, BF16), vmem((n_q, 2, n_y) + block, BF16),
        vmem((n_q, 2) + block, BF16), vmem((n_q, 2) + block, BF16), vmem(block, BF16), vmem(block, BF16),
        vmem((2 * half, depth), F32), vmem((1, 2 * half), F32),
        vmem((n_y, 1, 2 * half), F32), vmem((n_z, 1, 2 * half), F32),
        vmem((2, chunks, chunk, d_model), F32),
        vmem((2, chunks, chunk, d_model), BF16), vmem((2, chunks, chunk, d_model), BF16),
        vmem((chunks, chunk, d_model), BF16), vmem((chunks, chunk, d_model), BF16),
        vmem((chunks, n_x, chunk, d_model), BF16), vmem((chunks, chunk, d_model), BF16),
        dma((3, n_z)), dma((3, n_z)), dma((3, n_z, n_y)), dma((3, n_z, n_y)),
        dma((2,)), dma((2,)), dma((2, n_x)), dma((2, n_x)), dma((2, n_x)), dma((2, n_x)),
        dma((n_q, 2, n_y)), dma((n_q, 2, n_y)), dma((n_q, 2)), dma((n_q, 2)), dma, dma,
        dma((n_y,)), dma((n_y,)), dma((n_z,)), dma((n_z,)),
        dma((2, chunks)), dma((2, chunks)), dma((chunks,)), dma((chunks,)),
        dma((chunks, n_x)), dma((chunks, n_x)), dma((chunks,)), dma((chunks,)), dma((6 + chunks,)),
    ]
    grad, down, norms = pl.pallas_call(
        functools.partial(fused_kernel, n_z, n_y, n_x),
        out_shape=[
            jax.ShapeDtypeStruct((rows, d_model), BF16),
            jax.ShapeDtypeStruct((2 * half, depth), F32),
            jax.ShapeDtypeStruct((1, 2 * half), F32),
        ],
        in_specs=[anywhere, anywhere, inside, anywhere, anywhere, anywhere],
        out_specs=[anywhere, anywhere, inside],
        scratch_shapes=scratch,
        compiler_params=pltpu.CompilerParams(
            collective_id=1, has_side_effects=True, vmem_limit_bytes=60000 * 1024
        ),
    )(tokens, cotangent, norm_gain.reshape(1, d_model), w_gate, w_up, w_down)
    return grad, down, norms.reshape(2 * half)


def shards(n_fs, n_tp, tokens, norm_gain, w_gate, w_up, w_down, cotangent):
    n_y = 2 ** ((n_fs.bit_length() - 1) // 2)
    n_z, n_x = n_fs // n_y, n_tp // 2
    n_q = n_z // 2
    f, t = lax.axis_index("fs"), lax.axis_index("tp")
    z, y, x, c = f // n_y, f % n_y, t // 2, t % 2
    q, h = z // 2, z % 2
    rows, d_model = tokens.shape
    depth, half = w_gate.shape[0], w_gate.shape[1] // 2
    piece = rows // n_tp

    if piece % 16 == 0 and depth % 128 == 0 and half % 128 == 0:
        return fused(n_z, n_y, n_x, tokens, norm_gain, w_gate, w_up, w_down, cotangent)

    def to_z(a, step):
        return lax.ppermute(a, "fs", [(i, (i + step * n_y) % n_fs) for i in range(n_fs)])

    def to_y(a, step):
        return lax.ppermute(
            a, "fs", [(i, i // n_y * n_y + (i + step) % n_y) for i in range(n_fs)]
        )

    def to_twin(a):
        return lax.ppermute(
            a, "fs", [(i, (i // n_y ^ 1) * n_y + i % n_y) for i in range(n_fs)]
        )

    def to_x(a, step):
        return lax.ppermute(a, "tp", [(i, (i + 2 * step) % n_tp) for i in range(n_tp)])

    def to_core(a):
        return lax.ppermute(a, "tp", [(i, i ^ 1) for i in range(n_tp)])

    mine = jnp.stack(
        [lax.dynamic_slice_in_dim(a, t * piece, piece, 0) for a in (tokens, cotangent)]
    )
    down_t = w_down.T

    def half_of(which):
        gate_up = jnp.concatenate(
            [lax.dynamic_slice_in_dim(w, which * half, half, 1) for w in (w_gate, w_up)], axis=1
        )
        return gate_up, lax.dynamic_slice_in_dim(down_t, which * half, half, 1)

    own, other = half_of(h), half_of(1 - h)

    w_gu, w_dn, got = gather_all(n_z, n_y, n_x, own, other, mine)
    w_gu, w_dn = w_gu.reshape(d_model, 2 * half), w_dn.reshape(d_model, half)
    got = got.reshape(2, rows, d_model)
    tokens2 = jnp.concatenate([tokens, got[0]], axis=0)
    cot2 = jnp.concatenate([cotangent, got[1]], axis=0)

    xf = tokens2.astype(F32)
    inv = lax.rsqrt(jnp.mean(xf * xf, axis=-1, keepdims=True) + EPS)
    normed = (xf * inv * norm_gain).astype(BF16)
    gate_up = jnp.dot(normed, w_gu, preferred_element_type=F32)
    gate, up = gate_up[:, :half], gate_up[:, half:]
    sig = jax.nn.sigmoid(gate)
    act = gate * sig
    hidden = (act * up).astype(BF16)

    share = 0.5 * lax.dot_general(
        cot2, hidden, (((0,), (0,)), ((), ())), preferred_element_type=F32
    )
    share = share.reshape(n_q, 2, n_y, depth, half)
    share, w_dn = lax.optimization_barrier((share, w_dn))

    def sent_over_y(pair):
        block = take(share, pair)
        return [to_y(take(block, (y + s) % n_y, 1).astype(BF16), s) for s in range(1, n_y)]

    def over_y(pair, came):
        return sum([a.astype(F32) for a in came], take(take(share, pair), y, 1))

    first = [sent_over_y((q + s) % n_q) for s in range(1, n_q)]

    d_hidden = 0.5 * jnp.dot(cot2, w_dn, preferred_element_type=F32)
    d_gate = (d_hidden * up * sig * (1.0 + gate * (1.0 - sig))).astype(BF16)
    d_up = (d_hidden * act).astype(BF16)
    d_both = jnp.concatenate([d_gate, d_up], axis=1)
    part = lax.dot_general(
        d_both, w_gu, (((1,), (1,)), ((), ())), preferred_element_type=F32
    )
    part, first = lax.optimization_barrier((part.astype(BF16), first))

    away = [
        to_z(over_y((q + s) % n_q, first[s - 1]).astype(BF16), 2 * s) for s in range(1, n_q)
    ]
    total = over_y(q, sent_over_y(q))
    total = sum([a.astype(F32) for a in away], total)
    kept = take(total, h)
    came = to_twin(take(total, 1 - h).astype(BF16)).astype(F32)
    grad_down = place([(h, kept.T), (1 - h, came.T)], 2).reshape(2 * half, depth)
    norms = jnp.sum(grad_down * grad_down, axis=1)
    norms = sum([to_y(norms, s) for s in range(1, n_y)], norms)
    down_norms = sum([to_z(norms, s) for s in range(1, n_z)], norms)

    part = part.reshape(2, n_x, 2, piece, d_model)
    part = take(part, c, 2).astype(F32) + to_core(take(part, 1 - c, 2)).astype(F32)
    total = take(part, x, 1)
    for s in range(1, n_x):
        total = total + to_x(take(part, (x + s) % n_x, 1).astype(BF16), s).astype(F32)
    d_normed = total[0] + to_twin(total[1].astype(BF16)).astype(F32)

    xp = lax.dynamic_slice_in_dim(tokens, t * piece, piece, 0).astype(F32)
    inv_p = lax.rsqrt(jnp.mean(xp * xp, axis=-1, keepdims=True) + EPS)
    scaled = xp * inv_p
    d_scaled = d_normed * norm_gain
    inner = jnp.mean(d_scaled * scaled, axis=-1, keepdims=True)
    grad = (inv_p * (d_scaled - scaled * inner)).astype(BF16)
    grad = place([(x, grad)] + [((x - s) % n_x, to_x(grad, s)) for s in range(1, n_x)], n_x)
    grad = place([(c, grad), (1 - c, to_core(grad))], 2)
    grad_tokens = grad.transpose(1, 0, 2, 3).reshape(rows, d_model)
    return (grad_tokens, grad_down, down_norms)


def solution(mesh):
    in_specs = (P("fs", None), P(), P("fs", "tp"), P("fs", "tp"), P("tp", "fs"), P("fs", None))
    out_specs = (P("fs", None), P("tp", "fs"), P("tp"))
    return jax.shard_map(
        functools.partial(shards, mesh.shape["fs"], mesh.shape["tp"]),
        mesh=mesh, in_specs=in_specs, out_specs=out_specs, check_vma=False,
    )
```

```python
import functools

import jax
import jax.numpy as jnp
from jax import lax
from jax.experimental import pallas as pl
from jax.experimental.pallas import tpu as pltpu
from jax.sharding import PartitionSpec as P

EPS = 1e-06
BF16 = jnp.bfloat16
F32 = jnp.float32


def place(pieces, count):
    first = pieces[0][1]
    held = jnp.zeros((count,) + first.shape, first.dtype)
    for position, piece in pieces:
        held = lax.dynamic_update_slice_in_dim(held, piece[None], position, 0)
    return held


def take(array, position, axis=0):
    return lax.dynamic_index_in_dim(array, position, axis, keepdims=False)


def gather_kernel(n_z, n_y, n_x, own_gu, own_dn, other_gu, other_dn, mine, w_gu, w_dn, got,
                  z_send, z_recv, y_send, y_recv, x_send, x_recv, c_send, c_recv, local):
    f, t = lax.axis_index("fs"), lax.axis_index("tp")
    z, y, x, c = lax.div(f, n_y), lax.rem(f, n_y), lax.div(t, 2), lax.rem(t, 2)
    n_tp = 2 * n_x
    sources = ((own_gu, other_gu), (own_dn, other_dn))
    held = (w_gu, w_dn)

    def at_z(s):
        return {"fs": lax.rem(z + s, n_z) * n_y + y}

    def at_y(r):
        return {"fs": z * n_y + lax.rem(y + r, n_y)}

    def at_x(s):
        return {"tp": lax.rem(t + 2 * s, n_tp)}

    twin = {"fs": (z + 1 - 2 * lax.rem(z, 2)) * n_y + y}
    core = {"tp": t + 1 - 2 * c}

    barrier = pltpu.get_barrier_semaphore()
    friends = [at_z(s) for s in range(1, n_z)] + [at_y(r) for r in range(1, n_y)]
    friends += [at_x(s) for s in range(1, n_x)] + [core]
    for friend in friends:
        pl.semaphore_signal(barrier, inc=1, device_id=friend, device_id_type=pl.DeviceIdType.MESH)
    pl.semaphore_wait(barrier, len(friends))

    started = []

    def send(src, dst, out_sem, in_sem, to):
        copy = pltpu.make_async_remote_copy(
            src_ref=src, dst_ref=dst, send_sem=out_sem, recv_sem=in_sem,
            device_id=to, device_id_type=pl.DeviceIdType.MESH,
        )
        copy.start()
        started.append(copy)
        return copy

    order = sorted(range(1, n_z), key=lambda s: min(s, n_z - s))
    from_z = {}

    def start_z(k):
        for s in order:
            from_z[k, s] = send(
                sources[k][s % 2], held[k].at[f], z_send.at[k, s], z_recv.at[k, s], at_z(s)
            )

    late = []

    def forward(k, s):
        if s == 0:
            src = sources[k][0]
            slot = f
        else:
            from_z[k, s].wait_recv()
            slot = lax.rem(z + n_z - s, n_z) * n_y + y
            src = held[k].at[slot]
        for r in range(1, n_y):
            late.append(send(
                src, held[k].at[slot], y_send.at[k, s, r], y_recv.at[k, s, r], at_y(r)
            ))

    start_z(0)
    forward(0, 0)
    tokens = send(mine, got.at[:, x, c], x_send.at[0], x_recv.at[0], twin)
    start_z(1)
    forward(1, 0)
    stays = [pltpu.make_async_copy(sources[k][0], held[k].at[f], local.at[k]) for k in range(2)]
    for copy in stays:
        copy.start()
    for s in order:
        forward(0, s)
    tokens.wait_recv()
    across = [
        send(got.at[:, x, c], got.at[:, x, c], x_send.at[s], x_recv.at[s], at_x(s))
        for s in range(1, n_x)
    ]
    for s in order[:-1]:
        forward(1, s)
    for copy in across:
        copy.wait_recv()
    late.append(send(got.at[:, :, c], got.at[:, :, c], c_send, c_recv, core))
    forward(1, order[-1])
    for copy in late:
        copy.wait_recv()
    for copy in started:
        copy.wait_send()
    for copy in stays:
        copy.wait()


def gather_all(n_z, n_y, n_x, own, other, mine):
    n_fs = n_z * n_y
    dma = pltpu.SemaphoreType.DMA
    anywhere = pl.BlockSpec(memory_space=pl.ANY)
    return pl.pallas_call(
        functools.partial(gather_kernel, n_z, n_y, n_x),
        out_shape=[jax.ShapeDtypeStruct((n_fs,) + a.shape, a.dtype) for a in own]
        + [jax.ShapeDtypeStruct((2, n_x, 2) + mine.shape[1:], mine.dtype)],
        in_specs=[anywhere] * 5,
        out_specs=[anywhere] * 3,
        scratch_shapes=[
            dma((2, n_z)), dma((2, n_z)), dma((2, n_z, n_y)), dma((2, n_z, n_y)),
            dma((n_x,)), dma((n_x,)), dma, dma, dma((2,)),
        ],
        compiler_params=pltpu.CompilerParams(collective_id=0, has_side_effects=True),
    )(*own, *other, mine)


def tile_of(extent, most):
    return max(n for n in range(16, most + 1, 16) if extent % n == 0)


def dot(a, b, contract):
    return lax.dot_general(a, b, (contract, ((), ())), preferred_element_type=F32)


def rows_at(start, count):
    return pl.ds(pl.multiple_of(start, 16), count)


def cols_at(start, count):
    return pl.ds(pl.multiple_of(start, 128), count)


def fused_kernel(n_z, n_y, n_x, tokens, cotangent, gain, w_gate, w_up, w_down,
                 o_grad, o_down, o_norms,
                 tok, cot, normed, wg, wu, wd, wg_t, wu_t, gate, up, d_hid, hid_t, d_gate, d_up,
                 own_share, y_out, y_in, q_out, q_in, t_out, t_in, kept, n_all,
                 part, c_out, c_in, m_out, m_in, x_all, grad,
                 z_send, z_recv, f_send, f_recv, tt_send, tt_recv, tx_send, tx_recv, tc_send, tc_recv,
                 y_send, y_recv, q_send, q_recv, t_send, t_recv, n_send, n_recv,
                 c_send, c_recv, m_send, m_recv, x_send, x_recv, g_send, g_recv, local):
    f, t = lax.axis_index("fs"), lax.axis_index("tp")
    z, y, x, c = lax.div(f, n_y), lax.rem(f, n_y), lax.div(t, 2), lax.rem(t, 2)
    q, h = lax.div(z, 2), lax.rem(z, 2)
    n_tp, n_q = 2 * n_x, n_z // 2
    rows, d_model = tokens.shape
    depth, half = wg.shape[1], wg.shape[2]
    piece = rows // n_tp
    chunks = c_out.shape[1]
    side = rows // 2
    chunk = side // chunks

    def at_z(s):
        return {"fs": lax.rem(z + s, n_z) * n_y + y}

    def at_y(r):
        return {"fs": z * n_y + lax.rem(y + r, n_y)}

    def at_x(s):
        return {"tp": lax.rem(t + 2 * s, n_tp)}

    twin = {"fs": (z + 1 - 2 * h) * n_y + y}
    core = {"tp": t + 1 - 2 * c}

    started, kept_local = [], []

    def send(src, dst, out_sem, in_sem, to):
        copy = pltpu.make_async_remote_copy(
            src_ref=src, dst_ref=dst, send_sem=out_sem, recv_sem=in_sem,
            device_id=to, device_id_type=pl.DeviceIdType.MESH,
        )
        copy.start()
        started.append(copy)
        return copy

    def bring(src, dst, sem):
        copy = pltpu.make_async_copy(src, dst, sem)
        copy.start()
        return copy

    held = (wg, wu, wd)

    def source(k, which):
        if k == 2:
            return w_down.at[rows_at(which * half, half), :]
        return (w_gate, w_up)[k].at[:, cols_at(which * half, half)]

    bring_tok = bring(tokens, tok.at[pl.ds(0, rows)], local.at[0])
    bring_cot = bring(cotangent, cot.at[pl.ds(0, rows)], local.at[1])
    stays = [bring(source(k, h), held[k].at[f], local.at[2 + k]) for k in range(3)]

    barrier = pltpu.get_barrier_semaphore()
    n_fs = n_z * n_y
    friends = [{"fs": lax.rem(f + s, n_fs)} for s in range(1, n_fs)]
    friends += [at_x(s) for s in range(1, n_x)] + [core]
    for friend in friends:
        pl.semaphore_signal(barrier, inc=1, device_id=friend, device_id_type=pl.DeviceIdType.MESH)
    pl.semaphore_wait(barrier, len(friends))

    over_y = {}
    others = [[b for b in range(n_z) if b != a] for a in range(n_z)]
    ends = (0, n_z - 1)
    nearest = [sorted(others[a], key=lambda b: abs(a - b)) for a in range(n_z)]
    arrival = [
        [a] + sorted(others[a], key=lambda b: 1 if b == a ^ 1 else 2 * (b not in ends)) for a in range(n_z)
    ]

    def pick(table, p):
        return sum(jnp.where(z == a, table[a][p], 0) for a in range(n_z))

    near = [z] + [pick(arrival, p) for p in range(1, n_z)]

    def start_z(k, p):
        to = pick(nearest, p)
        send(
            source(k, lax.rem(to, 2)), held[k].at[f], z_send.at[k, to], z_recv.at[k, z],
            {"fs": to * n_y + y},
        )

    def slot(p, r):
        return near[p] * n_y + lax.rem(y + n_y - r, n_y)

    def forward(k, p):
        if p == 0:
            src = source(k, h)
        else:
            src = held[k].at[slot(p, 0)]
            pltpu.make_async_remote_copy(
                src_ref=src, dst_ref=src, send_sem=z_send.at[k, near[p]], recv_sem=z_recv.at[k, near[p]],
                device_id={"fs": near[p] * n_y + y}, device_id_type=pl.DeviceIdType.MESH,
            ).wait_recv()
        for r in range(1, n_y):
            over_y[k, p, r] = send(
                src, held[k].at[slot(p, 0)], f_send.at[k, near[p], r], f_recv.at[k, near[p], r], at_y(r)
            )

    mine = rows_at(rows + t * piece, piece)
    raw, both = (tokens, cotangent), (tok, cot)

    def swap(a):
        at = rows_at(t * piece, piece)
        return send(raw[a].at[at], both[a].at[mine], tt_send.at[a], tt_recv.at[a], twin)

    def across(a):
        return [
            send(both[a].at[mine], both[a].at[mine], tx_send.at[a, s], tx_recv.at[a, s], at_x(s))
            for s in range(1, n_x)
        ]

    def meet(a):
        copies = []
        for k in range(n_x):
            at = rows_at(rows + (2 * k + c) * piece, piece)
            copies.append(send(both[a].at[at], both[a].at[at], tc_send.at[a, k], tc_recv.at[a, k], core))
        return copies

    def arrive(copies):
        for copy in copies:
            copy.wait_recv()

    swapped = []
    for p in reversed(range(n_z - 1)):
        start_z(0, p)
        start_z(1, p)
        if p == n_z - 2:
            forward(0, 0)
            forward(1, 0)
            forward(2, 0)
    for a in range(2):
        swapped.append(swap(a))
    for p in range(n_z - 1):
        start_z(2, p)

    norm_tile = tile_of(rows, 32)

    def normalize(first):
        @pl.loop(0, rows // norm_tile)
        def _(i):
            at = rows_at(first + i * norm_tile, norm_tile)
            xf = tok[at, :].astype(F32)
            inv = lax.rsqrt(jnp.mean(xf * xf, axis=-1, keepdims=True) + EPS)
            normed[at, :] = (xf * inv * gain[...]).astype(BF16)

    bring_tok.wait()
    normalize(0)

    m_tile = tile_of(2 * rows, 768)

    def add_gate_up(p, r, group):
        at_slot = slot(p, r)
        if group == 0:
            if p == 0 and r == 0:
                stays[0].wait()
                stays[1].wait()
            elif r > 0:
                over_y[0, p, r].wait_recv()
                over_y[1, p, r].wait_recv()
            wg_t[at_slot] = wg[at_slot].T
            wu_t[at_slot] = wu[at_slot].T
        at = pl.ds(group * rows, rows)
        a = normed[at, cols_at(at_slot * depth, depth)]
        for total, w in ((gate, wg), (up, wu)):
            term = dot(a, w[at_slot], ((1,), (0,)))
            total[at, :] = term if p == 0 and r == 0 else total[at, :] + term

    def add_d_hidden(s, r):
        if s == 0 and r == 0:
            stays[2].wait()
        elif r > 0:
            over_y[2, s, r].wait_recv()
        at_slot = slot(s, r)

        @pl.loop(0, 2 * rows // m_tile)
        def _(i):
            at = rows_at(i * m_tile, m_tile)
            term = dot(cot[at, cols_at(at_slot * depth, depth)], wd[at_slot], ((1,), (1,)))
            d_hid[at, :] = term if s == 0 and r == 0 else d_hid[at, :] + term

    add_gate_up(0, 0, 0)
    for p in range(1, n_z):
        forward(0, p)
        forward(1, p)
        for r in range(1, n_y):
            add_gate_up(p - 1, r, 0)
        add_gate_up(p, 0, 0)
    copies = [None, None]
    for a in range(2):
        arrive(swapped[a:a + 1])
        copies[a] = across(a)
    arrive(copies[0])
    met = meet(0)
    backward = range(n_z - 1, 0, -1)
    for p in backward[:1]:
        forward(2, p)
    arrive(met)
    normalize(rows)
    for p in range(n_z):
        for r in range(n_y):
            if p == n_z - 1 and r > 0:
                add_gate_up(p, r, 0)
            add_gate_up(p, r, 1)

    e_tile = tile_of(2 * rows, 128)

    @pl.loop(0, 2 * rows // e_tile)
    def _(i):
        at = rows_at(i * e_tile, e_tile)
        g, u = gate[at, :], up[at, :]
        sig = jax.nn.sigmoid(g)
        act = g * sig
        hid_t[:, cols_at(i * e_tile, e_tile)] = (act * u).T.astype(BF16)
        gate[at, :] = 0.5 * (u * sig * (1.0 + g * (1.0 - sig)))
        up[at, :] = 0.5 * act

    arrive(copies[1])
    bring_cot.wait()
    met = meet(1)
    for p in backward[1:2]:
        forward(2, p)
    arrive(met)
    s_tile = tile_of(half, 512)

    def share(block, put):
        @pl.loop(0, half // s_tile)
        def _(i):
            at = rows_at(i * s_tile, s_tile)
            put(at, 0.5 * dot(hid_t[at, :], cot[:, cols_at(block * depth, depth)], ((1,), (0,))))

    def block_of(step, rel, r):
        column = 2 * lax.rem(q + step, n_q) + (h if rel == 0 else 1 - h)
        return column * n_y + lax.rem(y + r, n_y)

    y_copies = {}

    def send_share(step, rel):
        for r in range(1, n_y):
            out = y_out.at[step, rel, r]

            def put(at, value):
                out[at, :] = value.astype(BF16)

            share(block_of(step, rel, r), put)
            y_copies[step, rel, r] = send(
                out, y_in.at[step, rel, r], y_send.at[step, rel, r], y_recv.at[step, rel, r], at_y(r)
            )

    def own_block(step, rel):
        out = own_share.at[step, rel]

        def put(at, value):
            out[at, :] = value

        share(block_of(step, rel, 0), put)

    q_copies = {}

    def cross(step, rel):
        for r in range(1, n_y):
            y_copies[step, rel, r].wait_recv()

        @pl.loop(0, half // s_tile)
        def _(i):
            at = rows_at(i * s_tile, s_tile)
            total = own_share[step, rel, at, :]
            for r in range(1, n_y):
                total = total + y_in[step, rel, r, at, :].astype(F32)
            q_out[step, rel, at, :] = total.astype(BF16)

        q_copies[step, rel] = send(
            q_out.at[step, rel], q_in.at[step, rel], q_send.at[step, rel], q_recv.at[step, rel],
            at_z(2 * step),
        )

    for p in backward[2:]:
        forward(2, p)
    for step in range(1, n_q):
        for rel in (1, 0):
            send_share(step, rel)
    for rel in (1, 0):
        send_share(0, rel)
    for step in range(1, n_q):
        for rel in (1, 0):
            own_block(step, rel)
    add_d_hidden(0, 0)
    for r in range(1, n_y):
        add_d_hidden(0, r)
    for p in backward:
        add_d_hidden(p, 0)
        for r in range(1, n_y):
            add_d_hidden(p, r)

    @pl.loop(0, 2 * rows // e_tile)
    def _(i):
        at = rows_at(i * e_tile, e_tile)
        d = d_hid[at, :]
        d_gate[at, :] = (d * gate[at, :]).astype(BF16)
        d_up[at, :] = (d * up[at, :]).astype(BF16)

    def partial(group, core_side, put):
        first = group * rows + core_side * side

        @pl.loop(0, n_z * n_y)
        def _(k):
            at = rows_at(first, side)
            put(cols_at(k * depth, depth),
                dot(d_gate[at, :], wg_t[k], ((1,), (0,))) + dot(d_up[at, :], wu_t[k], ((1,), (0,))))

    c_copies = {}

    def to_core(group):
        def put(at, value):
            for j in range(chunks):
                c_out[group, j, :, at] = value[j * chunk:(j + 1) * chunk].astype(BF16)

        partial(group, 1 - c, put)
        for j in range(chunks):
            c_copies[group, j] = send(
                c_out.at[group, j], c_in.at[group, j], c_send.at[group, j], c_recv.at[group, j], core
            )

    def keep(group):
        def put(at, value):
            for j in range(chunks):
                part[group, j, :, at] = value[j * chunk:(j + 1) * chunk]

        partial(group, c, put)

    l_tile = tile_of(chunk, 32)

    def each(body):
        @pl.loop(0, chunk // l_tile)
        def _(i):
            body(rows_at(i * l_tile, l_tile))

    to_core(1)
    keep(1)
    for step in range(1, n_q):
        cross(step, 1)
    m_copies = []
    for j in range(chunks):
        c_copies[1, j].wait_recv()

        def fold(at):
            m_out[j, at, :] = (part[1, j, at, :] + c_in[1, j, at, :].astype(F32)).astype(BF16)

        each(fold)
        m_copies.append(send(m_out.at[j], m_in.at[j], m_send.at[j], m_recv.at[j], twin))
    to_core(0)
    for step in range(1, n_q):
        cross(step, 0)
    keep(0)
    for rel in (1, 0):
        own_block(0, rel)
    x_copies = {}
    for j in range(chunks):
        c_copies[0, j].wait_recv()
        m_copies[j].wait_recv()

        def fold(at):
            x_all[j, x, at, :] = (
                part[0, j, at, :] + c_in[0, j, at, :].astype(F32) + m_in[j, at, :].astype(F32)
            ).astype(BF16)

        each(fold)
        for s in range(1, n_x):
            x_copies[j, s] = send(
                x_all.at[j, x], x_all.at[j, x], x_send.at[j, s], x_recv.at[j, s], at_x(s)
            )

    def finish(j):
        for s in range(1, n_x):
            x_copies[j, s].wait_recv()
        first = c * side + j * chunk

        @pl.loop(0, chunk // l_tile)
        def _(i):
            at = rows_at(i * l_tile, l_tile)
            to = rows_at(first + i * l_tile, l_tile)
            xf = tok[to, :].astype(F32)
            inv = lax.rsqrt(jnp.mean(xf * xf, axis=-1, keepdims=True) + EPS)
            scaled = xf * inv
            d_normed = x_all[j, 0, at, :].astype(F32)
            for k in range(1, n_x):
                d_normed = d_normed + x_all[j, k, at, :].astype(F32)
            d_scaled = d_normed * gain[...]
            inner = jnp.mean(d_scaled * scaled, axis=-1, keepdims=True)
            grad[j, at, :] = (inv * (d_scaled - scaled * inner)).astype(BF16)

        place_at = o_grad.at[rows_at(first, chunk)]
        kept_local.append(bring(grad.at[j], place_at, local.at[5 + j]))
        return send(grad.at[j], place_at, g_send.at[j], g_recv.at[j], core)

    shared = [finish(j) for j in range(chunks - 1)]

    def collect(rel, put):
        for r in range(1, n_y):
            y_copies[0, rel, r].wait_recv()
        for step in range(1, n_q):
            q_copies[step, rel].wait_recv()

        @pl.loop(0, half // s_tile)
        def _(i):
            at = rows_at(i * s_tile, s_tile)
            total = own_share[0, rel, at, :]
            for r in range(1, n_y):
                total = total + y_in[0, rel, r, at, :].astype(F32)
            for step in range(1, n_q):
                total = total + q_in[step, rel, at, :].astype(F32)
            put(i * s_tile, at, total)

    def put_twin(start, at, value):
        t_out[at, :] = value.astype(BF16)

    def put_kept(start, at, value):
        kept[rows_at(h * half + start, s_tile), :] = value

    collect(1, put_twin)
    traded = send(t_out, t_in, t_send, t_recv, twin)
    collect(0, put_kept)
    shared.append(finish(chunks - 1))
    traded.wait_recv()

    @pl.loop(0, half // s_tile)
    def _(i):
        at = rows_at(i * s_tile, s_tile)
        kept[rows_at((1 - h) * half + i * s_tile, s_tile), :] = t_in[at, :].astype(F32)

    kept_local.append(bring(kept, o_down, local.at[5 + chunks]))

    for i in range(2 * half // s_tile):
        g = kept[i * s_tile:(i + 1) * s_tile, :]
        squares = g * g
        folded = squares[:, :128]
        for k in range(1, depth // 128):
            folded = folded + squares[:, k * 128:(k + 1) * 128]
        n_all[f, :, i * s_tile:(i + 1) * s_tile] = jnp.sum(folded.T, axis=0, keepdims=True)
    exchange = [
        send(n_all.at[f], n_all.at[f], n_send.at[s], n_recv.at[s], {"fs": lax.rem(f + s, n_fs)})
        for s in range(1, n_fs)
    ]
    for copy in exchange:
        copy.wait_recv()
    total = n_all[0]
    for k in range(1, n_fs):
        total = total + n_all[k]
    o_norms[...] = total

    for copy in shared:
        copy.wait_recv()
    for copy in started:
        copy.wait_send()
    for copy in kept_local:
        copy.wait()


def fused(n_z, n_y, n_x, tokens, norm_gain, w_gate, w_up, w_down, cotangent):
    n_fs, n_tp, n_q = n_z * n_y, 2 * n_x, n_z // 2
    rows, d_model = tokens.shape
    depth, half = w_gate.shape[0], w_gate.shape[1] // 2
    chunks = max(n for n in (1, 2, 4) if rows % (32 * n) == 0)
    chunk = rows // 2 // chunks
    dma, vmem = pltpu.SemaphoreType.DMA, pltpu.VMEM
    anywhere = pl.BlockSpec(memory_space=pl.ANY)
    inside = pl.BlockSpec(memory_space=pltpu.VMEM)
    block = (half, depth)
    scratch = [
        vmem((2 * rows, d_model), BF16), vmem((2 * rows, d_model), BF16), vmem((2 * rows, d_model), BF16),
        vmem((n_fs, depth, half), BF16), vmem((n_fs, depth, half), BF16), vmem((n_fs, half, depth), BF16),
        vmem((n_fs, half, depth), BF16), vmem((n_fs, half, depth), BF16),
        vmem((2 * rows, half), F32), vmem((2 * rows, half), F32), vmem((2 * rows, half), F32),
        vmem((half, 2 * rows), BF16), vmem((2 * rows, half), BF16), vmem((2 * rows, half), BF16),
        vmem((n_q, 2) + block, F32), vmem((n_q, 2, n_y) + block, BF16), vmem((n_q, 2, n_y) + block, BF16),
        vmem((n_q, 2) + block, BF16), vmem((n_q, 2) + block, BF16), vmem(block, BF16), vmem(block, BF16),
        vmem((2 * half, depth), F32), vmem((n_fs, 1, 2 * half), F32),
        vmem((2, chunks, chunk, d_model), F32),
        vmem((2, chunks, chunk, d_model), BF16), vmem((2, chunks, chunk, d_model), BF16),
        vmem((chunks, chunk, d_model), BF16), vmem((chunks, chunk, d_model), BF16),
        vmem((chunks, n_x, chunk, d_model), BF16), vmem((chunks, chunk, d_model), BF16),
        dma((3, n_z)), dma((3, n_z)), dma((3, n_z, n_y)), dma((3, n_z, n_y)),
        dma((2,)), dma((2,)), dma((2, n_x)), dma((2, n_x)), dma((2, n_x)), dma((2, n_x)),
        dma((n_q, 2, n_y)), dma((n_q, 2, n_y)), dma((n_q, 2)), dma((n_q, 2)), dma, dma,
        dma((n_fs,)), dma((n_fs,)),
        dma((2, chunks)), dma((2, chunks)), dma((chunks,)), dma((chunks,)),
        dma((chunks, n_x)), dma((chunks, n_x)), dma((chunks,)), dma((chunks,)), dma((6 + chunks,)),
    ]
    grad, down, norms = pl.pallas_call(
        functools.partial(fused_kernel, n_z, n_y, n_x),
        out_shape=[
            jax.ShapeDtypeStruct((rows, d_model), BF16),
            jax.ShapeDtypeStruct((2 * half, depth), F32),
            jax.ShapeDtypeStruct((1, 2 * half), F32),
        ],
        in_specs=[anywhere, anywhere, inside, anywhere, anywhere, anywhere],
        out_specs=[anywhere, anywhere, inside],
        scratch_shapes=scratch,
        compiler_params=pltpu.CompilerParams(
            collective_id=1, has_side_effects=True, vmem_limit_bytes=60000 * 1024
        ),
    )(tokens, cotangent, norm_gain.reshape(1, d_model), w_gate, w_up, w_down)
    return grad, down, norms.reshape(2 * half)


def shards(n_fs, n_tp, tokens, norm_gain, w_gate, w_up, w_down, cotangent):
    n_y = 2 ** ((n_fs.bit_length() - 1) // 2)
    n_z, n_x = n_fs // n_y, n_tp // 2
    n_q = n_z // 2
    f, t = lax.axis_index("fs"), lax.axis_index("tp")
    z, y, x, c = f // n_y, f % n_y, t // 2, t % 2
    q, h = z // 2, z % 2
    rows, d_model = tokens.shape
    depth, half = w_gate.shape[0], w_gate.shape[1] // 2
    piece = rows // n_tp

    if piece % 16 == 0 and depth % 128 == 0 and half % 128 == 0:
        return fused(n_z, n_y, n_x, tokens, norm_gain, w_gate, w_up, w_down, cotangent)

    def to_z(a, step):
        return lax.ppermute(a, "fs", [(i, (i + step * n_y) % n_fs) for i in range(n_fs)])

    def to_y(a, step):
        return lax.ppermute(
            a, "fs", [(i, i // n_y * n_y + (i + step) % n_y) for i in range(n_fs)]
        )

    def to_twin(a):
        return lax.ppermute(
            a, "fs", [(i, (i // n_y ^ 1) * n_y + i % n_y) for i in range(n_fs)]
        )

    def to_x(a, step):
        return lax.ppermute(a, "tp", [(i, (i + 2 * step) % n_tp) for i in range(n_tp)])

    def to_core(a):
        return lax.ppermute(a, "tp", [(i, i ^ 1) for i in range(n_tp)])

    mine = jnp.stack(
        [lax.dynamic_slice_in_dim(a, t * piece, piece, 0) for a in (tokens, cotangent)]
    )
    down_t = w_down.T

    def half_of(which):
        gate_up = jnp.concatenate(
            [lax.dynamic_slice_in_dim(w, which * half, half, 1) for w in (w_gate, w_up)], axis=1
        )
        return gate_up, lax.dynamic_slice_in_dim(down_t, which * half, half, 1)

    own, other = half_of(h), half_of(1 - h)

    w_gu, w_dn, got = gather_all(n_z, n_y, n_x, own, other, mine)
    w_gu, w_dn = w_gu.reshape(d_model, 2 * half), w_dn.reshape(d_model, half)
    got = got.reshape(2, rows, d_model)
    tokens2 = jnp.concatenate([tokens, got[0]], axis=0)
    cot2 = jnp.concatenate([cotangent, got[1]], axis=0)

    xf = tokens2.astype(F32)
    inv = lax.rsqrt(jnp.mean(xf * xf, axis=-1, keepdims=True) + EPS)
    normed = (xf * inv * norm_gain).astype(BF16)
    gate_up = jnp.dot(normed, w_gu, preferred_element_type=F32)
    gate, up = gate_up[:, :half], gate_up[:, half:]
    sig = jax.nn.sigmoid(gate)
    act = gate * sig
    hidden = (act * up).astype(BF16)

    share = 0.5 * lax.dot_general(
        cot2, hidden, (((0,), (0,)), ((), ())), preferred_element_type=F32
    )
    share = share.reshape(n_q, 2, n_y, depth, half)
    share, w_dn = lax.optimization_barrier((share, w_dn))

    def sent_over_y(pair):
        block = take(share, pair)
        return [to_y(take(block, (y + s) % n_y, 1).astype(BF16), s) for s in range(1, n_y)]

    def over_y(pair, came):
        return sum([a.astype(F32) for a in came], take(take(share, pair), y, 1))

    first = [sent_over_y((q + s) % n_q) for s in range(1, n_q)]

    d_hidden = 0.5 * jnp.dot(cot2, w_dn, preferred_element_type=F32)
    d_gate = (d_hidden * up * sig * (1.0 + gate * (1.0 - sig))).astype(BF16)
    d_up = (d_hidden * act).astype(BF16)
    d_both = jnp.concatenate([d_gate, d_up], axis=1)
    part = lax.dot_general(
        d_both, w_gu, (((1,), (1,)), ((), ())), preferred_element_type=F32
    )
    part, first = lax.optimization_barrier((part.astype(BF16), first))

    away = [
        to_z(over_y((q + s) % n_q, first[s - 1]).astype(BF16), 2 * s) for s in range(1, n_q)
    ]
    total = over_y(q, sent_over_y(q))
    total = sum([a.astype(F32) for a in away], total)
    kept = take(total, h)
    came = to_twin(take(total, 1 - h).astype(BF16)).astype(F32)
    grad_down = place([(h, kept.T), (1 - h, came.T)], 2).reshape(2 * half, depth)
    norms = jnp.sum(grad_down * grad_down, axis=1)
    norms = sum([to_y(norms, s) for s in range(1, n_y)], norms)
    down_norms = sum([to_z(norms, s) for s in range(1, n_z)], norms)

    part = part.reshape(2, n_x, 2, piece, d_model)
    part = take(part, c, 2).astype(F32) + to_core(take(part, 1 - c, 2)).astype(F32)
    total = take(part, x, 1)
    for s in range(1, n_x):
        total = total + to_x(take(part, (x + s) % n_x, 1).astype(BF16), s).astype(F32)
    d_normed = total[0] + to_twin(total[1].astype(BF16)).astype(F32)

    xp = lax.dynamic_slice_in_dim(tokens, t * piece, piece, 0).astype(F32)
    inv_p = lax.rsqrt(jnp.mean(xp * xp, axis=-1, keepdims=True) + EPS)
    scaled = xp * inv_p
    d_scaled = d_normed * norm_gain
    inner = jnp.mean(d_scaled * scaled, axis=-1, keepdims=True)
    grad = (inv_p * (d_scaled - scaled * inner)).astype(BF16)
    grad = place([(x, grad)] + [((x - s) % n_x, to_x(grad, s)) for s in range(1, n_x)], n_x)
    grad = place([(c, grad), (1 - c, to_core(grad))], 2)
    grad_tokens = grad.transpose(1, 0, 2, 3).reshape(rows, d_model)
    return (grad_tokens, grad_down, down_norms)


def solution(mesh):
    in_specs = (P("fs", None), P(), P("fs", "tp"), P("fs", "tp"), P("tp", "fs"), P("fs", None))
    out_specs = (P("fs", None), P("tp", "fs"), P("tp"))
    return jax.shard_map(
        functools.partial(shards, mesh.shape["fs"], mesh.shape["tp"]),
        mesh=mesh, in_specs=in_specs, out_specs=out_specs, check_vma=False,
    )
```

```python
import functools

import jax
import jax.numpy as jnp
from jax import lax
from jax.experimental import pallas as pl
from jax.experimental.pallas import tpu as pltpu
from jax.sharding import PartitionSpec as P

EPS = 1e-06
BF16 = jnp.bfloat16
F32 = jnp.float32


def place(pieces, count):
    first = pieces[0][1]
    held = jnp.zeros((count,) + first.shape, first.dtype)
    for position, piece in pieces:
        held = lax.dynamic_update_slice_in_dim(held, piece[None], position, 0)
    return held


def take(array, position, axis=0):
    return lax.dynamic_index_in_dim(array, position, axis, keepdims=False)


def gather_kernel(n_z, n_y, n_x, own_gu, own_dn, other_gu, other_dn, mine, w_gu, w_dn, got,
                  z_send, z_recv, y_send, y_recv, x_send, x_recv, c_send, c_recv, local):
    f, t = lax.axis_index("fs"), lax.axis_index("tp")
    z, y, x, c = lax.div(f, n_y), lax.rem(f, n_y), lax.div(t, 2), lax.rem(t, 2)
    n_tp = 2 * n_x
    sources = ((own_gu, other_gu), (own_dn, other_dn))
    held = (w_gu, w_dn)

    def at_z(s):
        return {"fs": lax.rem(z + s, n_z) * n_y + y}

    def at_y(r):
        return {"fs": z * n_y + lax.rem(y + r, n_y)}

    def at_x(s):
        return {"tp": lax.rem(t + 2 * s, n_tp)}

    twin = {"fs": (z + 1 - 2 * lax.rem(z, 2)) * n_y + y}
    core = {"tp": t + 1 - 2 * c}

    barrier = pltpu.get_barrier_semaphore()
    friends = [at_z(s) for s in range(1, n_z)] + [at_y(r) for r in range(1, n_y)]
    friends += [at_x(s) for s in range(1, n_x)] + [core]
    for friend in friends:
        pl.semaphore_signal(barrier, inc=1, device_id=friend, device_id_type=pl.DeviceIdType.MESH)
    pl.semaphore_wait(barrier, len(friends))

    started = []

    def send(src, dst, out_sem, in_sem, to):
        copy = pltpu.make_async_remote_copy(
            src_ref=src, dst_ref=dst, send_sem=out_sem, recv_sem=in_sem,
            device_id=to, device_id_type=pl.DeviceIdType.MESH,
        )
        copy.start()
        started.append(copy)
        return copy

    order = sorted(range(1, n_z), key=lambda s: min(s, n_z - s))
    from_z = {}

    def start_z(k):
        for s in order:
            from_z[k, s] = send(
                sources[k][s % 2], held[k].at[f], z_send.at[k, s], z_recv.at[k, s], at_z(s)
            )

    late = []

    def forward(k, s):
        if s == 0:
            src = sources[k][0]
            slot = f
        else:
            from_z[k, s].wait_recv()
            slot = lax.rem(z + n_z - s, n_z) * n_y + y
            src = held[k].at[slot]
        for r in range(1, n_y):
            late.append(send(
                src, held[k].at[slot], y_send.at[k, s, r], y_recv.at[k, s, r], at_y(r)
            ))

    start_z(0)
    forward(0, 0)
    tokens = send(mine, got.at[:, x, c], x_send.at[0], x_recv.at[0], twin)
    start_z(1)
    forward(1, 0)
    stays = [pltpu.make_async_copy(sources[k][0], held[k].at[f], local.at[k]) for k in range(2)]
    for copy in stays:
        copy.start()
    for s in order:
        forward(0, s)
    tokens.wait_recv()
    across = [
        send(got.at[:, x, c], got.at[:, x, c], x_send.at[s], x_recv.at[s], at_x(s))
        for s in range(1, n_x)
    ]
    for s in order[:-1]:
        forward(1, s)
    for copy in across:
        copy.wait_recv()
    late.append(send(got.at[:, :, c], got.at[:, :, c], c_send, c_recv, core))
    forward(1, order[-1])
    for copy in late:
        copy.wait_recv()
    for copy in started:
        copy.wait_send()
    for copy in stays:
        copy.wait()


def gather_all(n_z, n_y, n_x, own, other, mine):
    n_fs = n_z * n_y
    dma = pltpu.SemaphoreType.DMA
    anywhere = pl.BlockSpec(memory_space=pl.ANY)
    return pl.pallas_call(
        functools.partial(gather_kernel, n_z, n_y, n_x),
        out_shape=[jax.ShapeDtypeStruct((n_fs,) + a.shape, a.dtype) for a in own]
        + [jax.ShapeDtypeStruct((2, n_x, 2) + mine.shape[1:], mine.dtype)],
        in_specs=[anywhere] * 5,
        out_specs=[anywhere] * 3,
        scratch_shapes=[
            dma((2, n_z)), dma((2, n_z)), dma((2, n_z, n_y)), dma((2, n_z, n_y)),
            dma((n_x,)), dma((n_x,)), dma, dma, dma((2,)),
        ],
        compiler_params=pltpu.CompilerParams(collective_id=0, has_side_effects=True),
    )(*own, *other, mine)


def tile_of(extent, most):
    return max(n for n in range(16, most + 1, 16) if extent % n == 0)


def dot(a, b, contract):
    return lax.dot_general(a, b, (contract, ((), ())), preferred_element_type=F32)


def rows_at(start, count):
    return pl.ds(pl.multiple_of(start, 16), count)


def cols_at(start, count):
    return pl.ds(pl.multiple_of(start, 128), count)


def fused_kernel(n_z, n_y, n_x, tokens, cotangent, gain_in, w_gate, w_up, w_down,
                 o_grad, o_down, o_norms,
                 gain, tok, cot, normed, wg, wu, wd, wg_t, wu_t, gate, up, d_hid, hid_t, d_gate, d_up,
                 own_share, y_out, y_in, q_out, q_in, t_out, t_in, n_all,
                 part, c_out, c_in, m_out, m_in, x_out, x_in,
                 z_send, z_recv, f_send, f_recv, tt_send, tt_recv, tx_send, tx_recv, tc_send, tc_recv,
                 y_send, y_recv, q_send, q_recv, t_send, t_recv, n_send, n_recv,
                 c_send, c_recv, m_send, m_recv, x_send, x_recv, a_send, a_recv, g_send, g_recv, local):
    f, t = lax.axis_index("fs"), lax.axis_index("tp")
    z, y, x, c = lax.div(f, n_y), lax.rem(f, n_y), lax.div(t, 2), lax.rem(t, 2)
    q, h = lax.div(z, 2), lax.rem(z, 2)
    n_tp, n_q = 2 * n_x, n_z // 2
    rows, d_model = tokens.shape
    depth, half = wg.shape[1], wg.shape[2]
    piece = rows // n_tp
    chunks, subs = c_out.shape[1], m_out.shape[0]
    side = rows // 2
    chunk = side // chunks

    def at_z(s):
        return {"fs": lax.rem(z + s, n_z) * n_y + y}

    def at_y(r):
        return {"fs": z * n_y + lax.rem(y + r, n_y)}

    def at_x(s):
        return {"tp": lax.rem(t + 2 * s, n_tp)}

    twin = {"fs": (z + 1 - 2 * h) * n_y + y}
    core = {"tp": t + 1 - 2 * c}

    started = []

    def send(src, dst, out_sem, in_sem, to):
        copy = pltpu.make_async_remote_copy(
            src_ref=src, dst_ref=dst, send_sem=out_sem, recv_sem=in_sem,
            device_id=to, device_id_type=pl.DeviceIdType.MESH,
        )
        copy.start()
        started.append(copy)
        return copy

    def bring(src, dst, sem):
        copy = pltpu.make_async_copy(src, dst, sem)
        copy.start()
        return copy

    kinds, step_rows = 4, half // 2

    def source(k, which):
        if k >= 2:
            return w_down.at[rows_at(which * half + (k - 2) * step_rows, step_rows), :]
        return (w_gate, w_up)[k].at[:, cols_at(which * half, half)]

    def held(k, at_slot):
        if k >= 2:
            return wd.at[at_slot, pl.ds((k - 2) * step_rows, step_rows)]
        return (wg, wu)[k].at[at_slot]

    bring_gain = bring(gain_in, gain, local.at[6])
    bring_tok = bring(tokens, tok.at[pl.ds(0, rows)], local.at[0])
    bring_cot = bring(cotangent, cot.at[pl.ds(0, rows)], local.at[1])
    stays = [bring(source(k, h), held(k, f), local.at[2 + k]) for k in range(kinds)]

    barrier = pltpu.get_barrier_semaphore()
    n_fs = n_z * n_y
    friends = [{"fs": lax.rem(f + s, n_fs)} for s in range(1, n_fs)]
    friends += [at_x(s) for s in range(1, n_x)] + [core]
    for friend in friends:
        pl.semaphore_signal(barrier, inc=1, device_id=friend, device_id_type=pl.DeviceIdType.MESH)
    pl.semaphore_wait(barrier, len(friends))

    over_y = {}
    others = [[b for b in range(n_z) if b != a] for a in range(n_z)]
    ends = (0, n_z - 1)
    nearest = [sorted(others[a], key=lambda b: abs(a - b)) for a in range(n_z)]
    arrival = [
        [a] + sorted(others[a], key=lambda b: 1 if b == a ^ 1 else 2 * (b not in ends)) for a in range(n_z)
    ]

    def pick(table, p):
        return sum(jnp.where(z == a, table[a][p], 0) for a in range(n_z))

    near = [z] + [pick(arrival, p) for p in range(1, n_z)]

    def start_z(k, p):
        to = pick(nearest, p)
        send(
            source(k, lax.rem(to, 2)), held(k, f), z_send.at[k, to], z_recv.at[k, z],
            {"fs": to * n_y + y},
        )

    def slot(p, r):
        return near[p] * n_y + lax.rem(y + n_y - r, n_y)

    def forwarding(k, p):
        if p == 0:
            src, came = source(k, h), None
        else:
            src = held(k, slot(p, 0))
            came = pltpu.make_async_remote_copy(
                src_ref=src, dst_ref=src, send_sem=z_send.at[k, near[p]], recv_sem=z_recv.at[k, near[p]],
                device_id={"fs": near[p] * n_y + y}, device_id_type=pl.DeviceIdType.MESH,
            )
        for r in range(1, n_y):
            over_y[k, p, r] = pltpu.make_async_remote_copy(
                src_ref=src, dst_ref=held(k, slot(p, 0)), send_sem=f_send.at[k, near[p], r],
                recv_sem=f_recv.at[k, near[p], r], device_id=at_y(r), device_id_type=pl.DeviceIdType.MESH,
            )
            started.append(over_y[k, p, r])

        def go():
            if came is not None:
                came.wait_recv()
            for r in range(1, n_y):
                over_y[k, p, r].start()

        return go

    def forward(k, p):
        forwarding(k, p)()

    mine = rows_at(rows + t * piece, piece)
    raw, both = (tokens, cotangent), (tok, cot)

    def swap(a):
        at = rows_at(t * piece, piece)
        return send(raw[a].at[at], both[a].at[mine], tt_send.at[a], tt_recv.at[a], twin)

    def across(a):
        return [
            send(both[a].at[mine], both[a].at[mine], tx_send.at[a, s], tx_recv.at[a, s], at_x(s))
            for s in range(1, n_x)
        ]

    def meet(a):
        copies = []
        for k in range(n_x):
            at = rows_at(rows + (2 * k + c) * piece, piece)
            copies.append(send(both[a].at[at], both[a].at[at], tc_send.at[a, k], tc_recv.at[a, k], core))
        return copies

    def arrive(copies):
        for copy in copies:
            copy.wait_recv()

    swapped = []
    for p in reversed(range(n_z - 1)):
        start_z(0, p)
        start_z(1, p)
        if p == n_z - 2:
            forward(0, 0)
            forward(1, 0)
            forward(2, 0)
            forward(3, 0)
    for a in range(2):
        swapped.append(swap(a))
    for p in range(n_z - 1):
        start_z(2, p)
        start_z(3, p)

    norm_tile = tile_of(rows, 32)

    def normalize(first):
        @pl.loop(0, rows // norm_tile)
        def _(i):
            at = rows_at(first + i * norm_tile, norm_tile)
            xf = tok[at, :].astype(F32)
            inv = lax.rsqrt(jnp.mean(xf * xf, axis=-1, keepdims=True) + EPS)
            normed[at, :] = (xf * inv * gain[...]).astype(BF16)

    bring_gain.wait()
    bring_tok.wait()
    normalize(0)

    m_tile = tile_of(2 * rows, 768)

    def add_gate_up(p, r, group):
        at_slot = slot(p, r)
        if group == 0:
            if p == 0 and r == 0:
                stays[0].wait()
                stays[1].wait()
            elif r > 0:
                over_y[0, p, r].wait_recv()
                over_y[1, p, r].wait_recv()
            wg_t[at_slot] = wg[at_slot].T
            wu_t[at_slot] = wu[at_slot].T
        at = pl.ds(group * rows, rows)
        a = normed[at, cols_at(at_slot * depth, depth)]
        for total, w in ((gate, wg), (up, wu)):
            term = dot(a, w[at_slot], ((1,), (0,)))
            total[at, :] = term if p == 0 and r == 0 else total[at, :] + term

    def add_d_hidden(s, r):
        if s == 0 and r == 0:
            stays[2].wait()
            stays[3].wait()
        elif r > 0:
            over_y[2, s, r].wait_recv()
            over_y[3, s, r].wait_recv()
        at_slot = slot(s, r)

        @pl.loop(0, 2 * rows // m_tile)
        def _(i):
            at = rows_at(i * m_tile, m_tile)
            term = dot(cot[at, cols_at(at_slot * depth, depth)], wd[at_slot], ((1,), (1,)))
            d_hid[at, :] = term if s == 0 and r == 0 else d_hid[at, :] + term

    add_gate_up(0, 0, 0)
    for p in range(1, n_z):
        forward(0, p)
        forward(1, p)
        for r in range(1, n_y):
            add_gate_up(p - 1, r, 0)
        add_gate_up(p, 0, 0)
    backward = range(n_z - 1, 0, -1)
    downs = [(forwarding(2, p), forwarding(3, p)) for p in backward]
    at_end = (z == 0) | (z == n_z - 1)

    def down(middle, end):
        for which, index in ((jnp.logical_not(at_end), middle), (at_end, end)):
            if index is not None and index < len(downs):
                @pl.when(which)
                def _():
                    downs[index][0]()
                    downs[index][1]()

    copies = [None, None]
    arrive(swapped[:1])
    copies[0] = across(0)
    down(0, None)
    arrive(swapped[1:])
    copies[1] = across(1)
    arrive(copies[0])
    met = meet(0)
    down(1, None)
    arrive(met)
    normalize(rows)
    down(None, 0)
    for p in range(n_z):
        for r in range(n_y):
            if p == n_z - 1 and r > 0:
                add_gate_up(p, r, 0)
            add_gate_up(p, r, 1)
    down(2, 1)

    e_tile = tile_of(2 * rows, 128)

    @pl.loop(0, 2 * rows // e_tile)
    def _(i):
        at = rows_at(i * e_tile, e_tile)
        g, u = gate[at, :], up[at, :]
        sig = jax.nn.sigmoid(g)
        act = g * sig
        hid_t[:, cols_at(i * e_tile, e_tile)] = (act * u).T.astype(BF16)
        gate[at, :] = 0.5 * (u * sig * (1.0 + g * (1.0 - sig)))
        up[at, :] = 0.5 * act

    arrive(copies[1])
    bring_cot.wait()
    arrive(meet(1))
    s_tile = tile_of(half, 512)

    def share(block, put):
        @pl.loop(0, half // s_tile)
        def _(i):
            at = rows_at(i * s_tile, s_tile)
            put(at, 0.5 * dot(hid_t[at, :], cot[:, cols_at(block * depth, depth)], ((1,), (0,))))

    def block_of(step, rel, r):
        column = 2 * lax.rem(q + step, n_q) + (h if rel == 0 else 1 - h)
        return column * n_y + lax.rem(y + r, n_y)

    y_copies = {}

    def send_share(step, rel):
        for r in range(1, n_y):
            out = y_out.at[step, rel, r]

            def put(at, value):
                out[at, :] = value.astype(BF16)

            share(block_of(step, rel, r), put)
            y_copies[step, rel, r] = send(
                out, y_in.at[step, rel, r], y_send.at[step, rel, r], y_recv.at[step, rel, r], at_y(r)
            )

    def own_block(step, rel):
        out = own_share.at[step, rel]

        def put(at, value):
            out[at, :] = value

        share(block_of(step, rel, 0), put)

    q_copies = {}

    def cross(step, rel):
        for r in range(1, n_y):
            y_copies[step, rel, r].wait_recv()

        @pl.loop(0, half // s_tile)
        def _(i):
            at = rows_at(i * s_tile, s_tile)
            total = own_share[step, rel, at, :]
            for r in range(1, n_y):
                total = total + y_in[step, rel, r, at, :].astype(F32)
            q_out[step, rel, at, :] = total.astype(BF16)

        q_copies[step, rel] = send(
            q_out.at[step, rel], q_in.at[step, rel], q_send.at[step, rel], q_recv.at[step, rel],
            at_z(2 * step),
        )

    down(None, 2)
    for index in range(3, len(downs)):
        down(index, index)
    for step in range(1, n_q):
        for rel in (1, 0):
            send_share(step, rel)
    for rel in (1, 0):
        send_share(0, rel)
    for step in range(1, n_q):
        for rel in (1, 0):
            own_block(step, rel)
    add_d_hidden(0, 0)
    for r in range(1, n_y):
        add_d_hidden(0, r)
    for p in backward:
        add_d_hidden(p, 0)
        for r in range(1, n_y):
            add_d_hidden(p, r)

    @pl.loop(0, 2 * rows // e_tile)
    def _(i):
        at = rows_at(i * e_tile, e_tile)
        d = d_hid[at, :]
        d_gate[at, :] = (d * gate[at, :]).astype(BF16)
        d_up[at, :] = (d * up[at, :]).astype(BF16)

    def partial(group, core_side, put):
        first = group * rows + core_side * side

        @pl.loop(0, n_z * n_y)
        def _(k):
            at = rows_at(first, side)
            put(cols_at(k * depth, depth),
                dot(d_gate[at, :], wg_t[k], ((1,), (0,))) + dot(d_up[at, :], wu_t[k], ((1,), (0,))))

    c_copies = {}

    def to_core(group):
        def put(at, value):
            for j in range(chunks):
                c_out[group, j, :, at] = value[j * chunk:(j + 1) * chunk].astype(BF16)

        partial(group, 1 - c, put)
        for j in range(chunks):
            c_copies[group, j] = send(
                c_out.at[group, j], c_in.at[group, j], c_send.at[group, j], c_recv.at[group, j], core
            )

    def keep(group):
        def put(at, value):
            for j in range(chunks):
                part[group, j, :, at] = value[j * chunk:(j + 1) * chunk]

        partial(group, c, put)

    l_tile = tile_of(chunk, 32)

    def each(body):
        @pl.loop(0, chunk // l_tile)
        def _(i):
            body(rows_at(i * l_tile, l_tile))

    x_copies = {}

    def to_x(group):
        for j in range(chunks):
            c_copies[group, j].wait_recv()
        for s in range(1, n_x):
            for u in range(subs):
                j = lax.rem(x + s, n_x) * subs + u

                def fold(at):
                    total = part[group, j, at, :] + c_in[group, j, at, :].astype(F32)
                    x_out[group, s, u, at, :] = total.astype(BF16)

                each(fold)
                x_copies[group, s, u] = send(
                    x_out.at[group, s, u], x_in.at[group, s, u],
                    x_send.at[group, s, u], x_recv.at[group, s, u], at_x(s)
                )

    def total_of(group, u, at):
        j = x * subs + u
        total = part[group, j, at, :] + c_in[group, j, at, :].astype(F32)
        for s in range(1, n_x):
            total = total + x_in[group, s, u, at, :].astype(F32)
        return total

    to_core(1)
    keep(1)
    to_x(1)
    for step in range(1, n_q):
        cross(step, 1)
    to_core(0)
    keep(0)
    to_x(0)
    for step in range(1, n_q):
        cross(step, 0)
    for rel in (1, 0):
        own_block(0, rel)
    m_copies = []
    for u in range(subs):
        for s in range(1, n_x):
            x_copies[1, s, u].wait_recv()

        def fold(at):
            m_out[u, at, :] = total_of(1, u, at).astype(BF16)

        each(fold)
        m_copies.append(send(m_out.at[u], m_in.at[u], m_send.at[u], m_recv.at[u], twin))
    shared, gathered = [], {}

    def place_of(at_x_index, u):
        return o_grad.at[rows_at((c * n_x + at_x_index) * (side // n_x) + u * chunk, chunk)]

    def finish(u):
        for s in range(1, n_x):
            x_copies[0, s, u].wait_recv()
        m_copies[u].wait_recv()
        first = (c * n_x + x) * (side // n_x) + u * chunk

        @pl.loop(0, chunk // l_tile)
        def _(i):
            at = rows_at(i * l_tile, l_tile)
            to = rows_at(first + i * l_tile, l_tile)
            xf = tok[to, :].astype(F32)
            inv = lax.rsqrt(jnp.mean(xf * xf, axis=-1, keepdims=True) + EPS)
            scaled = xf * inv
            d_normed = total_of(0, u, at) + m_in[u, at, :].astype(F32)
            d_scaled = d_normed * gain[...]
            inner = jnp.mean(d_scaled * scaled, axis=-1, keepdims=True)
            o_grad[to, :] = (inv * (d_scaled - scaled * inner)).astype(BF16)

        out = place_of(x, u)
        for s in range(1, n_x):
            gathered[u, s] = send(out, out, a_send.at[u, s], a_recv.at[u, s], at_x(s))
        shared.append(send(out, out, g_send.at[u, 0], g_recv.at[u, 0], core))

    def relay(u):
        for s in range(1, n_x):
            gathered[u, s].wait_recv()
            out = place_of(lax.rem(x + n_x - s, n_x), u)
            shared.append(send(out, out, g_send.at[u, s], g_recv.at[u, s], core))

    def collect(rel, put):
        for r in range(1, n_y):
            y_copies[0, rel, r].wait_recv()
        for step in range(1, n_q):
            q_copies[step, rel].wait_recv()
        total = own_share[0, rel]
        for r in range(1, n_y):
            total = total + y_in[0, rel, r].astype(F32)
        for step in range(1, n_q):
            total = total + q_in[step, rel].astype(F32)
        put(0, pl.ds(0, half), total)

    n_tile = tile_of(half, 128)

    def squares(value):
        folded = sum(value[:, k * 128:(k + 1) * 128] * value[:, k * 128:(k + 1) * 128] for k in range(depth // 128))
        return jnp.concatenate(
            [jnp.sum(folded[i:i + n_tile].T, axis=0, keepdims=True) for i in range(0, half, n_tile)], axis=1
        )

    def put_twin(start, at, value):
        t_out[at, :] = value.astype(BF16)
        n_all[f] = squares(value)

    def put_kept(start, at, value):
        o_down[rows_at(h * half + start, half), :] = value
        n_all[f] = n_all[f] + squares(value)

    collect(1, put_twin)
    traded = send(t_out, t_in, t_send, t_recv, twin)
    for u in range(subs - 1):
        finish(u)
    collect(0, put_kept)
    exchange = [
        send(n_all.at[f], n_all.at[f], n_send.at[s], n_recv.at[s], {"fs": lax.rem(f + s, n_fs)})
        for s in range(1, n_fs)
    ]
    finish(subs - 1)
    for u in range(subs - 1):
        relay(u)
    traded.wait_recv()
    o_down[rows_at((1 - h) * half, half), :] = t_in[...].astype(F32)
    for copy in exchange:
        copy.wait_recv()
    for side_of in range(2):
        total = sum(n_all[k] for k in range(n_fs) if k // n_y % 2 == side_of)
        o_norms[:, side_of * half:(side_of + 1) * half] = total
    relay(subs - 1)
    for copy in shared:
        copy.wait_recv()
    for copy in started:
        copy.wait_send()


def fused(n_z, n_y, n_x, tokens, norm_gain, w_gate, w_up, w_down, cotangent):
    n_fs, n_tp, n_q = n_z * n_y, 2 * n_x, n_z // 2
    rows, d_model = tokens.shape
    depth, half = w_gate.shape[0], w_gate.shape[1] // 2
    subs = 2 if rows % (32 * n_tp) == 0 else 1
    chunks = n_x * subs
    chunk = rows // 2 // chunks
    dma, vmem = pltpu.SemaphoreType.DMA, pltpu.VMEM
    outside = pl.BlockSpec(memory_space=pltpu.HBM)
    inside = pl.BlockSpec(memory_space=pltpu.VMEM)
    block = (half, depth)
    scratch = [
        vmem((1, d_model), F32),
        vmem((2 * rows, d_model), BF16), vmem((2 * rows, d_model), BF16), vmem((2 * rows, d_model), BF16),
        vmem((n_fs, depth, half), BF16), vmem((n_fs, depth, half), BF16), vmem((n_fs, half, depth), BF16),
        vmem((n_fs, half, depth), BF16), vmem((n_fs, half, depth), BF16),
        vmem((2 * rows, half), F32), vmem((2 * rows, half), F32), vmem((2 * rows, half), F32),
        vmem((half, 2 * rows), BF16), vmem((2 * rows, half), BF16), vmem((2 * rows, half), BF16),
        vmem((n_q, 2) + block, F32), vmem((n_q, 2, n_y) + block, BF16), vmem((n_q, 2, n_y) + block, BF16),
        vmem((n_q, 2) + block, BF16), vmem((n_q, 2) + block, BF16), vmem(block, BF16), vmem(block, BF16),
        vmem((n_fs, 1, half), F32),
        vmem((2, chunks, chunk, d_model), F32),
        vmem((2, chunks, chunk, d_model), BF16), vmem((2, chunks, chunk, d_model), BF16),
        vmem((subs, chunk, d_model), BF16), vmem((subs, chunk, d_model), BF16),
        vmem((2, n_x, subs, chunk, d_model), BF16), vmem((2, n_x, subs, chunk, d_model), BF16),
        dma((4, n_z)), dma((4, n_z)), dma((4, n_z, n_y)), dma((4, n_z, n_y)),
        dma((2,)), dma((2,)), dma((2, n_x)), dma((2, n_x)), dma((2, n_x)), dma((2, n_x)),
        dma((n_q, 2, n_y)), dma((n_q, 2, n_y)), dma((n_q, 2)), dma((n_q, 2)), dma, dma,
        dma((n_fs,)), dma((n_fs,)),
        dma((2, chunks)), dma((2, chunks)), dma((subs,)), dma((subs,)),
        dma((2, n_x, subs)), dma((2, n_x, subs)), dma((subs, n_x)), dma((subs, n_x)),
        dma((subs, n_x)), dma((subs, n_x)), dma((7,)),
    ]
    grad, down, norms = pl.pallas_call(
        functools.partial(fused_kernel, n_z, n_y, n_x),
        out_shape=[
            jax.ShapeDtypeStruct((rows, d_model), BF16),
            jax.ShapeDtypeStruct((2 * half, depth), F32),
            jax.ShapeDtypeStruct((1, 2 * half), F32),
        ],
        in_specs=[outside] * 6,
        out_specs=[inside, inside, inside],
        scratch_shapes=scratch,
        compiler_params=pltpu.CompilerParams(
            collective_id=1, has_side_effects=True, vmem_limit_bytes=48 * 2**20
        ),
    )(*[
        pltpu.with_memory_space_constraint(a, pltpu.HBM)
        for a in (tokens, cotangent, norm_gain.reshape(1, d_model), w_gate, w_up, w_down)
    ])
    return grad, down, norms.reshape(2 * half)


def shards(n_fs, n_tp, tokens, norm_gain, w_gate, w_up, w_down, cotangent):
    n_y = 2 ** ((n_fs.bit_length() - 1) // 2)
    n_z, n_x = n_fs // n_y, n_tp // 2
    n_q = n_z // 2
    f, t = lax.axis_index("fs"), lax.axis_index("tp")
    z, y, x, c = f // n_y, f % n_y, t // 2, t % 2
    q, h = z // 2, z % 2
    rows, d_model = tokens.shape
    depth, half = w_gate.shape[0], w_gate.shape[1] // 2
    piece = rows // n_tp

    if piece % 16 == 0 and depth % 128 == 0 and half % 128 == 0:
        return fused(n_z, n_y, n_x, tokens, norm_gain, w_gate, w_up, w_down, cotangent)

    def to_z(a, step):
        return lax.ppermute(a, "fs", [(i, (i + step * n_y) % n_fs) for i in range(n_fs)])

    def to_y(a, step):
        return lax.ppermute(
            a, "fs", [(i, i // n_y * n_y + (i + step) % n_y) for i in range(n_fs)]
        )

    def to_twin(a):
        return lax.ppermute(
            a, "fs", [(i, (i // n_y ^ 1) * n_y + i % n_y) for i in range(n_fs)]
        )

    def to_x(a, step):
        return lax.ppermute(a, "tp", [(i, (i + 2 * step) % n_tp) for i in range(n_tp)])

    def to_core(a):
        return lax.ppermute(a, "tp", [(i, i ^ 1) for i in range(n_tp)])

    mine = jnp.stack(
        [lax.dynamic_slice_in_dim(a, t * piece, piece, 0) for a in (tokens, cotangent)]
    )
    down_t = w_down.T

    def half_of(which):
        gate_up = jnp.concatenate(
            [lax.dynamic_slice_in_dim(w, which * half, half, 1) for w in (w_gate, w_up)], axis=1
        )
        return gate_up, lax.dynamic_slice_in_dim(down_t, which * half, half, 1)

    own, other = half_of(h), half_of(1 - h)

    w_gu, w_dn, got = gather_all(n_z, n_y, n_x, own, other, mine)
    w_gu, w_dn = w_gu.reshape(d_model, 2 * half), w_dn.reshape(d_model, half)
    got = got.reshape(2, rows, d_model)
    tokens2 = jnp.concatenate([tokens, got[0]], axis=0)
    cot2 = jnp.concatenate([cotangent, got[1]], axis=0)

    xf = tokens2.astype(F32)
    inv = lax.rsqrt(jnp.mean(xf * xf, axis=-1, keepdims=True) + EPS)
    normed = (xf * inv * norm_gain).astype(BF16)
    gate_up = jnp.dot(normed, w_gu, preferred_element_type=F32)
    gate, up = gate_up[:, :half], gate_up[:, half:]
    sig = jax.nn.sigmoid(gate)
    act = gate * sig
    hidden = (act * up).astype(BF16)

    share = 0.5 * lax.dot_general(
        cot2, hidden, (((0,), (0,)), ((), ())), preferred_element_type=F32
    )
    share = share.reshape(n_q, 2, n_y, depth, half)
    share, w_dn = lax.optimization_barrier((share, w_dn))

    def sent_over_y(pair):
        block = take(share, pair)
        return [to_y(take(block, (y + s) % n_y, 1).astype(BF16), s) for s in range(1, n_y)]

    def over_y(pair, came):
        return sum([a.astype(F32) for a in came], take(take(share, pair), y, 1))

    first = [sent_over_y((q + s) % n_q) for s in range(1, n_q)]

    d_hidden = 0.5 * jnp.dot(cot2, w_dn, preferred_element_type=F32)
    d_gate = (d_hidden * up * sig * (1.0 + gate * (1.0 - sig))).astype(BF16)
    d_up = (d_hidden * act).astype(BF16)
    d_both = jnp.concatenate([d_gate, d_up], axis=1)
    part = lax.dot_general(
        d_both, w_gu, (((1,), (1,)), ((), ())), preferred_element_type=F32
    )
    part, first = lax.optimization_barrier((part.astype(BF16), first))

    away = [
        to_z(over_y((q + s) % n_q, first[s - 1]).astype(BF16), 2 * s) for s in range(1, n_q)
    ]
    total = over_y(q, sent_over_y(q))
    total = sum([a.astype(F32) for a in away], total)
    kept = take(total, h)
    came = to_twin(take(total, 1 - h).astype(BF16)).astype(F32)
    grad_down = place([(h, kept.T), (1 - h, came.T)], 2).reshape(2 * half, depth)
    norms = jnp.sum(grad_down * grad_down, axis=1)
    norms = sum([to_y(norms, s) for s in range(1, n_y)], norms)
    down_norms = sum([to_z(norms, s) for s in range(1, n_z)], norms)

    part = part.reshape(2, n_x, 2, piece, d_model)
    part = take(part, c, 2).astype(F32) + to_core(take(part, 1 - c, 2)).astype(F32)
    total = take(part, x, 1)
    for s in range(1, n_x):
        total = total + to_x(take(part, (x + s) % n_x, 1).astype(BF16), s).astype(F32)
    d_normed = total[0] + to_twin(total[1].astype(BF16)).astype(F32)

    xp = lax.dynamic_slice_in_dim(tokens, t * piece, piece, 0).astype(F32)
    inv_p = lax.rsqrt(jnp.mean(xp * xp, axis=-1, keepdims=True) + EPS)
    scaled = xp * inv_p
    d_scaled = d_normed * norm_gain
    inner = jnp.mean(d_scaled * scaled, axis=-1, keepdims=True)
    grad = (inv_p * (d_scaled - scaled * inner)).astype(BF16)
    grad = place([(x, grad)] + [((x - s) % n_x, to_x(grad, s)) for s in range(1, n_x)], n_x)
    grad = place([(c, grad), (1 - c, to_core(grad))], 2)
    grad_tokens = grad.transpose(1, 0, 2, 3).reshape(rows, d_model)
    return (grad_tokens, grad_down, down_norms)


def solution(mesh):
    in_specs = (P("fs", None), P(), P("fs", "tp"), P("fs", "tp"), P("tp", "fs"), P("fs", None))
    out_specs = (P("fs", None), P("tp", "fs"), P("tp"))
    return jax.shard_map(
        functools.partial(shards, mesh.shape["fs"], mesh.shape["tp"]),
        mesh=mesh, in_specs=in_specs, out_specs=out_specs, check_vma=False,
    )
```

```python
import functools

import jax
import jax.numpy as jnp
from jax import lax
from jax.experimental import pallas as pl
from jax.experimental.pallas import tpu as pltpu
from jax.sharding import PartitionSpec as P

EPS = 1e-06
BF16 = jnp.bfloat16
F32 = jnp.float32


def place(pieces, count):
    first = pieces[0][1]
    held = jnp.zeros((count,) + first.shape, first.dtype)
    for position, piece in pieces:
        held = lax.dynamic_update_slice_in_dim(held, piece[None], position, 0)
    return held


def take(array, position, axis=0):
    return lax.dynamic_index_in_dim(array, position, axis, keepdims=False)


def gather_kernel(n_z, n_y, n_x, own_gu, own_dn, other_gu, other_dn, mine, w_gu, w_dn, got,
                  z_send, z_recv, y_send, y_recv, x_send, x_recv, c_send, c_recv, local):
    f, t = lax.axis_index("fs"), lax.axis_index("tp")
    z, y, x, c = lax.div(f, n_y), lax.rem(f, n_y), lax.div(t, 2), lax.rem(t, 2)
    n_tp = 2 * n_x
    sources = ((own_gu, other_gu), (own_dn, other_dn))
    held = (w_gu, w_dn)

    def at_z(s):
        return {"fs": lax.rem(z + s, n_z) * n_y + y}

    def at_y(r):
        return {"fs": z * n_y + lax.rem(y + r, n_y)}

    def at_x(s):
        return {"tp": lax.rem(t + 2 * s, n_tp)}

    twin = {"fs": (z + 1 - 2 * lax.rem(z, 2)) * n_y + y}
    core = {"tp": t + 1 - 2 * c}

    barrier = pltpu.get_barrier_semaphore()
    friends = [at_z(s) for s in range(1, n_z)] + [at_y(r) for r in range(1, n_y)]
    friends += [at_x(s) for s in range(1, n_x)] + [core]
    for friend in friends:
        pl.semaphore_signal(barrier, inc=1, device_id=friend, device_id_type=pl.DeviceIdType.MESH)
    pl.semaphore_wait(barrier, len(friends))

    started = []

    def send(src, dst, out_sem, in_sem, to):
        copy = pltpu.make_async_remote_copy(
            src_ref=src, dst_ref=dst, send_sem=out_sem, recv_sem=in_sem,
            device_id=to, device_id_type=pl.DeviceIdType.MESH,
        )
        copy.start()
        started.append(copy)
        return copy

    order = sorted(range(1, n_z), key=lambda s: min(s, n_z - s))
    from_z = {}

    def start_z(k):
        for s in order:
            from_z[k, s] = send(
                sources[k][s % 2], held[k].at[f], z_send.at[k, s], z_recv.at[k, s], at_z(s)
            )

    late = []

    def forward(k, s):
        if s == 0:
            src = sources[k][0]
            slot = f
        else:
            from_z[k, s].wait_recv()
            slot = lax.rem(z + n_z - s, n_z) * n_y + y
            src = held[k].at[slot]
        for r in range(1, n_y):
            late.append(send(
                src, held[k].at[slot], y_send.at[k, s, r], y_recv.at[k, s, r], at_y(r)
            ))

    start_z(0)
    forward(0, 0)
    tokens = send(mine, got.at[:, x, c], x_send.at[0], x_recv.at[0], twin)
    start_z(1)
    forward(1, 0)
    stays = [pltpu.make_async_copy(sources[k][0], held[k].at[f], local.at[k]) for k in range(2)]
    for copy in stays:
        copy.start()
    for s in order:
        forward(0, s)
    tokens.wait_recv()
    across = [
        send(got.at[:, x, c], got.at[:, x, c], x_send.at[s], x_recv.at[s], at_x(s))
        for s in range(1, n_x)
    ]
    for s in order[:-1]:
        forward(1, s)
    for copy in across:
        copy.wait_recv()
    late.append(send(got.at[:, :, c], got.at[:, :, c], c_send, c_recv, core))
    forward(1, order[-1])
    for copy in late:
        copy.wait_recv()
    for copy in started:
        copy.wait_send()
    for copy in stays:
        copy.wait()


def gather_all(n_z, n_y, n_x, own, other, mine):
    n_fs = n_z * n_y
    dma = pltpu.SemaphoreType.DMA
    anywhere = pl.BlockSpec(memory_space=pl.ANY)
    return pl.pallas_call(
        functools.partial(gather_kernel, n_z, n_y, n_x),
        out_shape=[jax.ShapeDtypeStruct((n_fs,) + a.shape, a.dtype) for a in own]
        + [jax.ShapeDtypeStruct((2, n_x, 2) + mine.shape[1:], mine.dtype)],
        in_specs=[anywhere] * 5,
        out_specs=[anywhere] * 3,
        scratch_shapes=[
            dma((2, n_z)), dma((2, n_z)), dma((2, n_z, n_y)), dma((2, n_z, n_y)),
            dma((n_x,)), dma((n_x,)), dma, dma, dma((2,)),
        ],
        compiler_params=pltpu.CompilerParams(collective_id=0, has_side_effects=True),
    )(*own, *other, mine)


def tile_of(extent, most):
    return max(n for n in range(16, most + 1, 16) if extent % n == 0)


def dot(a, b, contract):
    return lax.dot_general(a, b, (contract, ((), ())), preferred_element_type=F32)


def rows_at(start, count):
    return pl.ds(pl.multiple_of(start, 16), count)


def cols_at(start, count):
    return pl.ds(pl.multiple_of(start, 128), count)


def fused_kernel(n_z, n_y, n_x, tokens, cotangent, gain_in, w_gate, w_up, w_down,
                 o_grad, o_down, o_norms,
                 gain, tok, cot, normed, wg, wu, wd, wg_t, wu_t, gate, up, d_hid, hid_t, d_gate, d_up,
                 own_share, y_out, y_in, q_out, q_in, t_out, t_in, n_all,
                 part, c_out, c_in, m_out, m_in, x_out, x_in,
                 sent, z_recv, f_recv, tt_recv, tx_recv, tc_recv, y_recv, q_recv, t_recv, n_recv,
                 c_recv, m_recv, x_recv, a_recv, g_recv, local):
    f, t = lax.axis_index("fs"), lax.axis_index("tp")
    z, y, x, c = lax.div(f, n_y), lax.rem(f, n_y), lax.div(t, 2), lax.rem(t, 2)
    q, h = lax.div(z, 2), lax.rem(z, 2)
    n_tp, n_q = 2 * n_x, n_z // 2
    rows, d_model = tokens.shape
    depth, half = wg.shape[1], wg.shape[2]
    piece = rows // n_tp
    chunks, subs = c_out.shape[1], m_out.shape[0]
    side = rows // 2
    chunk = side // chunks

    def at_z(s):
        return {"fs": lax.rem(z + s, n_z) * n_y + y}

    def at_y(r):
        return {"fs": z * n_y + lax.rem(y + r, n_y)}

    def at_x(s):
        return {"tp": lax.rem(t + 2 * s, n_tp)}

    twin = {"fs": (z + 1 - 2 * h) * n_y + y}
    core = {"tp": t + 1 - 2 * c}

    started = [], []

    def copy_to(src, dst, in_sem, to, phase=0):
        copy = pltpu.make_async_remote_copy(
            src_ref=src, dst_ref=dst, send_sem=sent.at[phase], recv_sem=in_sem,
            device_id=to, device_id_type=pl.DeviceIdType.MESH,
        )
        started[phase].append(copy)
        return copy

    def send(*args):
        copy = copy_to(*args)
        copy.start()
        return copy

    def bring(src, dst, sem):
        copy = pltpu.make_async_copy(src, dst, sem)
        copy.start()
        return copy

    kinds = z_recv.shape[0]
    downs_of = range(2, kinds)
    step_rows = half // len(downs_of)

    def source(k, which):
        if k >= 2:
            return w_down.at[rows_at(which * half + (k - 2) * step_rows, step_rows), :]
        return (w_gate, w_up)[k].at[:, cols_at(which * half, half)]

    def held(k, at_slot):
        if k >= 2:
            return wd.at[at_slot, pl.ds((k - 2) * step_rows, step_rows)]
        return (wg, wu)[k].at[at_slot]

    bring_gain = bring(gain_in, gain, local.at[2 + z_recv.shape[0]])
    bring_tok = bring(tokens, tok.at[pl.ds(0, rows)], local.at[0])
    bring_cot = bring(cotangent, cot.at[pl.ds(0, rows)], local.at[1])
    stays = [bring(source(k, h), held(k, f), local.at[2 + k]) for k in range(kinds)]

    barrier = pltpu.get_barrier_semaphore()
    n_fs = n_z * n_y
    friends = [{"fs": lax.rem(f + s, n_fs)} for s in range(1, n_fs)]
    friends += [at_x(s) for s in range(1, n_x)] + [core]
    for friend in friends:
        pl.semaphore_signal(barrier, inc=1, device_id=friend, device_id_type=pl.DeviceIdType.MESH)
    pl.semaphore_wait(barrier, len(friends))

    over_y = {}
    others = [[b for b in range(n_z) if b != a] for a in range(n_z)]
    ends = (0, n_z - 1)
    nearest = [sorted(others[a], key=lambda b: abs(a - b)) for a in range(n_z)]
    arrival = [
        [a] + sorted(others[a], key=lambda b: 1 if b == a ^ 1 else 2 * (b not in ends)) for a in range(n_z)
    ]

    def pick(table, p):
        return sum(jnp.where(z == a, table[a][p], 0) for a in range(n_z))

    near = [z] + [pick(arrival, p) for p in range(1, n_z)]

    def start_z(k, p):
        to = pick(nearest, p)
        send(
            source(k, lax.rem(to, 2)), held(k, f), z_recv.at[k, z],
            {"fs": to * n_y + y},
        )

    def slot(p, r):
        return near[p] * n_y + lax.rem(y + n_y - r, n_y)

    def forwarding(k, p):
        if p == 0:
            src, came = source(k, h), None
        else:
            src = held(k, slot(p, 0))
            came = pltpu.make_async_remote_copy(
                src_ref=src, dst_ref=src, send_sem=sent.at[0], recv_sem=z_recv.at[k, near[p]],
                device_id={"fs": near[p] * n_y + y}, device_id_type=pl.DeviceIdType.MESH,
            )
        for r in range(1, n_y):
            over_y[k, p, r] = copy_to(src, held(k, slot(p, 0)), f_recv.at[k, near[p], r - 1], at_y(r))

        def go():
            if came is not None:
                came.wait_recv()
            for r in range(1, n_y):
                over_y[k, p, r].start()

        return go

    def forward(k, p):
        forwarding(k, p)()

    raw, both = (tokens, cotangent), (tok, cot)

    cuts = tt_recv.shape[1]
    cut = piece // cuts

    def cut_of(start, i):
        return rows_at(start + i * cut, cut)

    def swap(a):
        return [
            send(raw[a].at[cut_of(t * piece, i)], both[a].at[cut_of(rows + t * piece, i)],
                 tt_recv.at[a, i], twin)
            for i in range(cuts)
        ]

    def across(a, parts):
        copies = []
        for i in parts:
            swapped[a][i].wait_recv()
            at = both[a].at[cut_of(rows + t * piece, i)]
            copies += [send(at, at, tx_recv.at[a, i, s - 1], at_x(s)) for s in range(1, n_x)]
        return copies

    def meet(a):
        copies = []
        for k in range(n_x):
            at = rows_at(rows + (2 * k + c) * piece, piece)
            copies.append(send(both[a].at[at], both[a].at[at], tc_recv.at[a, k], core))
        return copies

    def arrive(copies):
        for copy in copies:
            copy.wait_recv()

    swapped = []
    for p in reversed(range(n_z - 1)):
        start_z(0, p)
        start_z(1, p)
        if p == n_z - 2:
            forward(0, 0)
            forward(1, 0)
            for k in downs_of:
                forward(k, 0)
    for a in range(2):
        swapped.append(swap(a))
    for p in range(n_z - 1):
        for k in downs_of:
            start_z(k, p)

    norm_tile = tile_of(rows, 32)

    def normalize(first):
        @pl.loop(0, rows // norm_tile)
        def _(i):
            at = rows_at(first + i * norm_tile, norm_tile)
            xf = tok[at, :].astype(F32)
            inv = lax.rsqrt(jnp.mean(xf * xf, axis=-1, keepdims=True) + EPS)
            normed[at, :] = (xf * inv * gain[...]).astype(BF16)

    bring_gain.wait()
    bring_tok.wait()
    normalize(0)

    m_tile = tile_of(2 * rows, 768)

    def add_gate_up(p, r, group):
        at_slot = slot(p, r)
        if group == 0:
            if p == 0 and r == 0:
                stays[0].wait()
                stays[1].wait()
            elif r > 0:
                over_y[0, p, r].wait_recv()
                over_y[1, p, r].wait_recv()
            wg_t[at_slot] = wg[at_slot].T
            wu_t[at_slot] = wu[at_slot].T
        at = pl.ds(group * rows, rows)
        a = normed[at, cols_at(at_slot * depth, depth)]
        for total, w in ((gate, wg), (up, wu)):
            term = dot(a, w[at_slot], ((1,), (0,)))
            total[at, :] = term if p == 0 and r == 0 else total[at, :] + term

    def add_d_hidden(s, r):
        if s == 0 and r == 0:
            for k in downs_of:
                stays[k].wait()
        elif r > 0:
            for k in downs_of:
                over_y[k, s, r].wait_recv()
        at_slot = slot(s, r)

        @pl.loop(0, 2 * rows // m_tile)
        def _(i):
            at = rows_at(i * m_tile, m_tile)
            term = dot(cot[at, cols_at(at_slot * depth, depth)], wd[at_slot], ((1,), (1,)))
            d_hid[at, :] = term if s == 0 and r == 0 else d_hid[at, :] + term

    add_gate_up(0, 0, 0)
    token_copies = []
    for p in range(1, n_z):
        forward(0, p)
        if p == n_z - 1:
            token_copies += across(0, range(cuts - 1))
        forward(1, p)
        if p == n_z - 1:
            token_copies += across(0, range(cuts - 1, cuts))
        for r in range(1, n_y):
            add_gate_up(p - 1, r, 0)
        add_gate_up(p, 0, 0)
    backward = range(n_z - 1, 0, -1)
    downs = [[forwarding(k, p) for k in downs_of] for p in backward]
    at_end = (z == 0) | (z == n_z - 1)

    def down(middle, end):
        for which, index in ((jnp.logical_not(at_end), middle), (at_end, end)):
            if index is not None and index < len(downs):
                @pl.when(which)
                def _():
                    for go in downs[index]:
                        go()

    down(0, None)
    cot_copies = across(1, range(cuts))
    arrive(token_copies)
    met = meet(0)
    down(1, None)
    arrive(met)
    normalize(rows)
    down(None, 0)
    for p in range(n_z):
        for r in range(n_y):
            if p == n_z - 1 and r > 0:
                add_gate_up(p, r, 0)
            add_gate_up(p, r, 1)
    down(2, 1)

    e_tile = tile_of(2 * rows, 128)

    @pl.loop(0, 2 * rows // e_tile)
    def _(i):
        at = rows_at(i * e_tile, e_tile)
        g, u = gate[at, :], up[at, :]
        sig = jax.nn.sigmoid(g)
        act = g * sig
        hid_t[:, cols_at(i * e_tile, e_tile)] = (act * u).T.astype(BF16)
        gate[at, :] = 0.5 * (u * sig * (1.0 + g * (1.0 - sig)))
        up[at, :] = 0.5 * act

    arrive(cot_copies)
    bring_cot.wait()
    arrive(meet(1))
    s_tile = tile_of(half, 512)

    def share(block, put):
        @pl.loop(0, half // s_tile)
        def _(i):
            at = rows_at(i * s_tile, s_tile)
            put(at, 0.5 * dot(hid_t[at, :], cot[:, cols_at(block * depth, depth)], ((1,), (0,))))

    def block_of(step, rel, r):
        column = 2 * lax.rem(q + step, n_q) + (h if rel == 0 else 1 - h)
        return column * n_y + lax.rem(y + r, n_y)

    y_copies = {}

    def send_share(step, rel):
        for r in range(1, n_y):
            out = y_out.at[step, rel, r]

            def put(at, value):
                out[at, :] = value.astype(BF16)

            share(block_of(step, rel, r), put)
            y_copies[step, rel, r] = send(
                out, y_in.at[step, rel, r], y_recv.at[step, rel, r - 1], at_y(r)
            )

    def own_block(step, rel):
        out = own_share.at[step, rel]

        def put(at, value):
            out[at, :] = value

        share(block_of(step, rel, 0), put)

    q_copies = {
        (step, rel): copy_to(q_out.at[step, rel], q_in.at[step, rel], q_recv.at[step, rel], at_z(2 * step))
        for step in range(1, n_q) for rel in range(2)
    }

    def cross(rel):
        for step in range(1, n_q):
            for r in range(1, n_y):
                y_copies[step, rel, r].wait_recv()
            total = own_share[step, rel]
            for r in range(1, n_y):
                total = total + y_in[step, rel, r].astype(F32)
            q_out[step, rel] = total.astype(BF16)
            q_copies[step, rel].start()

    down(None, 2)
    for step in range(1, n_q):
        send_share(step, 1)
    for index in range(3, len(downs)):
        down(index, index)
    for step in range(1, n_q):
        send_share(step, 0)
    for rel in (1, 0):
        send_share(0, rel)
    for step in range(1, n_q):
        for rel in (1, 0):
            own_block(step, rel)
    add_d_hidden(0, 0)
    for r in range(1, n_y):
        add_d_hidden(0, r)
    for p in backward:
        add_d_hidden(p, 0)
        for r in range(1, n_y):
            add_d_hidden(p, r)

    d_tile = tile_of(side, 128)

    @pl.loop(0, 2 * rows // d_tile)
    def _(i):
        at = rows_at(i * d_tile, d_tile)
        index = lax.div(i * d_tile, side)
        to = (index - lax.rem(index, 2) + lax.rem(index + c + 1, 2)) * side + lax.rem(i * d_tile, side)
        d = d_hid[at, :]
        d_gate[rows_at(to, d_tile), :] = (d * gate[at, :]).astype(BF16)
        d_up[rows_at(to, d_tile), :] = (d * up[at, :]).astype(BF16)

    c_copies = {}

    def owner_of(s):
        return lax.rem(x + s, n_x) * subs

    def partial(group):
        @pl.loop(0, n_z * n_y)
        def _(k):
            at, to = pl.ds(group * rows, rows), cols_at(k * depth, depth)
            value = dot(d_gate[at, :], wg_t[k], ((1,), (0,))) + dot(d_up[at, :], wu_t[k], ((1,), (0,)))
            for j in range(chunks):
                c_out[group, j, :, to] = value[j * chunk:(j + 1) * chunk].astype(BF16)
                part[group, j, :, to] = value[side + j * chunk:side + (j + 1) * chunk]

        for s in (*range(1, n_x), 0):
            for u in range(subs):
                j = owner_of(s) + u
                c_copies[group, s, u] = send(
                    c_out.at[group, j], c_in.at[group, j], c_recv.at[group, j], core
                )

    l_tile = tile_of(chunk, 32)

    def each(body):
        @pl.loop(0, chunk // l_tile)
        def _(i):
            body(rows_at(i * l_tile, l_tile))

    x_copies, m_copies = {}, {}

    def summed(group, j, at):
        return part[group, j, at, :] + c_in[group, j, at, :].astype(F32)

    def to_x(group):
        for u in range(subs):
            for s in range(1, n_x):
                c_copies[group, s, u].wait_recv()
                j = owner_of(s) + u

                def fold(at):
                    x_out[group, s, u, at, :] = summed(group, j, at).astype(BF16)

                each(fold)
                x_copies[group, s, u] = send(
                    x_out.at[group, s, u], x_in.at[group, s, u], x_recv.at[group, s - 1, u], at_x(s)
                )

    def total_of(group, u, at):
        total = summed(group, owner_of(0) + u, at)
        for s in range(1, n_x):
            total = total + x_in[group, s, u, at, :].astype(F32)
        return total

    partial(1)
    pl.when(jnp.logical_not(at_end))(functools.partial(cross, 1))
    to_x(1)
    pl.when(at_end)(functools.partial(cross, 1))
    partial(0)
    to_x(0)
    cross(0)
    for rel in (1, 0):
        own_block(0, rel)
    for u in range(subs):
        c_copies[1, 0, u].wait_recv()
        for s in range(1, n_x):
            x_copies[1, s, u].wait_recv()

        def fold(at):
            m_out[u, at, :] = total_of(1, u, at).astype(BF16)

        each(fold)
        m_copies[u] = send(m_out.at[u], m_in.at[u], m_recv.at[u], twin)
    for u in range(subs):
        c_copies[0, 0, u].wait_recv()
    shared, gathered = [], {}

    def place_of(at_x_index, u):
        return o_grad.at[rows_at((c * n_x + at_x_index) * piece + u * chunk, chunk)]

    def finish(u):
        for s in range(1, n_x):
            x_copies[0, s, u].wait_recv()
        m_copies[u].wait_recv()
        first = (c * n_x + x) * piece + u * chunk

        @pl.loop(0, chunk // l_tile)
        def _(i):
            at = rows_at(i * l_tile, l_tile)
            to = rows_at(first + i * l_tile, l_tile)
            xf = tok[to, :].astype(F32)
            inv = lax.rsqrt(jnp.mean(xf * xf, axis=-1, keepdims=True) + EPS)
            scaled = xf * inv
            d_normed = total_of(0, u, at) + m_in[u, at, :].astype(F32)
            d_scaled = d_normed * gain[...]
            inner = jnp.mean(d_scaled * scaled, axis=-1, keepdims=True)
            o_grad[to, :] = (inv * (d_scaled - scaled * inner)).astype(BF16)

        out = place_of(x, u)
        for s in range(1, n_x):
            gathered[u, s] = send(out, out, a_recv.at[u, s - 1], at_x(s), 1)
        shared.append(send(out, out, g_recv.at[u, 0], core, 1))

    def relay(u):
        for s in range(1, n_x):
            gathered[u, s].wait_recv()
            out = place_of(lax.rem(x + n_x - s, n_x), u)
            shared.append(send(out, out, g_recv.at[u, s], core, 1))

    def collect(rel, put):
        for r in range(1, n_y):
            y_copies[0, rel, r].wait_recv()
        for step in range(1, n_q):
            q_copies[step, rel].wait_recv()
        total = own_share[0, rel]
        for r in range(1, n_y):
            total = total + y_in[0, rel, r].astype(F32)
        for step in range(1, n_q):
            total = total + q_in[step, rel].astype(F32)
        put(0, pl.ds(0, half), total)

    n_tile = tile_of(half, 128)

    def squares(value):
        folded = sum(value[:, k * 128:(k + 1) * 128] * value[:, k * 128:(k + 1) * 128] for k in range(depth // 128))
        return jnp.concatenate(
            [jnp.sum(folded[i:i + n_tile].T, axis=0, keepdims=True) for i in range(0, half, n_tile)], axis=1
        )

    def put_twin(start, at, value):
        t_out[at, :] = value.astype(BF16)
        n_all[f] = squares(value)

    def put_kept(start, at, value):
        o_down[rows_at(h * half + start, half), :] = value
        n_all[f] = n_all[f] + squares(value)

    collect(1, put_twin)
    for u in range(subs - 1):
        finish(u)
    collect(0, put_kept)
    exchange = [
        send(n_all.at[f], n_all.at[f], n_recv.at[s - 1], {"fs": lax.rem(f + s, n_fs)}, 1)
        for s in range(1, n_fs)
    ]
    traded = send(t_out, t_in, t_recv, twin, 1)
    finish(subs - 1)
    for copy in started[0]:
        copy.wait_send()
    for u in range(subs - 1):
        relay(u)
    traded.wait_recv()
    o_down[rows_at((1 - h) * half, half), :] = t_in[...].astype(F32)
    for copy in exchange:
        copy.wait_recv()
    for side_of in range(2):
        total = sum(n_all[k] for k in range(n_fs) if k // n_y % 2 == side_of)
        o_norms[:, side_of * half:(side_of + 1) * half] = total
    relay(subs - 1)
    for copy in shared:
        copy.wait_recv()
    for copy in started[1]:
        copy.wait_send()


def put_out(grad, down, norms, o_grad, o_down, o_norms, done):
    copies = [
        pltpu.make_async_copy(src, dst, done.at[i])
        for i, (src, dst) in enumerate(((grad, o_grad), (down, o_down), (norms, o_norms)))
    ]
    for copy in copies:
        copy.start()
    for copy in copies:
        copy.wait()


def fused(n_z, n_y, n_x, tokens, norm_gain, w_gate, w_up, w_down, cotangent):
    n_fs, n_tp, n_q = n_z * n_y, 2 * n_x, n_z // 2
    rows, d_model = tokens.shape
    depth, half = w_gate.shape[0], w_gate.shape[1] // 2
    piece = rows // n_tp
    cuts = 2 if piece % 32 == 0 else 1
    kinds = 2 + 4
    subs = max(n for n in (1, 2, 3) if piece % (16 * n) == 0)
    chunks = n_x * subs
    chunk = rows // 2 // chunks
    dma, vmem = pltpu.SemaphoreType.DMA, pltpu.VMEM
    outside = pl.BlockSpec(memory_space=pltpu.HBM)
    inside = pl.BlockSpec(memory_space=pltpu.VMEM)
    block = (half, depth)
    scratch = [
        vmem((1, d_model), F32),
        vmem((2 * rows, d_model), BF16), vmem((2 * rows, d_model), BF16), vmem((2 * rows, d_model), BF16),
        vmem((n_fs, depth, half), BF16), vmem((n_fs, depth, half), BF16), vmem((n_fs, half, depth), BF16),
        vmem((n_fs, half, depth), BF16), vmem((n_fs, half, depth), BF16),
        vmem((2 * rows, half), F32), vmem((2 * rows, half), F32), vmem((2 * rows, half), F32),
        vmem((half, 2 * rows), BF16), vmem((2 * rows, half), BF16), vmem((2 * rows, half), BF16),
        vmem((n_q, 2) + block, F32), vmem((n_q, 2, n_y) + block, BF16), vmem((n_q, 2, n_y) + block, BF16),
        vmem((n_q, 2) + block, BF16), vmem((n_q, 2) + block, BF16), vmem(block, BF16), vmem(block, BF16),
        vmem((n_fs, 1, half), F32),
        vmem((2, chunks, chunk, d_model), F32),
        vmem((2, chunks, chunk, d_model), BF16), vmem((2, chunks, chunk, d_model), BF16),
        vmem((subs, chunk, d_model), BF16), vmem((subs, chunk, d_model), BF16),
        vmem((2, n_x, subs, chunk, d_model), BF16), vmem((2, n_x, subs, chunk, d_model), BF16),
        dma((2,)), dma((kinds, n_z)), dma((kinds, n_z, n_y - 1)),
        dma((2, cuts)), dma((2, cuts, n_x - 1)), dma((2, n_x)),
        dma((n_q, 2, n_y - 1)), dma((n_q, 2)), dma, dma((n_fs - 1,)),
        dma((2, chunks)), dma((subs,)), dma((2, n_x - 1, subs)), dma((subs, n_x - 1)),
        dma((subs, n_x)), dma((kinds + 3,)),
    ]
    grad, down, norms = pl.pallas_call(
        functools.partial(fused_kernel, n_z, n_y, n_x),
        out_shape=[
            jax.ShapeDtypeStruct((rows, d_model), BF16),
            jax.ShapeDtypeStruct((2 * half, depth), F32),
            jax.ShapeDtypeStruct((1, 2 * half), F32),
        ],
        in_specs=[outside] * 6,
        out_specs=[inside, inside, inside],
        scratch_shapes=scratch,
        compiler_params=pltpu.CompilerParams(
            collective_id=1, has_side_effects=True, vmem_limit_bytes=48 * 2**20
        ),
    )(*[
        pltpu.with_memory_space_constraint(a, pltpu.HBM)
        for a in (tokens, cotangent, norm_gain.reshape(1, d_model), w_gate, w_up, w_down)
    ])
    grad, down, norms = pl.pallas_call(
        put_out,
        out_shape=[jax.ShapeDtypeStruct(a.shape, a.dtype) for a in (grad, down, norms)],
        in_specs=[pl.BlockSpec(memory_space=pl.ANY)] * 3,
        out_specs=[outside] * 3,
        scratch_shapes=[dma((3,))],
        compiler_params=pltpu.CompilerParams(vmem_limit_bytes=2**20),
    )(grad, down, norms)
    return grad, down, norms.reshape(2 * half)


def shards(n_fs, n_tp, tokens, norm_gain, w_gate, w_up, w_down, cotangent):
    n_y = 2 ** ((n_fs.bit_length() - 1) // 2)
    n_z, n_x = n_fs // n_y, n_tp // 2
    n_q = n_z // 2
    f, t = lax.axis_index("fs"), lax.axis_index("tp")
    z, y, x, c = f // n_y, f % n_y, t // 2, t % 2
    q, h = z // 2, z % 2
    rows, d_model = tokens.shape
    depth, half = w_gate.shape[0], w_gate.shape[1] // 2
    piece = rows // n_tp

    if piece % 16 == 0 and depth % 128 == 0 and half % 128 == 0:
        return fused(n_z, n_y, n_x, tokens, norm_gain, w_gate, w_up, w_down, cotangent)

    def to_z(a, step):
        return lax.ppermute(a, "fs", [(i, (i + step * n_y) % n_fs) for i in range(n_fs)])

    def to_y(a, step):
        return lax.ppermute(
            a, "fs", [(i, i // n_y * n_y + (i + step) % n_y) for i in range(n_fs)]
        )

    def to_twin(a):
        return lax.ppermute(
            a, "fs", [(i, (i // n_y ^ 1) * n_y + i % n_y) for i in range(n_fs)]
        )

    def to_x(a, step):
        return lax.ppermute(a, "tp", [(i, (i + 2 * step) % n_tp) for i in range(n_tp)])

    def to_core(a):
        return lax.ppermute(a, "tp", [(i, i ^ 1) for i in range(n_tp)])

    mine = jnp.stack(
        [lax.dynamic_slice_in_dim(a, t * piece, piece, 0) for a in (tokens, cotangent)]
    )
    down_t = w_down.T

    def half_of(which):
        gate_up = jnp.concatenate(
            [lax.dynamic_slice_in_dim(w, which * half, half, 1) for w in (w_gate, w_up)], axis=1
        )
        return gate_up, lax.dynamic_slice_in_dim(down_t, which * half, half, 1)

    own, other = half_of(h), half_of(1 - h)

    w_gu, w_dn, got = gather_all(n_z, n_y, n_x, own, other, mine)
    w_gu, w_dn = w_gu.reshape(d_model, 2 * half), w_dn.reshape(d_model, half)
    got = got.reshape(2, rows, d_model)
    tokens2 = jnp.concatenate([tokens, got[0]], axis=0)
    cot2 = jnp.concatenate([cotangent, got[1]], axis=0)

    xf = tokens2.astype(F32)
    inv = lax.rsqrt(jnp.mean(xf * xf, axis=-1, keepdims=True) + EPS)
    normed = (xf * inv * norm_gain).astype(BF16)
    gate_up = jnp.dot(normed, w_gu, preferred_element_type=F32)
    gate, up = gate_up[:, :half], gate_up[:, half:]
    sig = jax.nn.sigmoid(gate)
    act = gate * sig
    hidden = (act * up).astype(BF16)

    share = 0.5 * lax.dot_general(
        cot2, hidden, (((0,), (0,)), ((), ())), preferred_element_type=F32
    )
    share = share.reshape(n_q, 2, n_y, depth, half)
    share, w_dn = lax.optimization_barrier((share, w_dn))

    def sent_over_y(pair):
        block = take(share, pair)
        return [to_y(take(block, (y + s) % n_y, 1).astype(BF16), s) for s in range(1, n_y)]

    def over_y(pair, came):
        return sum([a.astype(F32) for a in came], take(take(share, pair), y, 1))

    first = [sent_over_y((q + s) % n_q) for s in range(1, n_q)]

    d_hidden = 0.5 * jnp.dot(cot2, w_dn, preferred_element_type=F32)
    d_gate = (d_hidden * up * sig * (1.0 + gate * (1.0 - sig))).astype(BF16)
    d_up = (d_hidden * act).astype(BF16)
    d_both = jnp.concatenate([d_gate, d_up], axis=1)
    part = lax.dot_general(
        d_both, w_gu, (((1,), (1,)), ((), ())), preferred_element_type=F32
    )
    part, first = lax.optimization_barrier((part.astype(BF16), first))

    away = [
        to_z(over_y((q + s) % n_q, first[s - 1]).astype(BF16), 2 * s) for s in range(1, n_q)
    ]
    total = over_y(q, sent_over_y(q))
    total = sum([a.astype(F32) for a in away], total)
    kept = take(total, h)
    came = to_twin(take(total, 1 - h).astype(BF16)).astype(F32)
    grad_down = place([(h, kept.T), (1 - h, came.T)], 2).reshape(2 * half, depth)
    norms = jnp.sum(grad_down * grad_down, axis=1)
    norms = sum([to_y(norms, s) for s in range(1, n_y)], norms)
    down_norms = sum([to_z(norms, s) for s in range(1, n_z)], norms)

    part = part.reshape(2, n_x, 2, piece, d_model)
    part = take(part, c, 2).astype(F32) + to_core(take(part, 1 - c, 2)).astype(F32)
    total = take(part, x, 1)
    for s in range(1, n_x):
        total = total + to_x(take(part, (x + s) % n_x, 1).astype(BF16), s).astype(F32)
    d_normed = total[0] + to_twin(total[1].astype(BF16)).astype(F32)

    xp = lax.dynamic_slice_in_dim(tokens, t * piece, piece, 0).astype(F32)
    inv_p = lax.rsqrt(jnp.mean(xp * xp, axis=-1, keepdims=True) + EPS)
    scaled = xp * inv_p
    d_scaled = d_normed * norm_gain
    inner = jnp.mean(d_scaled * scaled, axis=-1, keepdims=True)
    grad = (inv_p * (d_scaled - scaled * inner)).astype(BF16)
    grad = place([(x, grad)] + [((x - s) % n_x, to_x(grad, s)) for s in range(1, n_x)], n_x)
    grad = place([(c, grad), (1 - c, to_core(grad))], 2)
    grad_tokens = grad.transpose(1, 0, 2, 3).reshape(rows, d_model)
    return (grad_tokens, grad_down, down_norms)


def solution(mesh):
    in_specs = (P("fs", None), P(), P("fs", "tp"), P("fs", "tp"), P("tp", "fs"), P("fs", None))
    out_specs = (P("fs", None), P("tp", "fs"), P("tp"))
    return jax.shard_map(
        functools.partial(shards, mesh.shape["fs"], mesh.shape["tp"]),
        mesh=mesh, in_specs=in_specs, out_specs=out_specs, check_vma=False,
    )
```

```python
import functools

import jax
import jax.numpy as jnp
from jax import lax
from jax.experimental import pallas as pl
from jax.experimental.pallas import tpu as pltpu
from jax.sharding import PartitionSpec as P

EPS = 1e-06
BF16 = jnp.bfloat16
F32 = jnp.float32


def place(pieces, count):
    first = pieces[0][1]
    held = jnp.zeros((count,) + first.shape, first.dtype)
    for position, piece in pieces:
        held = lax.dynamic_update_slice_in_dim(held, piece[None], position, 0)
    return held


def take(array, position, axis=0):
    return lax.dynamic_index_in_dim(array, position, axis, keepdims=False)


def gather_kernel(n_z, n_y, n_x, own_gu, own_dn, other_gu, other_dn, mine, w_gu, w_dn, got,
                  z_send, z_recv, y_send, y_recv, x_send, x_recv, c_send, c_recv, local):
    f, t = lax.axis_index("fs"), lax.axis_index("tp")
    z, y, x, c = lax.div(f, n_y), lax.rem(f, n_y), lax.div(t, 2), lax.rem(t, 2)
    n_tp = 2 * n_x
    sources = ((own_gu, other_gu), (own_dn, other_dn))
    held = (w_gu, w_dn)

    def at_z(s):
        return {"fs": lax.rem(z + s, n_z) * n_y + y}

    def at_y(r):
        return {"fs": z * n_y + lax.rem(y + r, n_y)}

    def at_x(s):
        return {"tp": lax.rem(t + 2 * s, n_tp)}

    twin = {"fs": (z + 1 - 2 * lax.rem(z, 2)) * n_y + y}
    core = {"tp": t + 1 - 2 * c}

    barrier = pltpu.get_barrier_semaphore()
    friends = [at_z(s) for s in range(1, n_z)] + [at_y(r) for r in range(1, n_y)]
    friends += [at_x(s) for s in range(1, n_x)] + [core]
    for friend in friends:
        pl.semaphore_signal(barrier, inc=1, device_id=friend, device_id_type=pl.DeviceIdType.MESH)
    pl.semaphore_wait(barrier, len(friends))

    started = []

    def send(src, dst, out_sem, in_sem, to):
        copy = pltpu.make_async_remote_copy(
            src_ref=src, dst_ref=dst, send_sem=out_sem, recv_sem=in_sem,
            device_id=to, device_id_type=pl.DeviceIdType.MESH,
        )
        copy.start()
        started.append(copy)
        return copy

    order = sorted(range(1, n_z), key=lambda s: min(s, n_z - s))
    from_z = {}

    def start_z(k):
        for s in order:
            from_z[k, s] = send(
                sources[k][s % 2], held[k].at[f], z_send.at[k, s], z_recv.at[k, s], at_z(s)
            )

    late = []

    def forward(k, s):
        if s == 0:
            src = sources[k][0]
            slot = f
        else:
            from_z[k, s].wait_recv()
            slot = lax.rem(z + n_z - s, n_z) * n_y + y
            src = held[k].at[slot]
        for r in range(1, n_y):
            late.append(send(
                src, held[k].at[slot], y_send.at[k, s, r], y_recv.at[k, s, r], at_y(r)
            ))

    start_z(0)
    forward(0, 0)
    tokens = send(mine, got.at[:, x, c], x_send.at[0], x_recv.at[0], twin)
    start_z(1)
    forward(1, 0)
    stays = [pltpu.make_async_copy(sources[k][0], held[k].at[f], local.at[k]) for k in range(2)]
    for copy in stays:
        copy.start()
    for s in order:
        forward(0, s)
    tokens.wait_recv()
    across = [
        send(got.at[:, x, c], got.at[:, x, c], x_send.at[s], x_recv.at[s], at_x(s))
        for s in range(1, n_x)
    ]
    for s in order[:-1]:
        forward(1, s)
    for copy in across:
        copy.wait_recv()
    late.append(send(got.at[:, :, c], got.at[:, :, c], c_send, c_recv, core))
    forward(1, order[-1])
    for copy in late:
        copy.wait_recv()
    for copy in started:
        copy.wait_send()
    for copy in stays:
        copy.wait()


def gather_all(n_z, n_y, n_x, own, other, mine):
    n_fs = n_z * n_y
    dma = pltpu.SemaphoreType.DMA
    anywhere = pl.BlockSpec(memory_space=pl.ANY)
    return pl.pallas_call(
        functools.partial(gather_kernel, n_z, n_y, n_x),
        out_shape=[jax.ShapeDtypeStruct((n_fs,) + a.shape, a.dtype) for a in own]
        + [jax.ShapeDtypeStruct((2, n_x, 2) + mine.shape[1:], mine.dtype)],
        in_specs=[anywhere] * 5,
        out_specs=[anywhere] * 3,
        scratch_shapes=[
            dma((2, n_z)), dma((2, n_z)), dma((2, n_z, n_y)), dma((2, n_z, n_y)),
            dma((n_x,)), dma((n_x,)), dma, dma, dma((2,)),
        ],
        compiler_params=pltpu.CompilerParams(collective_id=0, has_side_effects=True),
    )(*own, *other, mine)


def tile_of(extent, most):
    return max(n for n in range(16, most + 1, 16) if extent % n == 0)


def dot(a, b, contract):
    return lax.dot_general(a, b, (contract, ((), ())), preferred_element_type=F32)


def rows_at(start, count):
    return pl.ds(pl.multiple_of(start, 16), count)


def cols_at(start, count):
    return pl.ds(pl.multiple_of(start, 128), count)


def fused_kernel(n_z, n_y, n_x, tokens, cotangent, gain_in, w_gate, w_up, w_down,
                 o_grad, o_down, o_norms,
                 gain, tok, cot, normed, wg, wu, wd, wg_t, wu_t, gate, up, d_hid, hid_t, d_gate, d_up,
                 own_share, y_out, y_in, q_out, q_in, t_out, t_in, n_all,
                 part, c_out, c_in, m_out, m_in, x_out, x_in,
                 sent, z_recv, f_recv, tt_recv, tx_recv, tc_recv, y_recv, q_recv, t_recv, n_recv,
                 c_recv, m_recv, x_recv, a_recv, g_recv, local):
    f, t = lax.axis_index("fs"), lax.axis_index("tp")
    z, y, x, c = lax.div(f, n_y), lax.rem(f, n_y), lax.div(t, 2), lax.rem(t, 2)
    q, h = lax.div(z, 2), lax.rem(z, 2)
    n_tp, n_q = 2 * n_x, n_z // 2
    rows, d_model = tokens.shape
    depth, half = wg.shape[1], wg.shape[2]
    piece = rows // n_tp
    chunks, subs = c_out.shape[1], m_out.shape[0]
    side = rows // 2
    chunk = side // chunks

    def at_z(s):
        return {"fs": lax.rem(z + s, n_z) * n_y + y}

    def at_y(r):
        return {"fs": z * n_y + lax.rem(y + r, n_y)}

    def at_x(s):
        return {"tp": lax.rem(t + 2 * s, n_tp)}

    twin = {"fs": (z + 1 - 2 * h) * n_y + y}
    core = {"tp": t + 1 - 2 * c}

    started = [], []

    def copy_to(src, dst, in_sem, to, phase=0):
        copy = pltpu.make_async_remote_copy(
            src_ref=src, dst_ref=dst, send_sem=sent.at[phase], recv_sem=in_sem,
            device_id=to, device_id_type=pl.DeviceIdType.MESH,
        )
        started[phase].append(copy)
        return copy

    def send(*args):
        copy = copy_to(*args)
        copy.start()
        return copy

    def bring(src, dst, sem):
        copy = pltpu.make_async_copy(src, dst, sem)
        copy.start()
        return copy

    kinds = z_recv.shape[0]
    downs_of = range(2, kinds)
    step_rows = half // len(downs_of)

    def source(k, which):
        if k >= 2:
            return w_down.at[rows_at(which * half + (k - 2) * step_rows, step_rows), :]
        return (w_gate, w_up)[k].at[:, cols_at(which * half, half)]

    def held(k, at_slot):
        if k >= 2:
            return wd.at[at_slot, pl.ds((k - 2) * step_rows, step_rows)]
        return (wg, wu)[k].at[at_slot]

    barrier = pltpu.get_barrier_semaphore()
    n_fs = n_z * n_y
    friends = [{"fs": lax.rem(f + s, n_fs)} for s in range(1, n_fs)]
    friends += [at_x(s) for s in range(1, n_x)] + [core]
    for friend in friends:
        pl.semaphore_signal(barrier, inc=1, device_id=friend, device_id_type=pl.DeviceIdType.MESH)
    bring_gain = bring(gain_in, gain, local.at[2 + z_recv.shape[0]])
    bring_tok = bring(tokens, tok.at[pl.ds(0, rows)], local.at[0])
    bring_cot = bring(cotangent, cot.at[pl.ds(0, rows)], local.at[1])
    stays = [bring(source(k, h), held(k, f), local.at[2 + k]) for k in range(kinds)]

    pl.semaphore_wait(barrier, len(friends))

    over_y = {}
    others = [[b for b in range(n_z) if b != a] for a in range(n_z)]
    ends = (0, n_z - 1)
    nearest = [sorted(others[a], key=lambda b: abs(a - b)) for a in range(n_z)]
    arrival = [
        [a] + sorted(others[a], key=lambda b: 1 if b == a ^ 1 else 2 * (b not in ends)) for a in range(n_z)
    ]

    def pick(table, p):
        return sum(jnp.where(z == a, table[a][p], 0) for a in range(n_z))

    near = [z] + [pick(arrival, p) for p in range(1, n_z)]

    def start_z(k, p):
        to = pick(nearest, p)
        send(
            source(k, lax.rem(to, 2)), held(k, f), z_recv.at[k, z],
            {"fs": to * n_y + y},
        )

    def slot(p, r):
        return near[p] * n_y + lax.rem(y + n_y - r, n_y)

    def forwarding(k, p):
        if p == 0:
            src, came = source(k, h), None
        else:
            src = held(k, slot(p, 0))
            came = pltpu.make_async_remote_copy(
                src_ref=src, dst_ref=src, send_sem=sent.at[0], recv_sem=z_recv.at[k, near[p]],
                device_id={"fs": near[p] * n_y + y}, device_id_type=pl.DeviceIdType.MESH,
            )
        for r in range(1, n_y):
            over_y[k, p, r] = copy_to(src, held(k, slot(p, 0)), f_recv.at[k, near[p], r - 1], at_y(r))

        def go():
            if came is not None:
                came.wait_recv()
            for r in range(1, n_y):
                over_y[k, p, r].start()

        return go

    def forward(k, p):
        forwarding(k, p)()

    raw, both = (tokens, cotangent), (tok, cot)

    cuts = tt_recv.shape[1]
    cut = piece // cuts

    def cut_of(start, i):
        return rows_at(start + i * cut, cut)

    def swap(a):
        return [
            send(raw[a].at[cut_of(t * piece, i)], both[a].at[cut_of(rows + t * piece, i)],
                 tt_recv.at[a, i], twin)
            for i in range(cuts)
        ]

    def across(a, parts):
        copies = []
        for i in parts:
            swapped[a][i].wait_recv()
            at = both[a].at[cut_of(rows + t * piece, i)]
            copies += [send(at, at, tx_recv.at[a, i, s - 1], at_x(s)) for s in range(1, n_x)]
        return copies

    def meet(a):
        copies = []
        for k in range(n_x):
            at = rows_at(rows + (2 * k + c) * piece, piece)
            copies.append(send(both[a].at[at], both[a].at[at], tc_recv.at[a, k], core))
        return copies

    def arrive(copies):
        for copy in copies:
            copy.wait_recv()

    swapped = []
    for p in reversed(range(n_z - 1)):
        start_z(0, p)
        start_z(1, p)
        if p == n_z - 2:
            forward(0, 0)
            forward(1, 0)
            for k in downs_of:
                forward(k, 0)
    for a in range(2):
        swapped.append(swap(a))
    for p in range(n_z - 1):
        for k in downs_of:
            start_z(k, p)

    norm_tile = tile_of(rows, 32)

    def normalize(first):
        @pl.loop(0, rows // norm_tile)
        def _(i):
            at = rows_at(first + i * norm_tile, norm_tile)
            xf = tok[at, :].astype(F32)
            inv = lax.rsqrt(jnp.mean(xf * xf, axis=-1, keepdims=True) + EPS)
            normed[at, :] = (xf * inv * gain[...]).astype(BF16)

    bring_gain.wait()
    bring_tok.wait()
    normalize(0)

    m_tile = tile_of(2 * rows, 768)

    def add_gate_up(p, r, group):
        at_slot = slot(p, r)
        if group == 0:
            if p == 0 and r == 0:
                stays[0].wait()
                stays[1].wait()
            elif r > 0:
                over_y[0, p, r].wait_recv()
                over_y[1, p, r].wait_recv()
            wg_t[at_slot] = wg[at_slot].T
            wu_t[at_slot] = wu[at_slot].T
        at = pl.ds(group * rows, rows)
        a = normed[at, cols_at(at_slot * depth, depth)]
        for total, w in ((gate, wg), (up, wu)):
            term = dot(a, w[at_slot], ((1,), (0,)))
            total[at, :] = term if p == 0 and r == 0 else total[at, :] + term

    def add_d_hidden(s, r):
        if s == 0 and r == 0:
            for k in downs_of:
                stays[k].wait()
        elif r > 0:
            for k in downs_of:
                over_y[k, s, r].wait_recv()
        at_slot = slot(s, r)

        @pl.loop(0, 2 * rows // m_tile)
        def _(i):
            at = rows_at(i * m_tile, m_tile)
            term = dot(cot[at, cols_at(at_slot * depth, depth)], wd[at_slot], ((1,), (1,)))
            d_hid[at, :] = term if s == 0 and r == 0 else d_hid[at, :] + term

    add_gate_up(0, 0, 0)
    token_copies = []
    for p in range(1, n_z):
        forward(0, p)
        if p == n_z - 1:
            token_copies += across(0, range(cuts - 1))
        forward(1, p)
        if p == n_z - 1:
            token_copies += across(0, range(cuts - 1, cuts))
        for r in range(1, n_y):
            add_gate_up(p - 1, r, 0)
        add_gate_up(p, 0, 0)
    backward = range(n_z - 1, 0, -1)
    downs = [[forwarding(k, p) for k in downs_of] for p in backward]
    at_end = (z == 0) | (z == n_z - 1)

    at_middle = jnp.logical_not(at_end)

    def down(middle, end, first=0, count=len(downs_of)):
        for which, index in ((at_middle, middle), (at_end, end)):
            if index is not None and index < len(downs):
                @pl.when(which)
                def _():
                    for go in downs[index][first:first + count]:
                        go()

    down(0, None)
    cot_copies = across(1, range(cuts))
    arrive(token_copies)
    met = meet(0)
    down(1, None)
    arrive(met)
    normalize(rows)
    down(None, 0)
    for p in range(n_z):
        for r in range(n_y):
            if p == n_z - 1 and r > 0:
                add_gate_up(p, r, 0)
            add_gate_up(p, r, 1)
        if p == n_z // 2:
            down(None, 1, 0, 1)
    down(2, None)
    down(None, 1, 1)

    e_tile = tile_of(2 * rows, 128)

    @pl.loop(0, 2 * rows // e_tile)
    def _(i):
        at = rows_at(i * e_tile, e_tile)
        g, u = gate[at, :], up[at, :]
        sig = jax.nn.sigmoid(g)
        act = g * sig
        hid_t[:, cols_at(i * e_tile, e_tile)] = (act * u).T.astype(BF16)
        gate[at, :] = 0.5 * (u * sig * (1.0 + g * (1.0 - sig)))
        up[at, :] = 0.5 * act

    arrive(cot_copies)
    bring_cot.wait()
    arrive(meet(1))
    s_tile = tile_of(half, 512)

    def share(block, put):
        @pl.loop(0, half // s_tile)
        def _(i):
            at = rows_at(i * s_tile, s_tile)
            put(at, 0.5 * dot(hid_t[at, :], cot[:, cols_at(block * depth, depth)], ((1,), (0,))))

    def block_of(step, rel, r):
        column = 2 * lax.rem(q + step, n_q) + (h if rel == 0 else 1 - h)
        return column * n_y + lax.rem(y + r, n_y)

    y_copies = {}

    def send_share(step, rel):
        for r in range(1, n_y):
            out = y_out.at[step, rel, r]

            def put(at, value):
                out[at, :] = value.astype(BF16)

            share(block_of(step, rel, r), put)
            y_copies[step, rel, r] = send(
                out, y_in.at[step, rel, r], y_recv.at[step, rel, r - 1], at_y(r)
            )

    def own_block(step, rel):
        out = own_share.at[step, rel]

        def put(at, value):
            out[at, :] = value

        share(block_of(step, rel, 0), put)

    q_copies = {
        (step, rel): copy_to(q_out.at[step, rel], q_in.at[step, rel], q_recv.at[step, rel], at_z(2 * step))
        for step in range(1, n_q) for rel in range(2)
    }

    def cross(rel):
        for step in range(1, n_q):
            for r in range(1, n_y):
                y_copies[step, rel, r].wait_recv()
            total = own_share[step, rel]
            for r in range(1, n_y):
                total = total + y_in[step, rel, r].astype(F32)
            q_out[step, rel] = total.astype(BF16)
            q_copies[step, rel].start()

    down(None, 2)
    for step in range(1, n_q):
        send_share(step, 1)
    for index in range(3, len(downs)):
        down(index, index)
    for step in range(1, n_q):
        send_share(step, 0)
    for rel in (1, 0):
        send_share(0, rel)
    for step in range(1, n_q):
        for rel in (1, 0):
            own_block(step, rel)
    add_d_hidden(0, 0)
    for r in range(1, n_y):
        add_d_hidden(0, r)
    for p in backward:
        add_d_hidden(p, 0)
        for r in range(1, n_y):
            add_d_hidden(p, r)

    d_tile = tile_of(piece, 128)

    @pl.loop(0, 2 * rows // d_tile)
    def _(i):
        at = rows_at(i * d_tile, d_tile)
        index = lax.div(i * d_tile, piece)
        group, index = lax.div(index, n_tp), lax.rem(index, n_tp)
        turn = lax.rem(lax.rem(index, n_x) + 2 * n_x - 1 - x, n_x)
        mine = lax.rem(lax.div(index, n_x) + c + 1, 2)
        to = group * rows + (2 * turn + mine) * piece + lax.rem(i * d_tile, piece)
        d = d_hid[at, :]
        d_gate[rows_at(to, d_tile), :] = (d * gate[at, :]).astype(BF16)
        d_up[rows_at(to, d_tile), :] = (d * up[at, :]).astype(BF16)

    c_copies = {}

    def owner_of(s):
        return lax.rem(x + s, n_x) * subs

    def partial(group, s):
        first = group * rows + (s - 1 if s else n_x - 1) * 2 * piece
        owner = owner_of(s)

        @pl.loop(0, n_z * n_y, unroll=4)
        def _(k):
            at, to = pl.ds(first, 2 * piece), cols_at(k * depth, depth)
            value = dot(d_gate[at, :], wg_t[k], ((1,), (0,))) + dot(d_up[at, :], wu_t[k], ((1,), (0,)))
            for u in range(subs):
                c_out[group, owner + u, :, to] = value[u * chunk:(u + 1) * chunk].astype(BF16)
                part[group, owner + u, :, to] = value[piece + u * chunk:piece + (u + 1) * chunk]

        for u in range(subs):
            j = owner + u
            c_copies[group, s, u] = send(
                c_out.at[group, j], c_in.at[group, j], c_recv.at[group, j], core
            )

    l_tile = tile_of(chunk, 32)

    def each(body):
        @pl.loop(0, chunk // l_tile)
        def _(i):
            body(rows_at(i * l_tile, l_tile))

    x_copies, m_copies = {}, {}

    def summed(group, j, at):
        return part[group, j, at, :] + c_in[group, j, at, :].astype(F32)

    def to_x(group):
        for u in range(subs):
            for s in range(1, n_x):
                c_copies[group, s, u].wait_recv()
                j = owner_of(s) + u

                def fold(at):
                    x_out[group, s, u, at, :] = summed(group, j, at).astype(BF16)

                each(fold)
                x_copies[group, s, u] = send(
                    x_out.at[group, s, u], x_in.at[group, s, u], x_recv.at[group, s - 1, u], at_x(s)
                )

    def total_of(group, u, at):
        total = summed(group, owner_of(0) + u, at)
        for s in range(1, n_x):
            total = total + x_in[group, s, u, at, :].astype(F32)
        return total

    for s in range(1, n_x):
        partial(1, s)
    pl.when(at_middle)(functools.partial(cross, 1))
    to_x(1)
    pl.when(at_end)(functools.partial(cross, 1))
    partial(1, 0)
    for s in range(1, n_x):
        partial(0, s)
    to_x(0)
    pl.when(at_middle)(functools.partial(cross, 0))
    partial(0, 0)
    for rel in (1, 0):
        own_block(0, rel)
    for u in range(subs):
        c_copies[1, 0, u].wait_recv()
        for s in range(1, n_x):
            x_copies[1, s, u].wait_recv()

        def fold(at):
            m_out[u, at, :] = total_of(1, u, at).astype(BF16)

        each(fold)
        m_copies[u] = send(m_out.at[u], m_in.at[u], m_recv.at[u], twin)
    pl.when(at_end)(functools.partial(cross, 0))
    for u in range(subs):
        c_copies[0, 0, u].wait_recv()
    shared, gathered = [], {}

    def place_of(at_x_index, u):
        return o_grad.at[rows_at((c * n_x + at_x_index) * piece + u * chunk, chunk)]

    def finish(u):
        for s in range(1, n_x):
            x_copies[0, s, u].wait_recv()
        m_copies[u].wait_recv()
        first = (c * n_x + x) * piece + u * chunk

        @pl.loop(0, chunk // l_tile)
        def _(i):
            at = rows_at(i * l_tile, l_tile)
            to = rows_at(first + i * l_tile, l_tile)
            xf = tok[to, :].astype(F32)
            inv = lax.rsqrt(jnp.mean(xf * xf, axis=-1, keepdims=True) + EPS)
            scaled = xf * inv
            d_normed = total_of(0, u, at) + m_in[u, at, :].astype(F32)
            d_scaled = d_normed * gain[...]
            inner = jnp.mean(d_scaled * scaled, axis=-1, keepdims=True)
            o_grad[to, :] = (inv * (d_scaled - scaled * inner)).astype(BF16)

        out = place_of(x, u)
        for s in range(1, n_x):
            gathered[u, s] = send(out, out, a_recv.at[u, s - 1], at_x(s), 1)
        shared.append(send(out, out, g_recv.at[u, 0], core, 1))

    def relay(u):
        for s in range(1, n_x):
            gathered[u, s].wait_recv()
            out = place_of(lax.rem(x + n_x - s, n_x), u)
            shared.append(send(out, out, g_recv.at[u, s], core, 1))

    def collect(rel, put):
        for r in range(1, n_y):
            y_copies[0, rel, r].wait_recv()
        for step in range(1, n_q):
            q_copies[step, rel].wait_recv()
        total = own_share[0, rel]
        for r in range(1, n_y):
            total = total + y_in[0, rel, r].astype(F32)
        for step in range(1, n_q):
            total = total + q_in[step, rel].astype(F32)
        put(0, pl.ds(0, half), total)

    n_tile = tile_of(half, 128)

    def squares(value):
        folded = sum(value[:, k * 128:(k + 1) * 128] * value[:, k * 128:(k + 1) * 128] for k in range(depth // 128))
        return jnp.concatenate(
            [jnp.sum(folded[i:i + n_tile].T, axis=0, keepdims=True) for i in range(0, half, n_tile)], axis=1
        )

    def put_twin(start, at, value):
        t_out[at, :] = value.astype(BF16)
        n_all[f] = squares(value)

    def put_kept(start, at, value):
        o_down[rows_at(h * half + start, half), :] = value
        n_all[f] = n_all[f] + squares(value)

    collect(1, put_twin)
    traded = copy_to(t_out, t_in, t_recv, twin, 1)
    pl.when(at_middle)(traded.start)
    for u in range(subs):
        finish(u)
    collect(0, put_kept)
    exchange = [
        send(n_all.at[f], n_all.at[f], n_recv.at[s - 1], {"fs": lax.rem(f + s, n_fs)}, 1)
        for s in range(1, n_fs)
    ]
    pl.when(at_end)(traded.start)
    for copy in started[0]:
        copy.wait_send()
    for u in range(subs):
        relay(u)
    for copy in exchange:
        copy.wait_recv()
    for side_of in range(2):
        total = sum(n_all[k] for k in range(n_fs) if k // n_y % 2 == side_of)
        o_norms[:, side_of * half:(side_of + 1) * half] = total
    for copy in started[1]:
        copy.wait_send()
    traded.wait_recv()
    o_down[rows_at((1 - h) * half, half), :] = t_in[...].astype(F32)
    for copy in shared:
        copy.wait_recv()


def put_out(grad, down, norms, o_grad, o_down, o_norms, done):
    copies = [
        pltpu.make_async_copy(src, dst, done.at[i])
        for i, (src, dst) in enumerate(((grad, o_grad), (down, o_down), (norms, o_norms)))
    ]
    for copy in copies:
        copy.start()
    for copy in copies:
        copy.wait()


def fused(n_z, n_y, n_x, tokens, norm_gain, w_gate, w_up, w_down, cotangent):
    n_fs, n_tp, n_q = n_z * n_y, 2 * n_x, n_z // 2
    rows, d_model = tokens.shape
    depth, half = w_gate.shape[0], w_gate.shape[1] // 2
    piece = rows // n_tp
    cuts = 2 if piece % 32 == 0 else 1
    kinds = 2 + 4
    subs = max(n for n in (1, 2, 3) if piece % (16 * n) == 0)
    chunks = n_x * subs
    chunk = rows // 2 // chunks
    dma, vmem = pltpu.SemaphoreType.DMA, pltpu.VMEM
    outside = pl.BlockSpec(memory_space=pltpu.HBM)
    inside = pl.BlockSpec(memory_space=pltpu.VMEM)
    block = (half, depth)
    scratch = [
        vmem((1, d_model), F32),
        vmem((2 * rows, d_model), BF16), vmem((2 * rows, d_model), BF16), vmem((2 * rows, d_model), BF16),
        vmem((n_fs, depth, half), BF16), vmem((n_fs, depth, half), BF16), vmem((n_fs, half, depth), BF16),
        vmem((n_fs, half, depth), BF16), vmem((n_fs, half, depth), BF16),
        vmem((2 * rows, half), F32), vmem((2 * rows, half), F32), vmem((2 * rows, half), F32),
        vmem((half, 2 * rows), BF16), vmem((2 * rows, half), BF16), vmem((2 * rows, half), BF16),
        vmem((n_q, 2) + block, F32), vmem((n_q, 2, n_y) + block, BF16), vmem((n_q, 2, n_y) + block, BF16),
        vmem((n_q, 2) + block, BF16), vmem((n_q, 2) + block, BF16), vmem(block, BF16), vmem(block, BF16),
        vmem((n_fs, 1, half), F32),
        vmem((2, chunks, chunk, d_model), F32),
        vmem((2, chunks, chunk, d_model), BF16), vmem((2, chunks, chunk, d_model), BF16),
        vmem((subs, chunk, d_model), BF16), vmem((subs, chunk, d_model), BF16),
        vmem((2, n_x, subs, chunk, d_model), BF16), vmem((2, n_x, subs, chunk, d_model), BF16),
        dma((2,)), dma((kinds, n_z)), dma((kinds, n_z, n_y - 1)),
        dma((2, cuts)), dma((2, cuts, n_x - 1)), dma((2, n_x)),
        dma((n_q, 2, n_y - 1)), dma((n_q, 2)), dma, dma((n_fs - 1,)),
        dma((2, chunks)), dma((subs,)), dma((2, n_x - 1, subs)), dma((subs, n_x - 1)),
        dma((subs, n_x)), dma((kinds + 3,)),
    ]
    grad, down, norms = pl.pallas_call(
        functools.partial(fused_kernel, n_z, n_y, n_x),
        out_shape=[
            jax.ShapeDtypeStruct((rows, d_model), BF16),
            jax.ShapeDtypeStruct((2 * half, depth), F32),
            jax.ShapeDtypeStruct((1, 2 * half), F32),
        ],
        in_specs=[outside] * 6,
        out_specs=[inside, inside, inside],
        scratch_shapes=scratch,
        compiler_params=pltpu.CompilerParams(
            collective_id=1, has_side_effects=True, vmem_limit_bytes=48 * 2**20
        ),
    )(*[
        pltpu.with_memory_space_constraint(a, pltpu.HBM)
        for a in (tokens, cotangent, norm_gain.reshape(1, d_model), w_gate, w_up, w_down)
    ])
    grad, down, norms = pl.pallas_call(
        put_out,
        out_shape=[jax.ShapeDtypeStruct(a.shape, a.dtype) for a in (grad, down, norms)],
        in_specs=[pl.BlockSpec(memory_space=pl.ANY)] * 3,
        out_specs=[outside] * 3,
        scratch_shapes=[dma((3,))],
        compiler_params=pltpu.CompilerParams(vmem_limit_bytes=2**20),
    )(grad, down, norms)
    return grad, down, norms.reshape(2 * half)


def shards(n_fs, n_tp, tokens, norm_gain, w_gate, w_up, w_down, cotangent):
    n_y = 2 ** ((n_fs.bit_length() - 1) // 2)
    n_z, n_x = n_fs // n_y, n_tp // 2
    n_q = n_z // 2
    f, t = lax.axis_index("fs"), lax.axis_index("tp")
    z, y, x, c = f // n_y, f % n_y, t // 2, t % 2
    q, h = z // 2, z % 2
    rows, d_model = tokens.shape
    depth, half = w_gate.shape[0], w_gate.shape[1] // 2
    piece = rows // n_tp

    if piece % 16 == 0 and depth % 128 == 0 and half % 128 == 0:
        return fused(n_z, n_y, n_x, tokens, norm_gain, w_gate, w_up, w_down, cotangent)

    def to_z(a, step):
        return lax.ppermute(a, "fs", [(i, (i + step * n_y) % n_fs) for i in range(n_fs)])

    def to_y(a, step):
        return lax.ppermute(
            a, "fs", [(i, i // n_y * n_y + (i + step) % n_y) for i in range(n_fs)]
        )

    def to_twin(a):
        return lax.ppermute(
            a, "fs", [(i, (i // n_y ^ 1) * n_y + i % n_y) for i in range(n_fs)]
        )

    def to_x(a, step):
        return lax.ppermute(a, "tp", [(i, (i + 2 * step) % n_tp) for i in range(n_tp)])

    def to_core(a):
        return lax.ppermute(a, "tp", [(i, i ^ 1) for i in range(n_tp)])

    mine = jnp.stack(
        [lax.dynamic_slice_in_dim(a, t * piece, piece, 0) for a in (tokens, cotangent)]
    )
    down_t = w_down.T

    def half_of(which):
        gate_up = jnp.concatenate(
            [lax.dynamic_slice_in_dim(w, which * half, half, 1) for w in (w_gate, w_up)], axis=1
        )
        return gate_up, lax.dynamic_slice_in_dim(down_t, which * half, half, 1)

    own, other = half_of(h), half_of(1 - h)

    w_gu, w_dn, got = gather_all(n_z, n_y, n_x, own, other, mine)
    w_gu, w_dn = w_gu.reshape(d_model, 2 * half), w_dn.reshape(d_model, half)
    got = got.reshape(2, rows, d_model)
    tokens2 = jnp.concatenate([tokens, got[0]], axis=0)
    cot2 = jnp.concatenate([cotangent, got[1]], axis=0)

    xf = tokens2.astype(F32)
    inv = lax.rsqrt(jnp.mean(xf * xf, axis=-1, keepdims=True) + EPS)
    normed = (xf * inv * norm_gain).astype(BF16)
    gate_up = jnp.dot(normed, w_gu, preferred_element_type=F32)
    gate, up = gate_up[:, :half], gate_up[:, half:]
    sig = jax.nn.sigmoid(gate)
    act = gate * sig
    hidden = (act * up).astype(BF16)

    share = 0.5 * lax.dot_general(
        cot2, hidden, (((0,), (0,)), ((), ())), preferred_element_type=F32
    )
    share = share.reshape(n_q, 2, n_y, depth, half)
    share, w_dn = lax.optimization_barrier((share, w_dn))

    def sent_over_y(pair):
        block = take(share, pair)
        return [to_y(take(block, (y + s) % n_y, 1).astype(BF16), s) for s in range(1, n_y)]

    def over_y(pair, came):
        return sum([a.astype(F32) for a in came], take(take(share, pair), y, 1))

    first = [sent_over_y((q + s) % n_q) for s in range(1, n_q)]

    d_hidden = 0.5 * jnp.dot(cot2, w_dn, preferred_element_type=F32)
    d_gate = (d_hidden * up * sig * (1.0 + gate * (1.0 - sig))).astype(BF16)
    d_up = (d_hidden * act).astype(BF16)
    d_both = jnp.concatenate([d_gate, d_up], axis=1)
    part = lax.dot_general(
        d_both, w_gu, (((1,), (1,)), ((), ())), preferred_element_type=F32
    )
    part, first = lax.optimization_barrier((part.astype(BF16), first))

    away = [
        to_z(over_y((q + s) % n_q, first[s - 1]).astype(BF16), 2 * s) for s in range(1, n_q)
    ]
    total = over_y(q, sent_over_y(q))
    total = sum([a.astype(F32) for a in away], total)
    kept = take(total, h)
    came = to_twin(take(total, 1 - h).astype(BF16)).astype(F32)
    grad_down = place([(h, kept.T), (1 - h, came.T)], 2).reshape(2 * half, depth)
    norms = jnp.sum(grad_down * grad_down, axis=1)
    norms = sum([to_y(norms, s) for s in range(1, n_y)], norms)
    down_norms = sum([to_z(norms, s) for s in range(1, n_z)], norms)

    part = part.reshape(2, n_x, 2, piece, d_model)
    part = take(part, c, 2).astype(F32) + to_core(take(part, 1 - c, 2)).astype(F32)
    total = take(part, x, 1)
    for s in range(1, n_x):
        total = total + to_x(take(part, (x + s) % n_x, 1).astype(BF16), s).astype(F32)
    d_normed = total[0] + to_twin(total[1].astype(BF16)).astype(F32)

    xp = lax.dynamic_slice_in_dim(tokens, t * piece, piece, 0).astype(F32)
    inv_p = lax.rsqrt(jnp.mean(xp * xp, axis=-1, keepdims=True) + EPS)
    scaled = xp * inv_p
    d_scaled = d_normed * norm_gain
    inner = jnp.mean(d_scaled * scaled, axis=-1, keepdims=True)
    grad = (inv_p * (d_scaled - scaled * inner)).astype(BF16)
    grad = place([(x, grad)] + [((x - s) % n_x, to_x(grad, s)) for s in range(1, n_x)], n_x)
    grad = place([(c, grad), (1 - c, to_core(grad))], 2)
    grad_tokens = grad.transpose(1, 0, 2, 3).reshape(rows, d_model)
    return (grad_tokens, grad_down, down_norms)


def solution(mesh):
    in_specs = (P("fs", None), P(), P("fs", "tp"), P("fs", "tp"), P("tp", "fs"), P("fs", None))
    out_specs = (P("fs", None), P("tp", "fs"), P("tp"))
    return jax.shard_map(
        functools.partial(shards, mesh.shape["fs"], mesh.shape["tp"]),
        mesh=mesh, in_specs=in_specs, out_specs=out_specs, check_vma=False,
    )
```

```python
import functools

import jax
import jax.numpy as jnp
from jax import lax
from jax.experimental import pallas as pl
from jax.experimental.pallas import tpu as pltpu
from jax.sharding import PartitionSpec as P

EPS = 1e-06
BF16 = jnp.bfloat16
F32 = jnp.float32


def place(pieces, count):
    first = pieces[0][1]
    held = jnp.zeros((count,) + first.shape, first.dtype)
    for position, piece in pieces:
        held = lax.dynamic_update_slice_in_dim(held, piece[None], position, 0)
    return held


def take(array, position, axis=0):
    return lax.dynamic_index_in_dim(array, position, axis, keepdims=False)


def gather_kernel(n_z, n_y, n_x, own_gu, own_dn, other_gu, other_dn, mine, w_gu, w_dn, got,
                  z_send, z_recv, y_send, y_recv, x_send, x_recv, c_send, c_recv, local):
    f, t = lax.axis_index("fs"), lax.axis_index("tp")
    z, y, x, c = lax.div(f, n_y), lax.rem(f, n_y), lax.div(t, 2), lax.rem(t, 2)
    n_tp = 2 * n_x
    sources = ((own_gu, other_gu), (own_dn, other_dn))
    held = (w_gu, w_dn)

    def at_z(s):
        return {"fs": lax.rem(z + s, n_z) * n_y + y}

    def at_y(r):
        return {"fs": z * n_y + lax.rem(y + r, n_y)}

    def at_x(s):
        return {"tp": lax.rem(t + 2 * s, n_tp)}

    twin = {"fs": (z + 1 - 2 * lax.rem(z, 2)) * n_y + y}
    core = {"tp": t + 1 - 2 * c}

    barrier = pltpu.get_barrier_semaphore()
    friends = [at_z(s) for s in range(1, n_z)] + [at_y(r) for r in range(1, n_y)]
    friends += [at_x(s) for s in range(1, n_x)] + [core]
    for friend in friends:
        pl.semaphore_signal(barrier, inc=1, device_id=friend, device_id_type=pl.DeviceIdType.MESH)
    pl.semaphore_wait(barrier, len(friends))

    started = []

    def send(src, dst, out_sem, in_sem, to):
        copy = pltpu.make_async_remote_copy(
            src_ref=src, dst_ref=dst, send_sem=out_sem, recv_sem=in_sem,
            device_id=to, device_id_type=pl.DeviceIdType.MESH,
        )
        copy.start()
        started.append(copy)
        return copy

    order = sorted(range(1, n_z), key=lambda s: min(s, n_z - s))
    from_z = {}

    def start_z(k):
        for s in order:
            from_z[k, s] = send(
                sources[k][s % 2], held[k].at[f], z_send.at[k, s], z_recv.at[k, s], at_z(s)
            )

    late = []

    def forward(k, s):
        if s == 0:
            src = sources[k][0]
            slot = f
        else:
            from_z[k, s].wait_recv()
            slot = lax.rem(z + n_z - s, n_z) * n_y + y
            src = held[k].at[slot]
        for r in range(1, n_y):
            late.append(send(
                src, held[k].at[slot], y_send.at[k, s, r], y_recv.at[k, s, r], at_y(r)
            ))

    start_z(0)
    forward(0, 0)
    tokens = send(mine, got.at[:, x, c], x_send.at[0], x_recv.at[0], twin)
    start_z(1)
    forward(1, 0)
    stays = [pltpu.make_async_copy(sources[k][0], held[k].at[f], local.at[k]) for k in range(2)]
    for copy in stays:
        copy.start()
    for s in order:
        forward(0, s)
    tokens.wait_recv()
    across = [
        send(got.at[:, x, c], got.at[:, x, c], x_send.at[s], x_recv.at[s], at_x(s))
        for s in range(1, n_x)
    ]
    for s in order[:-1]:
        forward(1, s)
    for copy in across:
        copy.wait_recv()
    late.append(send(got.at[:, :, c], got.at[:, :, c], c_send, c_recv, core))
    forward(1, order[-1])
    for copy in late:
        copy.wait_recv()
    for copy in started:
        copy.wait_send()
    for copy in stays:
        copy.wait()


def gather_all(n_z, n_y, n_x, own, other, mine):
    n_fs = n_z * n_y
    dma = pltpu.SemaphoreType.DMA
    anywhere = pl.BlockSpec(memory_space=pl.ANY)
    return pl.pallas_call(
        functools.partial(gather_kernel, n_z, n_y, n_x),
        out_shape=[jax.ShapeDtypeStruct((n_fs,) + a.shape, a.dtype) for a in own]
        + [jax.ShapeDtypeStruct((2, n_x, 2) + mine.shape[1:], mine.dtype)],
        in_specs=[anywhere] * 5,
        out_specs=[anywhere] * 3,
        scratch_shapes=[
            dma((2, n_z)), dma((2, n_z)), dma((2, n_z, n_y)), dma((2, n_z, n_y)),
            dma((n_x,)), dma((n_x,)), dma, dma, dma((2,)),
        ],
        compiler_params=pltpu.CompilerParams(collective_id=0, has_side_effects=True),
    )(*own, *other, mine)


def tile_of(extent, most):
    return max(n for n in range(16, most + 1, 16) if extent % n == 0)


def dot(a, b, contract):
    return lax.dot_general(a, b, (contract, ((), ())), preferred_element_type=F32)


def rows_at(start, count):
    return pl.ds(pl.multiple_of(start, 16), count)


def cols_at(start, count):
    return pl.ds(pl.multiple_of(start, 128), count)


def fused_kernel(n_z, n_y, n_x, tokens, cotangent, gain_in, w_gate, w_up, w_down,
                 o_grad, o_down, o_norms,
                 gain, tok, cot, normed, wg, wu, wd, wg_t, wu_t, gate, up, d_hid, hid_t, d_gate, d_up,
                 own_share, y_out, y_in, q_out, q_in, t_out, t_in, n_all,
                 part, c_out, c_in, m_out, m_in, x_out, x_in,
                 sent, z_recv, f_recv, tt_recv, tx_recv, tc_recv, y_recv, q_recv, t_recv, n_recv,
                 c_recv, m_recv, x_recv, a_recv, g_recv, local):
    f, t = lax.axis_index("fs"), lax.axis_index("tp")
    z, y, x, c = lax.div(f, n_y), lax.rem(f, n_y), lax.div(t, 2), lax.rem(t, 2)
    q, h = lax.div(z, 2), lax.rem(z, 2)
    n_tp, n_q = 2 * n_x, n_z // 2
    rows, d_model = tokens.shape
    depth, half = wg.shape[1], wg.shape[2]
    piece = rows // n_tp
    chunks, subs = c_out.shape[1], m_out.shape[0]
    side = rows // 2
    chunk = side // chunks

    def at_z(s):
        return {"fs": lax.rem(z + s, n_z) * n_y + y}

    def at_y(r):
        return {"fs": z * n_y + lax.rem(y + r, n_y)}

    def at_x(s):
        return {"tp": lax.rem(t + 2 * s, n_tp)}

    twin = {"fs": (z + 1 - 2 * h) * n_y + y}
    core = {"tp": t + 1 - 2 * c}

    started = [], []

    def copy_to(src, dst, in_sem, to, phase=0):
        copy = pltpu.make_async_remote_copy(
            src_ref=src, dst_ref=dst, send_sem=sent.at[phase], recv_sem=in_sem,
            device_id=to, device_id_type=pl.DeviceIdType.MESH,
        )
        started[phase].append(copy)
        return copy

    def all_of(ref, in_sem):
        pltpu.make_async_remote_copy(
            src_ref=ref, dst_ref=ref, send_sem=sent.at[0], recv_sem=in_sem,
            device_id=core, device_id_type=pl.DeviceIdType.MESH,
        ).wait_recv()

    def send(*args):
        copy = copy_to(*args)
        copy.start()
        return copy

    def bring(src, dst, sem):
        copy = pltpu.make_async_copy(src, dst, sem)
        copy.start()
        return copy

    kinds = z_recv.shape[0]
    downs_of = range(2, kinds)
    step_rows = half // len(downs_of)

    def source(k, which):
        if k >= 2:
            return w_down.at[rows_at(which * half + (k - 2) * step_rows, step_rows), :]
        return (w_gate, w_up)[k].at[:, cols_at(which * half, half)]

    def held(k, at_slot):
        if k >= 2:
            return wd.at[at_slot, pl.ds((k - 2) * step_rows, step_rows)]
        return (wg, wu)[k].at[at_slot]

    barrier = pltpu.get_barrier_semaphore()
    n_fs = n_z * n_y
    friends = [{"fs": lax.rem(f + s, n_fs)} for s in range(1, n_fs)]
    friends += [at_x(s) for s in range(1, n_x)] + [core]
    for friend in friends:
        pl.semaphore_signal(barrier, inc=1, device_id=friend, device_id_type=pl.DeviceIdType.MESH)
    bring_gain = bring(gain_in, gain, local.at[5])
    bring_tok = bring(tokens, tok.at[pl.ds(0, rows)], local.at[0])
    bring_cot = bring(cotangent, cot.at[pl.ds(0, rows)], local.at[1])
    stays = [bring(source(k, h), held(k, f), local.at[2 + k]) for k in range(2)]
    stays.append(bring(w_down.at[rows_at(h * half, half), :], wd.at[f], local.at[4]))

    pl.semaphore_wait(barrier, len(friends))

    over_y = {}
    others = [[b for b in range(n_z) if b != a] for a in range(n_z)]
    ends = (0, n_z - 1)
    nearest = [sorted(others[a], key=lambda b: abs(a - b)) for a in range(n_z)]
    arrival = [
        [a] + sorted(others[a], key=lambda b: 1 if b == a ^ 1 else 2 * (b not in ends)) for a in range(n_z)
    ]

    def pick(table, p):
        return sum(jnp.where(z == a, table[a][p], 0) for a in range(n_z))

    near = [z] + [pick(arrival, p) for p in range(1, n_z)]

    def start_z(k, p):
        to = pick(nearest, p)
        send(
            source(k, lax.rem(to, 2)), held(k, f), z_recv.at[k, z],
            {"fs": to * n_y + y},
        )

    def slot(p, r):
        return near[p] * n_y + lax.rem(y + n_y - r, n_y)

    def forwarding(k, p):
        if p == 0:
            src, came = source(k, h), None
        else:
            src = held(k, slot(p, 0))
            came = pltpu.make_async_remote_copy(
                src_ref=src, dst_ref=src, send_sem=sent.at[0], recv_sem=z_recv.at[k, near[p]],
                device_id={"fs": near[p] * n_y + y}, device_id_type=pl.DeviceIdType.MESH,
            )
        for r in range(1, n_y):
            over_y[k, p, r] = copy_to(src, held(k, slot(p, 0)), f_recv.at[min(k, 2), near[p], r - 1], at_y(r))

        def go():
            if came is not None:
                came.wait_recv()
            for r in range(1, n_y):
                over_y[k, p, r].start()

        return go

    def forward(k, p):
        forwarding(k, p)()

    raw, both = (tokens, cotangent), (tok, cot)

    cuts = tt_recv.shape[1]
    cut = piece // cuts

    def cut_of(start, i):
        return rows_at(start + i * cut, cut)

    def swap(a):
        return [
            send(raw[a].at[cut_of(t * piece, i)], both[a].at[cut_of(rows + t * piece, i)],
                 tt_recv.at[a, i], twin)
            for i in range(cuts)
        ]

    def across(a, parts):
        copies = []
        for i in parts:
            swapped[a][i].wait_recv()
            at = both[a].at[cut_of(rows + t * piece, i)]
            copies += [send(at, at, tx_recv.at[a, i, s - 1], at_x(s)) for s in range(1, n_x)]
        return copies

    def meet(a):
        copies = []
        for k in range(n_x):
            at = rows_at(rows + (2 * k + c) * piece, piece)
            copies.append(send(both[a].at[at], both[a].at[at], tc_recv.at[a, k], core))
        return copies

    def arrive(copies):
        for copy in copies:
            copy.wait_recv()

    swapped = []
    for p in reversed(range(n_z - 1)):
        start_z(0, p)
        start_z(1, p)
        if p == n_z - 2:
            forward(0, 0)
            forward(1, 0)
            for k in downs_of:
                forward(k, 0)
    for a in range(2):
        swapped.append(swap(a))
    for p in range(n_z - 1):
        for k in downs_of:
            start_z(k, p)

    norm_tile = tile_of(rows, 32)

    def normalize(first):
        @pl.loop(0, rows // norm_tile)
        def _(i):
            at = rows_at(first + i * norm_tile, norm_tile)
            xf = tok[at, :].astype(F32)
            inv = lax.rsqrt(jnp.mean(xf * xf, axis=-1, keepdims=True) + EPS)
            normed[at, :] = (xf * inv * gain[...]).astype(BF16)

    bring_gain.wait()
    bring_tok.wait()
    normalize(0)

    m_tile = tile_of(2 * rows, 768)

    def add_gate_up(p, r, group):
        at_slot = slot(p, r)
        if group == 0:
            if p == 0 and r == 0:
                stays[0].wait()
                stays[1].wait()
            elif r > 0:
                over_y[0, p, r].wait_recv()
                over_y[1, p, r].wait_recv()
            wg_t[at_slot] = wg[at_slot].T
            wu_t[at_slot] = wu[at_slot].T
        at = pl.ds(group * rows, rows)
        a = normed[at, cols_at(at_slot * depth, depth)]
        for total, w in ((gate, wg), (up, wu)):
            term = dot(a, w[at_slot], ((1,), (0,)))
            total[at, :] = term if p == 0 and r == 0 else total[at, :] + term

    def add_d_hidden(s, r):
        at_slot = slot(s, r)
        if s == 0 and r == 0:
            stays[2].wait()
        elif r > 0:
            all_of(wd.at[at_slot], f_recv.at[2, near[s], r - 1])

        @pl.loop(0, 2 * rows // m_tile)
        def _(i):
            at = rows_at(i * m_tile, m_tile)
            term = dot(cot[at, cols_at(at_slot * depth, depth)], wd[at_slot], ((1,), (1,)))
            d_hid[at, :] = term if s == 0 and r == 0 else d_hid[at, :] + term

    add_gate_up(0, 0, 0)
    token_copies = []
    for p in range(1, n_z):
        forward(0, p)
        if p == n_z - 1:
            token_copies += across(0, range(cuts - 1))
        forward(1, p)
        if p == n_z - 1:
            token_copies += across(0, range(cuts - 1, cuts))
        for r in range(1, n_y):
            add_gate_up(p - 1, r, 0)
        add_gate_up(p, 0, 0)
    backward = range(n_z - 1, 0, -1)
    downs = [[forwarding(k, p) for k in downs_of] for p in backward]
    at_end = (z == 0) | (z == n_z - 1)

    at_middle = jnp.logical_not(at_end)

    def down(middle, end, first=0, count=len(downs_of)):
        for which, index in ((at_middle, middle), (at_end, end)):
            if index is not None and index < len(downs):
                @pl.when(which)
                def _():
                    for go in downs[index][first:first + count]:
                        go()

    down(0, None)
    cot_copies = across(1, range(cuts))
    arrive(token_copies)
    met = meet(0)
    down(1, None)
    arrive(met)
    normalize(rows)
    down(None, 0)
    for p in range(n_z):
        for r in range(n_y):
            if p == n_z - 1 and r > 0:
                add_gate_up(p, r, 0)
            add_gate_up(p, r, 1)
        if p == n_z // 2:
            down(None, 1, 0, 1)
    down(2, None)
    down(None, 1, 1)

    e_tile = tile_of(2 * rows, 128)

    @pl.loop(0, 2 * rows // e_tile)
    def _(i):
        at = rows_at(i * e_tile, e_tile)
        g, u = gate[at, :], up[at, :]
        sig = jax.nn.sigmoid(g)
        act = g * sig
        hid_t[:, cols_at(i * e_tile, e_tile)] = (act * u).T.astype(BF16)
        gate[at, :] = 0.5 * (u * sig * (1.0 + g * (1.0 - sig)))
        up[at, :] = 0.5 * act

    arrive(cot_copies)
    bring_cot.wait()
    arrive(meet(1))
    s_tile = tile_of(half, 512)

    def share(block, put):
        @pl.loop(0, half // s_tile)
        def _(i):
            at = rows_at(i * s_tile, s_tile)
            put(at, 0.5 * dot(hid_t[at, :], cot[:, cols_at(block * depth, depth)], ((1,), (0,))))

    def block_of(step, rel, r):
        column = 2 * lax.rem(q + step, n_q) + (h if rel == 0 else 1 - h)
        return column * n_y + lax.rem(y + r, n_y)

    y_copies = {}

    def send_share(step, rel):
        for r in range(1, n_y):
            out = y_out.at[step, rel, r]

            def put(at, value):
                out[at, :] = value.astype(BF16)

            share(block_of(step, rel, r), put)
            y_copies[step, rel, r] = send(
                out, y_in.at[step, rel, r], y_recv.at[step, rel, r - 1], at_y(r)
            )

    def own_block(step, rel):
        out = own_share.at[step, rel]

        def put(at, value):
            out[at, :] = value

        share(block_of(step, rel, 0), put)

    q_copies = {
        (step, rel): copy_to(q_out.at[step, rel], q_in.at[step, rel], q_recv.at[step, rel], at_z(2 * step))
        for step in range(1, n_q) for rel in range(2)
    }

    def cross(rel):
        for step in range(1, n_q):
            for r in range(1, n_y):
                y_copies[step, rel, r].wait_recv()
            total = own_share[step, rel]
            for r in range(1, n_y):
                total = total + y_in[step, rel, r].astype(F32)
            q_out[step, rel] = total.astype(BF16)
            q_copies[step, rel].start()

    down(None, 2)
    for step in range(1, n_q):
        send_share(step, 1)
    for index in range(3, len(downs)):
        down(index, index)
    for step in range(1, n_q):
        send_share(step, 0)
    for rel in (1, 0):
        send_share(0, rel)
    for step in range(1, n_q):
        for rel in (1, 0):
            own_block(step, rel)
    add_d_hidden(0, 0)
    for r in range(1, n_y):
        add_d_hidden(0, r)
    for p in backward:
        add_d_hidden(p, 0)
        for r in range(1, n_y):
            add_d_hidden(p, r)

    d_tile = tile_of(piece, 128)

    @pl.loop(0, 2 * rows // d_tile)
    def _(i):
        at = rows_at(i * d_tile, d_tile)
        index = lax.div(i * d_tile, piece)
        group, index = lax.div(index, n_tp), lax.rem(index, n_tp)
        turn = lax.rem(lax.rem(index, n_x) + 2 * n_x - 1 - x, n_x)
        mine = lax.rem(lax.div(index, n_x) + c + 1, 2)
        to = group * rows + (2 * turn + mine) * piece + lax.rem(i * d_tile, piece)
        d = d_hid[at, :]
        d_gate[rows_at(to, d_tile), :] = (d * gate[at, :]).astype(BF16)
        d_up[rows_at(to, d_tile), :] = (d * up[at, :]).astype(BF16)

    c_copies = {}

    def owner_of(s):
        return lax.rem(x + s, n_x) * subs

    def partial(group, s):
        first = group * rows + (s - 1 if s else n_x - 1) * 2 * piece
        owner = owner_of(s)

        @pl.loop(0, n_z * n_y, unroll=4)
        def _(k):
            at, to = pl.ds(first, 2 * piece), cols_at(k * depth, depth)
            value = dot(d_gate[at, :], wg_t[k], ((1,), (0,))) + dot(d_up[at, :], wu_t[k], ((1,), (0,)))
            for u in range(subs):
                c_out[group, owner + u, :, to] = value[u * chunk:(u + 1) * chunk].astype(BF16)
                part[group, owner + u, :, to] = value[piece + u * chunk:piece + (u + 1) * chunk]

        for u in range(subs):
            j = owner + u
            c_copies[group, s, u] = send(
                c_out.at[group, j], c_in.at[group, j], c_recv.at[group, j], core
            )

    l_tile = tile_of(chunk, 32)

    def each(body):
        @pl.loop(0, chunk // l_tile)
        def _(i):
            body(rows_at(i * l_tile, l_tile))

    x_copies, m_copies = {}, {}

    def summed(group, j, at):
        return part[group, j, at, :] + c_in[group, j, at, :].astype(F32)

    def to_x(group):
        for u in range(subs):
            for s in range(1, n_x):
                c_copies[group, s, u].wait_recv()
                j = owner_of(s) + u

                def fold(at):
                    x_out[group, s, u, at, :] = summed(group, j, at).astype(BF16)

                each(fold)
                x_copies[group, s, u] = send(
                    x_out.at[group, s, u], x_in.at[group, s, u], x_recv.at[group, s - 1, u], at_x(s)
                )

    def total_of(group, u, at):
        total = summed(group, owner_of(0) + u, at)
        for s in range(1, n_x):
            total = total + x_in[group, s, u, at, :].astype(F32)
        return total

    for s in range(1, n_x):
        partial(1, s)
    pl.when(at_middle)(functools.partial(cross, 1))
    to_x(1)
    pl.when(at_end)(functools.partial(cross, 1))
    partial(1, 0)
    for s in range(1, n_x):
        partial(0, s)
    to_x(0)
    pl.when(at_middle)(functools.partial(cross, 0))
    partial(0, 0)
    for rel in (1, 0):
        own_block(0, rel)
    for u in range(subs):
        c_copies[1, 0, u].wait_recv()
        for s in range(1, n_x):
            x_copies[1, s, u].wait_recv()

        def fold(at):
            m_out[u, at, :] = total_of(1, u, at).astype(BF16)

        each(fold)
        m_copies[u] = send(m_out.at[u], m_in.at[u], m_recv.at[u], twin)
    pl.when(at_end)(functools.partial(cross, 0))
    for u in range(subs):
        c_copies[0, 0, u].wait_recv()
    gathered = {}

    def place_of(at_x_index, u):
        return o_grad.at[rows_at((c * n_x + at_x_index) * piece + u * chunk, chunk)]

    def finish(u):
        for s in range(1, n_x):
            x_copies[0, s, u].wait_recv()
        m_copies[u].wait_recv()
        first = (c * n_x + x) * piece + u * chunk

        @pl.loop(0, chunk // l_tile)
        def _(i):
            at = rows_at(i * l_tile, l_tile)
            to = rows_at(first + i * l_tile, l_tile)
            xf = tok[to, :].astype(F32)
            inv = lax.rsqrt(jnp.mean(xf * xf, axis=-1, keepdims=True) + EPS)
            scaled = xf * inv
            d_normed = total_of(0, u, at) + m_in[u, at, :].astype(F32)
            d_scaled = d_normed * gain[...]
            inner = jnp.mean(d_scaled * scaled, axis=-1, keepdims=True)
            o_grad[to, :] = (inv * (d_scaled - scaled * inner)).astype(BF16)

        out = place_of(x, u)
        for s in range(1, n_x):
            gathered[u, s] = send(out, out, a_recv.at[u, s - 1], at_x(s), 1)
        send(out, out, g_recv, core, 1)

    def relay(u):
        for s in range(1, n_x):
            gathered[u, s].wait_recv()
            out = place_of(lax.rem(x + n_x - s, n_x), u)
            send(out, out, g_recv, core, 1)

    def collect(rel, put):
        for r in range(1, n_y):
            y_copies[0, rel, r].wait_recv()
        for step in range(1, n_q):
            q_copies[step, rel].wait_recv()
        total = own_share[0, rel]
        for r in range(1, n_y):
            total = total + y_in[0, rel, r].astype(F32)
        for step in range(1, n_q):
            total = total + q_in[step, rel].astype(F32)
        put(0, pl.ds(0, half), total)

    n_tile = tile_of(half, 128)

    def squares(value):
        folded = sum(value[:, k * 128:(k + 1) * 128] * value[:, k * 128:(k + 1) * 128] for k in range(depth // 128))
        return jnp.concatenate(
            [jnp.sum(folded[i:i + n_tile].T, axis=0, keepdims=True) for i in range(0, half, n_tile)], axis=1
        )

    def put_twin(start, at, value):
        t_out[at, :] = value.astype(BF16)
        n_all[f] = squares(value)

    def put_kept(start, at, value):
        o_down[rows_at(h * half + start, half), :] = value
        n_all[f] = n_all[f] + squares(value)

    collect(1, put_twin)
    traded = copy_to(t_out, t_in, t_recv, twin, 1)
    pl.when(at_middle)(traded.start)
    for u in range(subs):
        finish(u)
    collect(0, put_kept)
    for s in range(1, n_fs):
        send(n_all.at[f], n_all.at[f], n_recv, {"fs": lax.rem(f + s, n_fs)}, 1)
    pl.when(at_end)(traded.start)
    for copy in started[0]:
        copy.wait_send()
    for u in range(subs):
        relay(u)
    all_of(n_all.at[pl.ds(0, n_fs - 1)], n_recv)
    for side_of in range(2):
        total = sum(n_all[k] for k in range(n_fs) if k // n_y % 2 == side_of)
        o_norms[:, side_of * half:(side_of + 1) * half] = total
    for copy in started[1]:
        copy.wait_send()
    traded.wait_recv()
    o_down[rows_at((1 - h) * half, half), :] = t_in[...].astype(F32)
    all_of(o_grad.at[rows_at((1 - c) * side, side)], g_recv)


def put_out(grad, down, norms, o_grad, o_down, o_norms, done):
    copies = [
        pltpu.make_async_copy(src, dst, done.at[i])
        for i, (src, dst) in enumerate(((grad, o_grad), (down, o_down), (norms, o_norms)))
    ]
    for copy in copies:
        copy.start()
    for copy in copies:
        copy.wait()


def fused(n_z, n_y, n_x, tokens, norm_gain, w_gate, w_up, w_down, cotangent):
    n_fs, n_tp, n_q = n_z * n_y, 2 * n_x, n_z // 2
    rows, d_model = tokens.shape
    depth, half = w_gate.shape[0], w_gate.shape[1] // 2
    piece = rows // n_tp
    cuts = 2 if piece % 32 == 0 else 1
    kinds = 2 + 4
    subs = max(n for n in (1, 2, 3) if piece % (16 * n) == 0)
    chunks = n_x * subs
    chunk = rows // 2 // chunks
    dma, vmem = pltpu.SemaphoreType.DMA, pltpu.VMEM
    outside = pl.BlockSpec(memory_space=pltpu.HBM)
    inside = pl.BlockSpec(memory_space=pltpu.VMEM)
    block = (half, depth)
    scratch = [
        vmem((1, d_model), F32),
        vmem((2 * rows, d_model), BF16), vmem((2 * rows, d_model), BF16), vmem((2 * rows, d_model), BF16),
        vmem((n_fs, depth, half), BF16), vmem((n_fs, depth, half), BF16), vmem((n_fs, half, depth), BF16),
        vmem((n_fs, half, depth), BF16), vmem((n_fs, half, depth), BF16),
        vmem((2 * rows, half), F32), vmem((2 * rows, half), F32), vmem((2 * rows, half), F32),
        vmem((half, 2 * rows), BF16), vmem((2 * rows, half), BF16), vmem((2 * rows, half), BF16),
        vmem((n_q, 2) + block, F32), vmem((n_q, 2, n_y) + block, BF16), vmem((n_q, 2, n_y) + block, BF16),
        vmem((n_q, 2) + block, BF16), vmem((n_q, 2) + block, BF16), vmem(block, BF16), vmem(block, BF16),
        vmem((n_fs, 1, half), F32),
        vmem((2, chunks, chunk, d_model), F32),
        vmem((2, chunks, chunk, d_model), BF16), vmem((2, chunks, chunk, d_model), BF16),
        vmem((subs, chunk, d_model), BF16), vmem((subs, chunk, d_model), BF16),
        vmem((2, n_x, subs, chunk, d_model), BF16), vmem((2, n_x, subs, chunk, d_model), BF16),
        dma((2,)), dma((kinds, n_z)), dma((3, n_z, n_y - 1)),
        dma((2, cuts)), dma((2, cuts, n_x - 1)), dma((2, n_x)),
        dma((n_q, 2, n_y - 1)), dma((n_q, 2)), dma, dma,
        dma((2, chunks)), dma((subs,)), dma((2, n_x - 1, subs)), dma((subs, n_x - 1)),
        dma, dma((6,)),
    ]
    grad, down, norms = pl.pallas_call(
        functools.partial(fused_kernel, n_z, n_y, n_x),
        out_shape=[
            jax.ShapeDtypeStruct((rows, d_model), BF16),
            jax.ShapeDtypeStruct((2 * half, depth), F32),
            jax.ShapeDtypeStruct((1, 2 * half), F32),
        ],
        in_specs=[outside] * 6,
        out_specs=[inside, inside, inside],
        scratch_shapes=scratch,
        compiler_params=pltpu.CompilerParams(
            collective_id=1, has_side_effects=True, vmem_limit_bytes=48 * 2**20
        ),
    )(*[
        pltpu.with_memory_space_constraint(a, pltpu.HBM)
        for a in (tokens, cotangent, norm_gain.reshape(1, d_model), w_gate, w_up, w_down)
    ])
    grad, down, norms = pl.pallas_call(
        put_out,
        out_shape=[jax.ShapeDtypeStruct(a.shape, a.dtype) for a in (grad, down, norms)],
        in_specs=[pl.BlockSpec(memory_space=pl.ANY)] * 3,
        out_specs=[outside] * 3,
        scratch_shapes=[dma((3,))],
        compiler_params=pltpu.CompilerParams(vmem_limit_bytes=2**20),
    )(grad, down, norms)
    return grad, down, norms.reshape(2 * half)


def shards(n_fs, n_tp, tokens, norm_gain, w_gate, w_up, w_down, cotangent):
    n_y = 2 ** ((n_fs.bit_length() - 1) // 2)
    n_z, n_x = n_fs // n_y, n_tp // 2
    n_q = n_z // 2
    f, t = lax.axis_index("fs"), lax.axis_index("tp")
    z, y, x, c = f // n_y, f % n_y, t // 2, t % 2
    q, h = z // 2, z % 2
    rows, d_model = tokens.shape
    depth, half = w_gate.shape[0], w_gate.shape[1] // 2
    piece = rows // n_tp

    if piece % 16 == 0 and depth % 128 == 0 and half % 128 == 0:
        return fused(n_z, n_y, n_x, tokens, norm_gain, w_gate, w_up, w_down, cotangent)

    def to_z(a, step):
        return lax.ppermute(a, "fs", [(i, (i + step * n_y) % n_fs) for i in range(n_fs)])

    def to_y(a, step):
        return lax.ppermute(
            a, "fs", [(i, i // n_y * n_y + (i + step) % n_y) for i in range(n_fs)]
        )

    def to_twin(a):
        return lax.ppermute(
            a, "fs", [(i, (i // n_y ^ 1) * n_y + i % n_y) for i in range(n_fs)]
        )

    def to_x(a, step):
        return lax.ppermute(a, "tp", [(i, (i + 2 * step) % n_tp) for i in range(n_tp)])

    def to_core(a):
        return lax.ppermute(a, "tp", [(i, i ^ 1) for i in range(n_tp)])

    mine = jnp.stack(
        [lax.dynamic_slice_in_dim(a, t * piece, piece, 0) for a in (tokens, cotangent)]
    )
    down_t = w_down.T

    def half_of(which):
        gate_up = jnp.concatenate(
            [lax.dynamic_slice_in_dim(w, which * half, half, 1) for w in (w_gate, w_up)], axis=1
        )
        return gate_up, lax.dynamic_slice_in_dim(down_t, which * half, half, 1)

    own, other = half_of(h), half_of(1 - h)

    w_gu, w_dn, got = gather_all(n_z, n_y, n_x, own, other, mine)
    w_gu, w_dn = w_gu.reshape(d_model, 2 * half), w_dn.reshape(d_model, half)
    got = got.reshape(2, rows, d_model)
    tokens2 = jnp.concatenate([tokens, got[0]], axis=0)
    cot2 = jnp.concatenate([cotangent, got[1]], axis=0)

    xf = tokens2.astype(F32)
    inv = lax.rsqrt(jnp.mean(xf * xf, axis=-1, keepdims=True) + EPS)
    normed = (xf * inv * norm_gain).astype(BF16)
    gate_up = jnp.dot(normed, w_gu, preferred_element_type=F32)
    gate, up = gate_up[:, :half], gate_up[:, half:]
    sig = jax.nn.sigmoid(gate)
    act = gate * sig
    hidden = (act * up).astype(BF16)

    share = 0.5 * lax.dot_general(
        cot2, hidden, (((0,), (0,)), ((), ())), preferred_element_type=F32
    )
    share = share.reshape(n_q, 2, n_y, depth, half)
    share, w_dn = lax.optimization_barrier((share, w_dn))

    def sent_over_y(pair):
        block = take(share, pair)
        return [to_y(take(block, (y + s) % n_y, 1).astype(BF16), s) for s in range(1, n_y)]

    def over_y(pair, came):
        return sum([a.astype(F32) for a in came], take(take(share, pair), y, 1))

    first = [sent_over_y((q + s) % n_q) for s in range(1, n_q)]

    d_hidden = 0.5 * jnp.dot(cot2, w_dn, preferred_element_type=F32)
    d_gate = (d_hidden * up * sig * (1.0 + gate * (1.0 - sig))).astype(BF16)
    d_up = (d_hidden * act).astype(BF16)
    d_both = jnp.concatenate([d_gate, d_up], axis=1)
    part = lax.dot_general(
        d_both, w_gu, (((1,), (1,)), ((), ())), preferred_element_type=F32
    )
    part, first = lax.optimization_barrier((part.astype(BF16), first))

    away = [
        to_z(over_y((q + s) % n_q, first[s - 1]).astype(BF16), 2 * s) for s in range(1, n_q)
    ]
    total = over_y(q, sent_over_y(q))
    total = sum([a.astype(F32) for a in away], total)
    kept = take(total, h)
    came = to_twin(take(total, 1 - h).astype(BF16)).astype(F32)
    grad_down = place([(h, kept.T), (1 - h, came.T)], 2).reshape(2 * half, depth)
    norms = jnp.sum(grad_down * grad_down, axis=1)
    norms = sum([to_y(norms, s) for s in range(1, n_y)], norms)
    down_norms = sum([to_z(norms, s) for s in range(1, n_z)], norms)

    part = part.reshape(2, n_x, 2, piece, d_model)
    part = take(part, c, 2).astype(F32) + to_core(take(part, 1 - c, 2)).astype(F32)
    total = take(part, x, 1)
    for s in range(1, n_x):
        total = total + to_x(take(part, (x + s) % n_x, 1).astype(BF16), s).astype(F32)
    d_normed = total[0] + to_twin(total[1].astype(BF16)).astype(F32)

    xp = lax.dynamic_slice_in_dim(tokens, t * piece, piece, 0).astype(F32)
    inv_p = lax.rsqrt(jnp.mean(xp * xp, axis=-1, keepdims=True) + EPS)
    scaled = xp * inv_p
    d_scaled = d_normed * norm_gain
    inner = jnp.mean(d_scaled * scaled, axis=-1, keepdims=True)
    grad = (inv_p * (d_scaled - scaled * inner)).astype(BF16)
    grad = place([(x, grad)] + [((x - s) % n_x, to_x(grad, s)) for s in range(1, n_x)], n_x)
    grad = place([(c, grad), (1 - c, to_core(grad))], 2)
    grad_tokens = grad.transpose(1, 0, 2, 3).reshape(rows, d_model)
    return (grad_tokens, grad_down, down_norms)


def solution(mesh):
    in_specs = (P("fs", None), P(), P("fs", "tp"), P("fs", "tp"), P("tp", "fs"), P("fs", None))
    out_specs = (P("fs", None), P("tp", "fs"), P("tp"))
    return jax.shard_map(
        functools.partial(shards, mesh.shape["fs"], mesh.shape["tp"]),
        mesh=mesh, in_specs=in_specs, out_specs=out_specs, check_vma=False,
    )
```

```python
import functools

import jax
import jax.numpy as jnp
from jax import lax
from jax.experimental import pallas as pl
from jax.experimental.pallas import tpu as pltpu
from jax.sharding import PartitionSpec as P

EPS = 1e-06
BF16 = jnp.bfloat16
F32 = jnp.float32


def place(pieces, count):
    first = pieces[0][1]
    held = jnp.zeros((count,) + first.shape, first.dtype)
    for position, piece in pieces:
        held = lax.dynamic_update_slice_in_dim(held, piece[None], position, 0)
    return held


def take(array, position, axis=0):
    return lax.dynamic_index_in_dim(array, position, axis, keepdims=False)


def gather_kernel(n_z, n_y, n_x, own_gu, own_dn, other_gu, other_dn, mine, w_gu, w_dn, got,
                  z_send, z_recv, y_send, y_recv, x_send, x_recv, c_send, c_recv, local):
    f, t = lax.axis_index("fs"), lax.axis_index("tp")
    z, y, x, c = lax.div(f, n_y), lax.rem(f, n_y), lax.div(t, 2), lax.rem(t, 2)
    n_tp = 2 * n_x
    sources = ((own_gu, other_gu), (own_dn, other_dn))
    held = (w_gu, w_dn)

    def at_z(s):
        return {"fs": lax.rem(z + s, n_z) * n_y + y}

    def at_y(r):
        return {"fs": z * n_y + lax.rem(y + r, n_y)}

    def at_x(s):
        return {"tp": lax.rem(t + 2 * s, n_tp)}

    twin = {"fs": (z + 1 - 2 * lax.rem(z, 2)) * n_y + y}
    core = {"tp": t + 1 - 2 * c}

    barrier = pltpu.get_barrier_semaphore()
    friends = [at_z(s) for s in range(1, n_z)] + [at_y(r) for r in range(1, n_y)]
    friends += [at_x(s) for s in range(1, n_x)] + [core]
    for friend in friends:
        pl.semaphore_signal(barrier, inc=1, device_id=friend, device_id_type=pl.DeviceIdType.MESH)
    pl.semaphore_wait(barrier, len(friends))

    started = []

    def send(src, dst, out_sem, in_sem, to):
        copy = pltpu.make_async_remote_copy(
            src_ref=src, dst_ref=dst, send_sem=out_sem, recv_sem=in_sem,
            device_id=to, device_id_type=pl.DeviceIdType.MESH,
        )
        copy.start()
        started.append(copy)
        return copy

    order = sorted(range(1, n_z), key=lambda s: min(s, n_z - s))
    from_z = {}

    def start_z(k):
        for s in order:
            from_z[k, s] = send(
                sources[k][s % 2], held[k].at[f], z_send.at[k, s], z_recv.at[k, s], at_z(s)
            )

    late = []

    def forward(k, s):
        if s == 0:
            src = sources[k][0]
            slot = f
        else:
            from_z[k, s].wait_recv()
            slot = lax.rem(z + n_z - s, n_z) * n_y + y
            src = held[k].at[slot]
        for r in range(1, n_y):
            late.append(send(
                src, held[k].at[slot], y_send.at[k, s, r], y_recv.at[k, s, r], at_y(r)
            ))

    start_z(0)
    forward(0, 0)
    tokens = send(mine, got.at[:, x, c], x_send.at[0], x_recv.at[0], twin)
    start_z(1)
    forward(1, 0)
    stays = [pltpu.make_async_copy(sources[k][0], held[k].at[f], local.at[k]) for k in range(2)]
    for copy in stays:
        copy.start()
    for s in order:
        forward(0, s)
    tokens.wait_recv()
    across = [
        send(got.at[:, x, c], got.at[:, x, c], x_send.at[s], x_recv.at[s], at_x(s))
        for s in range(1, n_x)
    ]
    for s in order[:-1]:
        forward(1, s)
    for copy in across:
        copy.wait_recv()
    late.append(send(got.at[:, :, c], got.at[:, :, c], c_send, c_recv, core))
    forward(1, order[-1])
    for copy in late:
        copy.wait_recv()
    for copy in started:
        copy.wait_send()
    for copy in stays:
        copy.wait()


def gather_all(n_z, n_y, n_x, own, other, mine):
    n_fs = n_z * n_y
    dma = pltpu.SemaphoreType.DMA
    anywhere = pl.BlockSpec(memory_space=pl.ANY)
    return pl.pallas_call(
        functools.partial(gather_kernel, n_z, n_y, n_x),
        out_shape=[jax.ShapeDtypeStruct((n_fs,) + a.shape, a.dtype) for a in own]
        + [jax.ShapeDtypeStruct((2, n_x, 2) + mine.shape[1:], mine.dtype)],
        in_specs=[anywhere] * 5,
        out_specs=[anywhere] * 3,
        scratch_shapes=[
            dma((2, n_z)), dma((2, n_z)), dma((2, n_z, n_y)), dma((2, n_z, n_y)),
            dma((n_x,)), dma((n_x,)), dma, dma, dma((2,)),
        ],
        compiler_params=pltpu.CompilerParams(collective_id=0, has_side_effects=True),
    )(*own, *other, mine)


def tile_of(extent, most):
    return max(n for n in range(16, most + 1, 16) if extent % n == 0)


def dot(a, b, contract):
    return lax.dot_general(a, b, (contract, ((), ())), preferred_element_type=F32)


def rows_at(start, count):
    return pl.ds(pl.multiple_of(start, 16), count)


def cols_at(start, count):
    return pl.ds(pl.multiple_of(start, 128), count)


def fused_kernel(n_z, n_y, n_x, tokens, cotangent, gain_in, w_gate, w_up, w_down,
                 o_grad, o_down, o_norms,
                 gain, tok, cot, normed, wg, wu, wd, wg_t, wu_t, gate, up, d_hid, hid_t, d_gate, d_up,
                 own_share, y_out, y_in, q_out, q_in, t_out, t_in, n_all,
                 part, c_out, c_in, m_out, m_in, x_out, x_in,
                 sent, z_recv, f_recv, tt_recv, tx_recv, tc_recv, y_recv, q_recv, t_recv, n_recv,
                 c_recv, m_recv, x_recv, a_recv, g_recv, local):
    f, t = lax.axis_index("fs"), lax.axis_index("tp")
    z, y, x, c = lax.div(f, n_y), lax.rem(f, n_y), lax.div(t, 2), lax.rem(t, 2)
    q, h = lax.div(z, 2), lax.rem(z, 2)
    n_tp, n_q = 2 * n_x, n_z // 2
    rows, d_model = tokens.shape
    depth, half = wg.shape[1], wg.shape[2]
    piece = rows // n_tp
    chunks, subs = c_out.shape[1], m_out.shape[0]
    side = rows // 2
    chunk = side // chunks

    def at_z(s):
        return {"fs": lax.rem(z + s, n_z) * n_y + y}

    def at_y(r):
        return {"fs": z * n_y + lax.rem(y + r, n_y)}

    def at_x(s):
        return {"tp": lax.rem(t + 2 * s, n_tp)}

    twin = {"fs": (z + 1 - 2 * h) * n_y + y}
    core = {"tp": t + 1 - 2 * c}

    started = [], []

    def copy_to(src, dst, in_sem, to, phase=0):
        copy = pltpu.make_async_remote_copy(
            src_ref=src, dst_ref=dst, send_sem=sent.at[phase], recv_sem=in_sem,
            device_id=to, device_id_type=pl.DeviceIdType.MESH,
        )
        started[phase].append(copy)
        return copy

    def all_of(ref, in_sem):
        pltpu.make_async_remote_copy(
            src_ref=ref, dst_ref=ref, send_sem=sent.at[0], recv_sem=in_sem,
            device_id=core, device_id_type=pl.DeviceIdType.MESH,
        ).wait_recv()

    def send(*args):
        copy = copy_to(*args)
        copy.start()
        return copy

    def bring(src, dst, sem):
        copy = pltpu.make_async_copy(src, dst, sem)
        copy.start()
        return copy

    kinds = z_recv.shape[0]
    downs_of = range(2, kinds)
    step_rows = half // len(downs_of)

    def source(k, which):
        if k >= 2:
            return w_down.at[rows_at(which * half + (k - 2) * step_rows, step_rows), :]
        return (w_gate, w_up)[k].at[:, cols_at(which * half, half)]

    def held(k, at_slot):
        if k >= 2:
            return wd.at[at_slot, pl.ds((k - 2) * step_rows, step_rows)]
        return (wg, wu)[k].at[at_slot]

    barrier = pltpu.get_barrier_semaphore()
    n_fs = n_z * n_y
    friends = [{"fs": lax.rem(f + s, n_fs)} for s in range(1, n_fs)]
    friends += [at_x(s) for s in range(1, n_x)] + [core]
    for friend in friends:
        pl.semaphore_signal(barrier, inc=1, device_id=friend, device_id_type=pl.DeviceIdType.MESH)
    bring_gain = bring(gain_in, gain, local.at[5])
    bring_tok = bring(tokens, tok.at[pl.ds(0, rows)], local.at[0])
    bring_cot = bring(cotangent, cot.at[pl.ds(0, rows)], local.at[1])
    stays = [bring(source(k, h), held(k, f), local.at[2 + k]) for k in range(2)]
    stays.append(bring(w_down.at[rows_at(h * half, half), :], wd.at[f], local.at[4]))

    pl.semaphore_wait(barrier, len(friends))

    over_y = {}
    others = [[b for b in range(n_z) if b != a] for a in range(n_z)]
    ends = (0, n_z - 1)
    nearest = [sorted(others[a], key=lambda b: abs(a - b)) for a in range(n_z)]
    arrival = [
        [a] + sorted(others[a], key=lambda b: 1 if b == a ^ 1 else 2 * (b not in ends)) for a in range(n_z)
    ]

    def pick(table, p):
        return sum(jnp.where(z == a, table[a][p], 0) for a in range(n_z))

    near = [z] + [pick(arrival, p) for p in range(1, n_z)]

    def start_z(k, p):
        to = pick(nearest, p)
        send(
            source(k, lax.rem(to, 2)), held(k, f), z_recv.at[k, z],
            {"fs": to * n_y + y},
        )

    def slot(p, r):
        return near[p] * n_y + lax.rem(y + n_y - r, n_y)

    def forwarding(k, p):
        if p == 0:
            src, came = source(k, h), None
        else:
            src = held(k, slot(p, 0))
            came = pltpu.make_async_remote_copy(
                src_ref=src, dst_ref=src, send_sem=sent.at[0], recv_sem=z_recv.at[k, near[p]],
                device_id={"fs": near[p] * n_y + y}, device_id_type=pl.DeviceIdType.MESH,
            )
        for r in range(1, n_y):
            over_y[k, p, r] = copy_to(src, held(k, slot(p, 0)), f_recv.at[min(k, 2), near[p], r - 1], at_y(r))

        def go():
            if came is not None:
                came.wait_recv()
            for r in range(1, n_y):
                over_y[k, p, r].start()

        return go

    def forward(k, p):
        forwarding(k, p)()

    raw, both = (tokens, cotangent), (tok, cot)

    cuts = tt_recv.shape[1]
    cut = piece // cuts

    def cut_of(start, i):
        return rows_at(start + i * cut, cut)

    def swap(a):
        return [
            send(raw[a].at[cut_of(t * piece, i)], both[a].at[cut_of(rows + t * piece, i)],
                 tt_recv.at[a, i], twin)
            for i in range(cuts)
        ]

    def across(a, parts):
        copies = []
        for i in parts:
            swapped[a][i].wait_recv()
            at = both[a].at[cut_of(rows + t * piece, i)]
            copies += [send(at, at, tx_recv.at[a, i, s - 1], at_x(s)) for s in range(1, n_x)]
        return copies

    def meet(a):
        copies = []
        for k in range(n_x):
            at = rows_at(rows + (2 * k + c) * piece, piece)
            copies.append(send(both[a].at[at], both[a].at[at], tc_recv.at[a, k], core))
        return copies

    def arrive(copies):
        for copy in copies:
            copy.wait_recv()

    swapped = []
    for p in reversed(range(n_z - 1)):
        start_z(0, p)
        start_z(1, p)
        if p == n_z - 2:
            forward(0, 0)
            forward(1, 0)
            for k in downs_of:
                forward(k, 0)
    for a in range(2):
        swapped.append(swap(a))
    for p in range(n_z - 1):
        for k in downs_of:
            start_z(k, p)

    norm_tile = tile_of(rows, 32)

    def normalize(first):
        @pl.loop(0, rows // norm_tile)
        def _(i):
            at = rows_at(first + i * norm_tile, norm_tile)
            xf = tok[at, :].astype(F32)
            inv = lax.rsqrt(jnp.mean(xf * xf, axis=-1, keepdims=True) + EPS)
            normed[at, :] = (xf * inv * gain[...]).astype(BF16)

    bring_gain.wait()
    bring_tok.wait()
    normalize(0)

    m_tile = tile_of(2 * rows, 768)

    def add_gate_up(p, r, group):
        at_slot = slot(p, r)
        if group == 0:
            if p == 0 and r == 0:
                stays[0].wait()
                stays[1].wait()
            elif r > 0:
                over_y[0, p, r].wait_recv()
                over_y[1, p, r].wait_recv()
            wg_t[at_slot] = wg[at_slot].T
            wu_t[at_slot] = wu[at_slot].T
        at = pl.ds(group * rows, rows)
        a = normed[at, cols_at(at_slot * depth, depth)]
        for total, w in ((gate, wg), (up, wu)):
            term = dot(a, w[at_slot], ((1,), (0,)))
            total[at, :] = term if p == 0 and r == 0 else total[at, :] + term

    def add_d_hidden(s, r):
        at_slot = slot(s, r)
        if s == 0 and r == 0:
            stays[2].wait()
        elif r > 0:
            all_of(wd.at[at_slot], f_recv.at[2, near[s], r - 1])

        @pl.loop(0, 2 * rows // m_tile)
        def _(i):
            at = rows_at(i * m_tile, m_tile)
            term = dot(cot[at, cols_at(at_slot * depth, depth)], wd[at_slot], ((1,), (1,)))
            d_hid[at, :] = term if s == 0 and r == 0 else d_hid[at, :] + term

    add_gate_up(0, 0, 0)
    token_copies = []
    for p in range(1, n_z):
        forward(0, p)
        if p == n_z - 1:
            token_copies += across(0, range(cuts - 1))
        forward(1, p)
        if p == n_z - 1:
            token_copies += across(0, range(cuts - 1, cuts))
        for r in range(1, n_y):
            add_gate_up(p - 1, r, 0)
        add_gate_up(p, 0, 0)
    backward = range(n_z - 1, 0, -1)
    downs = [[forwarding(k, p) for k in downs_of] for p in backward]
    at_end = (z == 0) | (z == n_z - 1)

    at_middle = jnp.logical_not(at_end)

    def down(middle, end, first=0, count=len(downs_of)):
        for which, index in ((at_middle, middle), (at_end, end)):
            if index is not None and index < len(downs):
                @pl.when(which)
                def _():
                    for go in downs[index][first:first + count]:
                        go()

    down(0, None)
    cot_copies = across(1, range(cuts))
    arrive(token_copies)
    met = meet(0)
    down(1, None)
    arrive(met)
    normalize(rows)
    down(None, 0)
    for p in range(n_z):
        for r in range(n_y):
            if p == n_z - 1 and r > 0:
                add_gate_up(p, r, 0)
            add_gate_up(p, r, 1)
        if p == n_z // 2:
            down(None, 1, 0, 1)
    down(2, None)
    down(None, 1, 1)

    e_tile = tile_of(2 * rows, 128)

    @pl.loop(0, 2 * rows // e_tile)
    def _(i):
        at = rows_at(i * e_tile, e_tile)
        g, u = gate[at, :], up[at, :]
        sig = jax.nn.sigmoid(g)
        act = g * sig
        hid_t[:, cols_at(i * e_tile, e_tile)] = (act * u).T.astype(BF16)
        gate[at, :] = 0.5 * (u * sig * (1.0 + g * (1.0 - sig)))
        up[at, :] = 0.5 * act

    arrive(cot_copies)
    bring_cot.wait()
    arrive(meet(1))
    parts = y_recv.shape[3]
    some = half // parts

    def rows_of(part):
        return pl.ds(part * some, some)

    def share(block, at):
        return 0.5 * dot(hid_t[at, :], cot[:, cols_at(block * depth, depth)], ((1,), (0,)))

    def block_of(step, rel, r):
        column = 2 * lax.rem(q + step, n_q) + (h if rel == 0 else 1 - h)
        return column * n_y + lax.rem(y + r, n_y)

    y_copies = {}

    def send_share(step, rel):
        for part in range(parts):
            at = rows_of(part)
            for r in range(1, n_y):
                out = y_out.at[step, rel, r, at]
                out[...] = share(block_of(step, rel, r), at).astype(BF16)
                y_copies[step, rel, r, part] = send(
                    out, y_in.at[step, rel, r, at], y_recv.at[step, rel, r - 1, part], at_y(r)
                )

    def own_block(step, rel):
        own_share[step, rel] = share(block_of(step, rel, 0), pl.ds(0, half))

    q_copies = {
        (step, rel, part): copy_to(
            q_out.at[step, rel, rows_of(part)], q_in.at[step, rel, rows_of(part)],
            q_recv.at[step, rel, part], at_z(2 * step),
        )
        for step in range(1, n_q) for rel in range(2) for part in range(parts)
    }

    def cross(rel):
        for part in range(parts):
            at = rows_of(part)
            for step in range(1, n_q):
                for r in range(1, n_y):
                    y_copies[step, rel, r, part].wait_recv()
                total = own_share[step, rel, at]
                for r in range(1, n_y):
                    total = total + y_in[step, rel, r, at].astype(F32)
                q_out[step, rel, at] = total.astype(BF16)
                q_copies[step, rel, part].start()

    down(None, 2)
    for step in range(1, n_q):
        send_share(step, 1)
    for index in range(3, len(downs)):
        down(index, index)
    for step in range(1, n_q):
        send_share(step, 0)
    for rel in (1, 0):
        send_share(0, rel)
    for step in range(1, n_q):
        for rel in (1, 0):
            own_block(step, rel)
    add_d_hidden(0, 0)
    for r in range(1, n_y):
        add_d_hidden(0, r)
    for p in backward:
        add_d_hidden(p, 0)
        for r in range(1, n_y):
            add_d_hidden(p, r)

    d_tile = tile_of(piece, 128)

    @pl.loop(0, 2 * rows // d_tile)
    def _(i):
        at = rows_at(i * d_tile, d_tile)
        index = lax.div(i * d_tile, piece)
        group, index = lax.div(index, n_tp), lax.rem(index, n_tp)
        turn = lax.rem(lax.rem(index, n_x) + 2 * n_x - 1 - x, n_x)
        mine = lax.rem(lax.div(index, n_x) + c + 1, 2)
        to = group * rows + (2 * turn + mine) * piece + lax.rem(i * d_tile, piece)
        d = d_hid[at, :]
        d_gate[rows_at(to, d_tile), :] = (d * gate[at, :]).astype(BF16)
        d_up[rows_at(to, d_tile), :] = (d * up[at, :]).astype(BF16)

    c_copies = {}

    def owner_of(s):
        return lax.rem(x + s, n_x) * subs

    def partial(group, s):
        first = group * rows + (s - 1 if s else n_x - 1) * 2 * piece
        owner = owner_of(s)

        @pl.loop(0, n_z * n_y, unroll=4)
        def _(k):
            at, to = pl.ds(first, 2 * piece), cols_at(k * depth, depth)
            value = dot(d_gate[at, :], wg_t[k], ((1,), (0,))) + dot(d_up[at, :], wu_t[k], ((1,), (0,)))
            for u in range(subs):
                c_out[group, owner + u, :, to] = value[u * chunk:(u + 1) * chunk].astype(BF16)
                part[group, owner + u, :, to] = value[piece + u * chunk:piece + (u + 1) * chunk]

        for u in range(subs):
            j = owner + u
            c_copies[group, s, u] = send(
                c_out.at[group, j], c_in.at[group, j], c_recv.at[group, j], core
            )

    l_tile = tile_of(chunk, 32)

    def each(body):
        @pl.loop(0, chunk // l_tile)
        def _(i):
            body(rows_at(i * l_tile, l_tile))

    x_copies, m_copies = {}, {}

    def summed(group, j, at):
        return part[group, j, at, :] + c_in[group, j, at, :].astype(F32)

    def to_x(group):
        for u in range(subs):
            for s in range(1, n_x):
                c_copies[group, s, u].wait_recv()
                j = owner_of(s) + u

                def fold(at):
                    x_out[group, s, u, at, :] = summed(group, j, at).astype(BF16)

                each(fold)
                x_copies[group, s, u] = send(
                    x_out.at[group, s, u], x_in.at[group, s, u], x_recv.at[group, s - 1, u], at_x(s)
                )

    def total_of(group, u, at):
        total = summed(group, owner_of(0) + u, at)
        for s in range(1, n_x):
            total = total + x_in[group, s, u, at, :].astype(F32)
        return total

    for s in range(1, n_x):
        partial(1, s)
    pl.when(at_middle)(functools.partial(cross, 1))
    to_x(1)
    pl.when(at_end)(functools.partial(cross, 1))
    partial(1, 0)
    for s in range(1, n_x):
        partial(0, s)
    to_x(0)
    pl.when(at_middle)(functools.partial(cross, 0))
    partial(0, 0)
    for rel in (1, 0):
        own_block(0, rel)
    for u in range(subs):
        c_copies[1, 0, u].wait_recv()
        for s in range(1, n_x):
            x_copies[1, s, u].wait_recv()

        def fold(at):
            m_out[u, at, :] = total_of(1, u, at).astype(BF16)

        each(fold)
        m_copies[u] = send(m_out.at[u], m_in.at[u], m_recv.at[u], twin)
    pl.when(at_end)(functools.partial(cross, 0))
    for u in range(subs):
        c_copies[0, 0, u].wait_recv()
    gathered = {}

    def place_of(at_x_index, u):
        return o_grad.at[rows_at((c * n_x + at_x_index) * piece + u * chunk, chunk)]

    def finish(u):
        for s in range(1, n_x):
            x_copies[0, s, u].wait_recv()
        m_copies[u].wait_recv()
        first = (c * n_x + x) * piece + u * chunk

        @pl.loop(0, chunk // l_tile)
        def _(i):
            at = rows_at(i * l_tile, l_tile)
            to = rows_at(first + i * l_tile, l_tile)
            xf = tok[to, :].astype(F32)
            inv = lax.rsqrt(jnp.mean(xf * xf, axis=-1, keepdims=True) + EPS)
            scaled = xf * inv
            d_normed = total_of(0, u, at) + m_in[u, at, :].astype(F32)
            d_scaled = d_normed * gain[...]
            inner = jnp.mean(d_scaled * scaled, axis=-1, keepdims=True)
            o_grad[to, :] = (inv * (d_scaled - scaled * inner)).astype(BF16)

        out = place_of(x, u)
        for s in range(1, n_x):
            gathered[u, s] = send(out, out, a_recv.at[u, s - 1], at_x(s), 1)
        send(out, out, g_recv, core, 1)

    def relay(u):
        for s in range(1, n_x):
            gathered[u, s].wait_recv()
            out = place_of(lax.rem(x + n_x - s, n_x), u)
            send(out, out, g_recv, core, 1)

    def collect(rel, put):
        for part in range(parts):
            for r in range(1, n_y):
                y_copies[0, rel, r, part].wait_recv()
            for step in range(1, n_q):
                q_copies[step, rel, part].wait_recv()
        total = own_share[0, rel]
        for r in range(1, n_y):
            total = total + y_in[0, rel, r].astype(F32)
        for step in range(1, n_q):
            total = total + q_in[step, rel].astype(F32)
        put(0, pl.ds(0, half), total)

    n_tile = tile_of(half, 128)

    def squares(value):
        folded = sum(value[:, k * 128:(k + 1) * 128] * value[:, k * 128:(k + 1) * 128] for k in range(depth // 128))
        return jnp.concatenate(
            [jnp.sum(folded[i:i + n_tile].T, axis=0, keepdims=True) for i in range(0, half, n_tile)], axis=1
        )

    def put_twin(start, at, value):
        t_out[at, :] = value.astype(BF16)
        n_all[f] = squares(value)

    def put_kept(start, at, value):
        o_down[rows_at(h * half + start, half), :] = value
        n_all[f] = n_all[f] + squares(value)

    collect(1, put_twin)
    traded = copy_to(t_out, t_in, t_recv, twin, 1)
    pl.when(at_middle)(traded.start)
    for u in range(subs):
        finish(u)
    collect(0, put_kept)
    for s in range(1, n_fs):
        send(n_all.at[f], n_all.at[f], n_recv, {"fs": lax.rem(f + s, n_fs)}, 1)
    pl.when(at_end)(traded.start)
    for copy in started[0]:
        copy.wait_send()
    for u in range(subs):
        relay(u)
    all_of(n_all.at[pl.ds(0, n_fs - 1)], n_recv)
    for side_of in range(2):
        total = sum(n_all[k] for k in range(n_fs) if k // n_y % 2 == side_of)
        o_norms[:, side_of * half:(side_of + 1) * half] = total
    for copy in started[1]:
        copy.wait_send()
    traded.wait_recv()
    o_down[rows_at((1 - h) * half, half), :] = t_in[...].astype(F32)
    all_of(o_grad.at[rows_at((1 - c) * side, side)], g_recv)


def put_out(grad, down, norms, o_grad, o_down, o_norms, done):
    copies = [
        pltpu.make_async_copy(src, dst, done.at[i])
        for i, (src, dst) in enumerate(((grad, o_grad), (down, o_down), (norms, o_norms)))
    ]
    for copy in copies:
        copy.start()
    for copy in copies:
        copy.wait()


def fused(n_z, n_y, n_x, tokens, norm_gain, w_gate, w_up, w_down, cotangent):
    n_fs, n_tp, n_q = n_z * n_y, 2 * n_x, n_z // 2
    rows, d_model = tokens.shape
    depth, half = w_gate.shape[0], w_gate.shape[1] // 2
    piece = rows // n_tp
    cuts = 2 if piece % 32 == 0 else 1
    kinds, parts = 2 + 4, 2
    subs = max(n for n in (1, 2, 3) if piece % (16 * n) == 0)
    chunks = n_x * subs
    chunk = rows // 2 // chunks
    dma, vmem = pltpu.SemaphoreType.DMA, pltpu.VMEM
    outside = pl.BlockSpec(memory_space=pltpu.HBM)
    inside = pl.BlockSpec(memory_space=pltpu.VMEM)
    block = (half, depth)
    scratch = [
        vmem((1, d_model), F32),
        vmem((2 * rows, d_model), BF16), vmem((2 * rows, d_model), BF16), vmem((2 * rows, d_model), BF16),
        vmem((n_fs, depth, half), BF16), vmem((n_fs, depth, half), BF16), vmem((n_fs, half, depth), BF16),
        vmem((n_fs, half, depth), BF16), vmem((n_fs, half, depth), BF16),
        vmem((2 * rows, half), F32), vmem((2 * rows, half), F32), vmem((2 * rows, half), F32),
        vmem((half, 2 * rows), BF16), vmem((2 * rows, half), BF16), vmem((2 * rows, half), BF16),
        vmem((n_q, 2) + block, F32), vmem((n_q, 2, n_y) + block, BF16), vmem((n_q, 2, n_y) + block, BF16),
        vmem((n_q, 2) + block, BF16), vmem((n_q, 2) + block, BF16), vmem(block, BF16), vmem(block, BF16),
        vmem((n_fs, 1, half), F32),
        vmem((2, chunks, chunk, d_model), F32),
        vmem((2, chunks, chunk, d_model), BF16), vmem((2, chunks, chunk, d_model), BF16),
        vmem((subs, chunk, d_model), BF16), vmem((subs, chunk, d_model), BF16),
        vmem((2, n_x, subs, chunk, d_model), BF16), vmem((2, n_x, subs, chunk, d_model), BF16),
        dma((2,)), dma((kinds, n_z)), dma((3, n_z, n_y - 1)),
        dma((2, cuts)), dma((2, cuts, n_x - 1)), dma((2, n_x)),
        dma((n_q, 2, n_y - 1, parts)), dma((n_q, 2, parts)), dma, dma,
        dma((2, chunks)), dma((subs,)), dma((2, n_x - 1, subs)), dma((subs, n_x - 1)),
        dma, dma((6,)),
    ]
    grad, down, norms = pl.pallas_call(
        functools.partial(fused_kernel, n_z, n_y, n_x),
        out_shape=[
            jax.ShapeDtypeStruct((rows, d_model), BF16),
            jax.ShapeDtypeStruct((2 * half, depth), F32),
            jax.ShapeDtypeStruct((1, 2 * half), F32),
        ],
        in_specs=[outside] * 6,
        out_specs=[inside, inside, inside],
        scratch_shapes=scratch,
        compiler_params=pltpu.CompilerParams(
            collective_id=1, has_side_effects=True, vmem_limit_bytes=48 * 2**20
        ),
    )(*[
        pltpu.with_memory_space_constraint(a, pltpu.HBM)
        for a in (tokens, cotangent, norm_gain.reshape(1, d_model), w_gate, w_up, w_down)
    ])
    grad, down, norms = pl.pallas_call(
        put_out,
        out_shape=[jax.ShapeDtypeStruct(a.shape, a.dtype) for a in (grad, down, norms)],
        in_specs=[pl.BlockSpec(memory_space=pl.ANY)] * 3,
        out_specs=[outside] * 3,
        scratch_shapes=[dma((3,))],
        compiler_params=pltpu.CompilerParams(vmem_limit_bytes=2**20),
    )(grad, down, norms)
    return grad, down, norms.reshape(2 * half)


def shards(n_fs, n_tp, tokens, norm_gain, w_gate, w_up, w_down, cotangent):
    n_y = 2 ** ((n_fs.bit_length() - 1) // 2)
    n_z, n_x = n_fs // n_y, n_tp // 2
    n_q = n_z // 2
    f, t = lax.axis_index("fs"), lax.axis_index("tp")
    z, y, x, c = f // n_y, f % n_y, t // 2, t % 2
    q, h = z // 2, z % 2
    rows, d_model = tokens.shape
    depth, half = w_gate.shape[0], w_gate.shape[1] // 2
    piece = rows // n_tp

    if piece % 16 == 0 and depth % 128 == 0 and half % 128 == 0:
        return fused(n_z, n_y, n_x, tokens, norm_gain, w_gate, w_up, w_down, cotangent)

    def to_z(a, step):
        return lax.ppermute(a, "fs", [(i, (i + step * n_y) % n_fs) for i in range(n_fs)])

    def to_y(a, step):
        return lax.ppermute(
            a, "fs", [(i, i // n_y * n_y + (i + step) % n_y) for i in range(n_fs)]
        )

    def to_twin(a):
        return lax.ppermute(
            a, "fs", [(i, (i // n_y ^ 1) * n_y + i % n_y) for i in range(n_fs)]
        )

    def to_x(a, step):
        return lax.ppermute(a, "tp", [(i, (i + 2 * step) % n_tp) for i in range(n_tp)])

    def to_core(a):
        return lax.ppermute(a, "tp", [(i, i ^ 1) for i in range(n_tp)])

    mine = jnp.stack(
        [lax.dynamic_slice_in_dim(a, t * piece, piece, 0) for a in (tokens, cotangent)]
    )
    down_t = w_down.T

    def half_of(which):
        gate_up = jnp.concatenate(
            [lax.dynamic_slice_in_dim(w, which * half, half, 1) for w in (w_gate, w_up)], axis=1
        )
        return gate_up, lax.dynamic_slice_in_dim(down_t, which * half, half, 1)

    own, other = half_of(h), half_of(1 - h)

    w_gu, w_dn, got = gather_all(n_z, n_y, n_x, own, other, mine)
    w_gu, w_dn = w_gu.reshape(d_model, 2 * half), w_dn.reshape(d_model, half)
    got = got.reshape(2, rows, d_model)
    tokens2 = jnp.concatenate([tokens, got[0]], axis=0)
    cot2 = jnp.concatenate([cotangent, got[1]], axis=0)

    xf = tokens2.astype(F32)
    inv = lax.rsqrt(jnp.mean(xf * xf, axis=-1, keepdims=True) + EPS)
    normed = (xf * inv * norm_gain).astype(BF16)
    gate_up = jnp.dot(normed, w_gu, preferred_element_type=F32)
    gate, up = gate_up[:, :half], gate_up[:, half:]
    sig = jax.nn.sigmoid(gate)
    act = gate * sig
    hidden = (act * up).astype(BF16)

    share = 0.5 * lax.dot_general(
        cot2, hidden, (((0,), (0,)), ((), ())), preferred_element_type=F32
    )
    share = share.reshape(n_q, 2, n_y, depth, half)
    share, w_dn = lax.optimization_barrier((share, w_dn))

    def sent_over_y(pair):
        block = take(share, pair)
        return [to_y(take(block, (y + s) % n_y, 1).astype(BF16), s) for s in range(1, n_y)]

    def over_y(pair, came):
        return sum([a.astype(F32) for a in came], take(take(share, pair), y, 1))

    first = [sent_over_y((q + s) % n_q) for s in range(1, n_q)]

    d_hidden = 0.5 * jnp.dot(cot2, w_dn, preferred_element_type=F32)
    d_gate = (d_hidden * up * sig * (1.0 + gate * (1.0 - sig))).astype(BF16)
    d_up = (d_hidden * act).astype(BF16)
    d_both = jnp.concatenate([d_gate, d_up], axis=1)
    part = lax.dot_general(
        d_both, w_gu, (((1,), (1,)), ((), ())), preferred_element_type=F32
    )
    part, first = lax.optimization_barrier((part.astype(BF16), first))

    away = [
        to_z(over_y((q + s) % n_q, first[s - 1]).astype(BF16), 2 * s) for s in range(1, n_q)
    ]
    total = over_y(q, sent_over_y(q))
    total = sum([a.astype(F32) for a in away], total)
    kept = take(total, h)
    came = to_twin(take(total, 1 - h).astype(BF16)).astype(F32)
    grad_down = place([(h, kept.T), (1 - h, came.T)], 2).reshape(2 * half, depth)
    norms = jnp.sum(grad_down * grad_down, axis=1)
    norms = sum([to_y(norms, s) for s in range(1, n_y)], norms)
    down_norms = sum([to_z(norms, s) for s in range(1, n_z)], norms)

    part = part.reshape(2, n_x, 2, piece, d_model)
    part = take(part, c, 2).astype(F32) + to_core(take(part, 1 - c, 2)).astype(F32)
    total = take(part, x, 1)
    for s in range(1, n_x):
        total = total + to_x(take(part, (x + s) % n_x, 1).astype(BF16), s).astype(F32)
    d_normed = total[0] + to_twin(total[1].astype(BF16)).astype(F32)

    xp = lax.dynamic_slice_in_dim(tokens, t * piece, piece, 0).astype(F32)
    inv_p = lax.rsqrt(jnp.mean(xp * xp, axis=-1, keepdims=True) + EPS)
    scaled = xp * inv_p
    d_scaled = d_normed * norm_gain
    inner = jnp.mean(d_scaled * scaled, axis=-1, keepdims=True)
    grad = (inv_p * (d_scaled - scaled * inner)).astype(BF16)
    grad = place([(x, grad)] + [((x - s) % n_x, to_x(grad, s)) for s in range(1, n_x)], n_x)
    grad = place([(c, grad), (1 - c, to_core(grad))], 2)
    grad_tokens = grad.transpose(1, 0, 2, 3).reshape(rows, d_model)
    return (grad_tokens, grad_down, down_norms)


def solution(mesh):
    in_specs = (P("fs", None), P(), P("fs", "tp"), P("fs", "tp"), P("tp", "fs"), P("fs", None))
    out_specs = (P("fs", None), P("tp", "fs"), P("tp"))
    return jax.shard_map(
        functools.partial(shards, mesh.shape["fs"], mesh.shape["tp"]),
        mesh=mesh, in_specs=in_specs, out_specs=out_specs, check_vma=False,
    )
```

```python
import functools

import jax
import jax.numpy as jnp
from jax import lax
from jax.experimental import pallas as pl
from jax.experimental.pallas import tpu as pltpu
from jax.sharding import PartitionSpec as P

EPS = 1e-06
BF16 = jnp.bfloat16
F32 = jnp.float32


def place(pieces, count):
    first = pieces[0][1]
    held = jnp.zeros((count,) + first.shape, first.dtype)
    for position, piece in pieces:
        held = lax.dynamic_update_slice_in_dim(held, piece[None], position, 0)
    return held


def take(array, position, axis=0):
    return lax.dynamic_index_in_dim(array, position, axis, keepdims=False)


def gather_kernel(n_z, n_y, n_x, own_gu, own_dn, other_gu, other_dn, mine, w_gu, w_dn, got,
                  z_send, z_recv, y_send, y_recv, x_send, x_recv, c_send, c_recv, local):
    f, t = lax.axis_index("fs"), lax.axis_index("tp")
    z, y, x, c = lax.div(f, n_y), lax.rem(f, n_y), lax.div(t, 2), lax.rem(t, 2)
    n_tp = 2 * n_x
    sources = ((own_gu, other_gu), (own_dn, other_dn))
    held = (w_gu, w_dn)

    def at_z(s):
        return {"fs": lax.rem(z + s, n_z) * n_y + y}

    def at_y(r):
        return {"fs": z * n_y + lax.rem(y + r, n_y)}

    def at_x(s):
        return {"tp": lax.rem(t + 2 * s, n_tp)}

    twin = {"fs": (z + 1 - 2 * lax.rem(z, 2)) * n_y + y}
    core = {"tp": t + 1 - 2 * c}

    barrier = pltpu.get_barrier_semaphore()
    friends = [at_z(s) for s in range(1, n_z)] + [at_y(r) for r in range(1, n_y)]
    friends += [at_x(s) for s in range(1, n_x)] + [core]
    for friend in friends:
        pl.semaphore_signal(barrier, inc=1, device_id=friend, device_id_type=pl.DeviceIdType.MESH)
    pl.semaphore_wait(barrier, len(friends))

    started = []

    def send(src, dst, out_sem, in_sem, to):
        copy = pltpu.make_async_remote_copy(
            src_ref=src, dst_ref=dst, send_sem=out_sem, recv_sem=in_sem,
            device_id=to, device_id_type=pl.DeviceIdType.MESH,
        )
        copy.start()
        started.append(copy)
        return copy

    order = sorted(range(1, n_z), key=lambda s: min(s, n_z - s))
    from_z = {}

    def start_z(k):
        for s in order:
            from_z[k, s] = send(
                sources[k][s % 2], held[k].at[f], z_send.at[k, s], z_recv.at[k, s], at_z(s)
            )

    late = []

    def forward(k, s):
        if s == 0:
            src = sources[k][0]
            slot = f
        else:
            from_z[k, s].wait_recv()
            slot = lax.rem(z + n_z - s, n_z) * n_y + y
            src = held[k].at[slot]
        for r in range(1, n_y):
            late.append(send(
                src, held[k].at[slot], y_send.at[k, s, r], y_recv.at[k, s, r], at_y(r)
            ))

    start_z(0)
    forward(0, 0)
    tokens = send(mine, got.at[:, x, c], x_send.at[0], x_recv.at[0], twin)
    start_z(1)
    forward(1, 0)
    stays = [pltpu.make_async_copy(sources[k][0], held[k].at[f], local.at[k]) for k in range(2)]
    for copy in stays:
        copy.start()
    for s in order:
        forward(0, s)
    tokens.wait_recv()
    across = [
        send(got.at[:, x, c], got.at[:, x, c], x_send.at[s], x_recv.at[s], at_x(s))
        for s in range(1, n_x)
    ]
    for s in order[:-1]:
        forward(1, s)
    for copy in across:
        copy.wait_recv()
    late.append(send(got.at[:, :, c], got.at[:, :, c], c_send, c_recv, core))
    forward(1, order[-1])
    for copy in late:
        copy.wait_recv()
    for copy in started:
        copy.wait_send()
    for copy in stays:
        copy.wait()


def gather_all(n_z, n_y, n_x, own, other, mine):
    n_fs = n_z * n_y
    dma = pltpu.SemaphoreType.DMA
    anywhere = pl.BlockSpec(memory_space=pl.ANY)
    return pl.pallas_call(
        functools.partial(gather_kernel, n_z, n_y, n_x),
        out_shape=[jax.ShapeDtypeStruct((n_fs,) + a.shape, a.dtype) for a in own]
        + [jax.ShapeDtypeStruct((2, n_x, 2) + mine.shape[1:], mine.dtype)],
        in_specs=[anywhere] * 5,
        out_specs=[anywhere] * 3,
        scratch_shapes=[
            dma((2, n_z)), dma((2, n_z)), dma((2, n_z, n_y)), dma((2, n_z, n_y)),
            dma((n_x,)), dma((n_x,)), dma, dma, dma((2,)),
        ],
        compiler_params=pltpu.CompilerParams(collective_id=0, has_side_effects=True),
    )(*own, *other, mine)


def tile_of(extent, most):
    return max(n for n in range(16, most + 1, 16) if extent % n == 0)


def dot(a, b, contract):
    return lax.dot_general(a, b, (contract, ((), ())), preferred_element_type=F32)


def rows_at(start, count):
    return pl.ds(pl.multiple_of(start, 16), count)


def cols_at(start, count):
    return pl.ds(pl.multiple_of(start, 128), count)


def fused_kernel(n_z, n_y, n_x, tokens, cotangent, gain_in, w_gate, w_up, w_down,
                 o_grad, o_down, o_norms,
                 gain, tok, cot, normed, wg, wu, wd, wg_t, wu_t, gate, up, d_hid, hid_t, d_gate, d_up,
                 own_share, y_out, y_in, q_out, q_in, t_out, t_in, n_all,
                 part, c_out, c_in, m_out, m_in, x_out, x_in,
                 sent, z_recv, f_recv, tt_recv, tx_recv, tc_recv, y_recv, q_recv, t_recv, n_recv,
                 c_recv, m_recv, x_recv, a_recv, g_recv, local):
    f, t = lax.axis_index("fs"), lax.axis_index("tp")
    z, y, x, c = lax.div(f, n_y), lax.rem(f, n_y), lax.div(t, 2), lax.rem(t, 2)
    q, h = lax.div(z, 2), lax.rem(z, 2)
    n_tp, n_q = 2 * n_x, n_z // 2
    rows, d_model = tokens.shape
    depth, half = wg.shape[1], wg.shape[2]
    piece = rows // n_tp
    chunks, subs = c_out.shape[1], m_out.shape[0]
    side = rows // 2
    chunk = side // chunks

    def at_z(s):
        return {"fs": lax.rem(z + s, n_z) * n_y + y}

    def at_y(r):
        return {"fs": z * n_y + lax.rem(y + r, n_y)}

    def at_x(s):
        return {"tp": lax.rem(t + 2 * s, n_tp)}

    twin = {"fs": (z + 1 - 2 * h) * n_y + y}
    core = {"tp": t + 1 - 2 * c}

    started = [], []

    def copy_to(src, dst, in_sem, to, phase=0):
        copy = pltpu.make_async_remote_copy(
            src_ref=src, dst_ref=dst, send_sem=sent.at[phase], recv_sem=in_sem,
            device_id=to, device_id_type=pl.DeviceIdType.MESH,
        )
        started[phase].append(copy)
        return copy

    def all_of(ref, in_sem):
        pltpu.make_async_remote_copy(
            src_ref=ref, dst_ref=ref, send_sem=sent.at[0], recv_sem=in_sem,
            device_id=core, device_id_type=pl.DeviceIdType.MESH,
        ).wait_recv()

    def send(*args):
        copy = copy_to(*args)
        copy.start()
        return copy

    def bring(src, dst, sem):
        copy = pltpu.make_async_copy(src, dst, sem)
        copy.start()
        return copy

    kinds = z_recv.shape[0]
    downs_of = range(2, kinds)
    step_rows = half // len(downs_of)

    def source(k, which):
        if k >= 2:
            return w_down.at[rows_at(which * half + (k - 2) * step_rows, step_rows), :]
        return (w_gate, w_up)[k].at[:, cols_at(which * half, half)]

    def held(k, at_slot):
        if k >= 2:
            return wd.at[at_slot, pl.ds((k - 2) * step_rows, step_rows)]
        return (wg, wu)[k].at[at_slot]

    barrier = pltpu.get_barrier_semaphore()
    n_fs = n_z * n_y
    friends = [{"fs": lax.rem(f + s, n_fs)} for s in range(1, n_fs)]
    friends += [at_x(s) for s in range(1, n_x)] + [core]
    for friend in friends:
        pl.semaphore_signal(barrier, inc=1, device_id=friend, device_id_type=pl.DeviceIdType.MESH)
    bring_gain = bring(gain_in, gain, local.at[5])
    bring_tok = bring(tokens, tok.at[pl.ds(0, rows)], local.at[0])
    bring_cot = bring(cotangent, cot.at[pl.ds(0, rows)], local.at[1])
    stays = [bring(source(k, h), held(k, f), local.at[2 + k]) for k in range(2)]
    stays.append(bring(w_down.at[rows_at(h * half, half), :], wd.at[f], local.at[4]))

    pl.semaphore_wait(barrier, len(friends))

    over_y = {}
    others = [[b for b in range(n_z) if b != a] for a in range(n_z)]
    ends = (0, n_z - 1)
    nearest = [sorted(others[a], key=lambda b: abs(a - b)) for a in range(n_z)]
    arrival = [
        [a] + sorted(others[a], key=lambda b: 1 if b == a ^ 1 else 2 * (b not in ends)) for a in range(n_z)
    ]

    def pick(table, p):
        return sum(jnp.where(z == a, table[a][p], 0) for a in range(n_z))

    near = [z] + [pick(arrival, p) for p in range(1, n_z)]

    def start_z(k, p):
        to = pick(nearest, p)
        send(
            source(k, lax.rem(to, 2)), held(k, f), z_recv.at[k, z],
            {"fs": to * n_y + y},
        )

    def slot(p, r):
        return near[p] * n_y + lax.rem(y + n_y - r, n_y)

    def forwarding(k, p):
        if p == 0:
            src, came = source(k, h), None
        else:
            src = held(k, slot(p, 0))
            came = pltpu.make_async_remote_copy(
                src_ref=src, dst_ref=src, send_sem=sent.at[0], recv_sem=z_recv.at[k, near[p]],
                device_id={"fs": near[p] * n_y + y}, device_id_type=pl.DeviceIdType.MESH,
            )
        for r in range(1, n_y):
            over_y[k, p, r] = copy_to(src, held(k, slot(p, 0)), f_recv.at[min(k, 2), near[p], r - 1], at_y(r))

        def go():
            if came is not None:
                came.wait_recv()
            for r in range(1, n_y):
                over_y[k, p, r].start()

        return go

    def forward(k, p):
        forwarding(k, p)()

    raw, both = (tokens, cotangent), (tok, cot)

    cuts = tt_recv.shape[1]
    cut = piece // cuts

    def cut_of(start, i):
        return rows_at(start + i * cut, cut)

    def swap(a):
        return [
            send(raw[a].at[cut_of(t * piece, i)], both[a].at[cut_of(rows + t * piece, i)],
                 tt_recv.at[a, i], twin)
            for i in range(cuts)
        ]

    def across(a, parts):
        copies = []
        for i in parts:
            swapped[a][i].wait_recv()
            at = both[a].at[cut_of(rows + t * piece, i)]
            copies += [send(at, at, tx_recv.at[a, i, s - 1], at_x(s)) for s in range(1, n_x)]
        return copies

    def meet(a):
        copies = []
        for k in range(n_x):
            at = rows_at(rows + (2 * k + c) * piece, piece)
            copies.append(send(both[a].at[at], both[a].at[at], tc_recv.at[a, k], core))
        return copies

    def arrive(copies):
        for copy in copies:
            copy.wait_recv()

    swapped = []
    for p in reversed(range(n_z - 1)):
        start_z(0, p)
        start_z(1, p)
        if p == n_z - 2:
            forward(0, 0)
            forward(1, 0)
            for k in downs_of:
                forward(k, 0)
    for a in range(2):
        swapped.append(swap(a))
    for p in range(n_z - 1):
        for k in downs_of:
            start_z(k, p)

    norm_tile = tile_of(rows, 32)

    def normalize(first):
        @pl.loop(0, rows // norm_tile)
        def _(i):
            at = rows_at(first + i * norm_tile, norm_tile)
            xf = tok[at, :].astype(F32)
            inv = lax.rsqrt(jnp.mean(xf * xf, axis=-1, keepdims=True) + EPS)
            normed[at, :] = (xf * inv * gain[...]).astype(BF16)

    bring_gain.wait()
    bring_tok.wait()
    normalize(0)

    m_tile = tile_of(2 * rows, 768)

    def add_gate_up(p, r, group):
        at_slot = slot(p, r)
        if group == 0:
            if p == 0 and r == 0:
                stays[0].wait()
                stays[1].wait()
            elif r > 0:
                over_y[0, p, r].wait_recv()
                over_y[1, p, r].wait_recv()
            wg_t[at_slot] = wg[at_slot].T
            wu_t[at_slot] = wu[at_slot].T
        at = pl.ds(group * rows, rows)
        a = normed[at, cols_at(at_slot * depth, depth)]
        for total, w in ((gate, wg), (up, wu)):
            term = dot(a, w[at_slot], ((1,), (0,)))
            total[at, :] = term if p == 0 and r == 0 else total[at, :] + term

    def add_d_hidden(s, r):
        at_slot = slot(s, r)
        if s == 0 and r == 0:
            stays[2].wait()
        elif r > 0:
            all_of(wd.at[at_slot], f_recv.at[2, near[s], r - 1])

        @pl.loop(0, 2 * rows // m_tile)
        def _(i):
            at = rows_at(i * m_tile, m_tile)
            term = dot(cot[at, cols_at(at_slot * depth, depth)], wd[at_slot], ((1,), (1,)))
            d_hid[at, :] = term if s == 0 and r == 0 else d_hid[at, :] + term

    add_gate_up(0, 0, 0)
    token_copies = []
    for p in range(1, n_z):
        forward(0, p)
        if p == n_z - 1:
            token_copies += across(0, range(cuts - 1))
        forward(1, p)
        if p == n_z - 1:
            token_copies += across(0, range(cuts - 1, cuts))
        for r in range(1, n_y):
            add_gate_up(p - 1, r, 0)
        add_gate_up(p, 0, 0)
    backward = range(n_z - 1, 0, -1)
    downs = [[forwarding(k, p) for k in downs_of] for p in backward]
    at_end = (z == 0) | (z == n_z - 1)

    at_middle = jnp.logical_not(at_end)

    def down(middle, end, first=0, count=len(downs_of)):
        for which, index in ((at_middle, middle), (at_end, end)):
            if index is not None and index < len(downs):
                @pl.when(which)
                def _():
                    for go in downs[index][first:first + count]:
                        go()

    down(0, None)
    cot_copies = across(1, range(cuts))
    arrive(token_copies)
    met = meet(0)
    down(1, None)
    arrive(met)
    normalize(rows)
    down(None, 0)
    for p in range(n_z):
        for r in range(n_y):
            if p == n_z - 1 and r > 0:
                add_gate_up(p, r, 0)
            add_gate_up(p, r, 1)
        if p == n_z // 2:
            down(None, 1, 0, 1)
    down(2, None)
    down(None, 1, 1)

    e_tile = tile_of(2 * rows, 128)

    @pl.loop(0, 2 * rows // e_tile)
    def _(i):
        at = rows_at(i * e_tile, e_tile)
        g, u = gate[at, :], up[at, :]
        sig = jax.nn.sigmoid(g)
        act = g * sig
        hid_t[:, cols_at(i * e_tile, e_tile)] = (act * u).T.astype(BF16)
        gate[at, :] = 0.5 * (u * sig * (1.0 + g * (1.0 - sig)))
        up[at, :] = 0.5 * act

    arrive(cot_copies)
    bring_cot.wait()
    arrive(meet(1))
    parts = y_recv.shape[3]
    some = half // parts

    def rows_of(part):
        return pl.ds(part * some, some)

    def share(block, at):
        return 0.5 * dot(hid_t[at, :], cot[:, cols_at(block * depth, depth)], ((1,), (0,)))

    def block_of(step, rel, r):
        column = 2 * lax.rem(q + step, n_q) + (h if rel == 0 else 1 - h)
        return column * n_y + lax.rem(y + r, n_y)

    y_copies = {}

    def send_share(step, rel):
        for part in range(parts):
            at = rows_of(part)
            for r in range(1, n_y):
                out = y_out.at[step, rel, r, at]
                out[...] = share(block_of(step, rel, r), at).astype(BF16)
                y_copies[step, rel, r, part] = send(
                    out, y_in.at[step, rel, r, at], y_recv.at[step, rel, r - 1, part], at_y(r)
                )

    def own_block(step, rel):
        own_share[step, rel] = share(block_of(step, rel, 0), pl.ds(0, half))

    q_copies = {
        (step, rel, part): copy_to(
            q_out.at[step, rel, rows_of(part)], q_in.at[step, rel, rows_of(part)],
            q_recv.at[step, rel, part], at_z(2 * step),
        )
        for step in range(1, n_q) for rel in range(2) for part in range(parts)
    }

    def cross(rel):
        for part in range(parts):
            at = rows_of(part)
            for step in range(1, n_q):
                for r in range(1, n_y):
                    y_copies[step, rel, r, part].wait_recv()
                total = own_share[step, rel, at]
                for r in range(1, n_y):
                    total = total + y_in[step, rel, r, at].astype(F32)
                q_out[step, rel, at] = total.astype(BF16)
                q_copies[step, rel, part].start()

    down(None, 2)
    for step in range(1, n_q):
        send_share(step, 1)
    for index in range(3, len(downs)):
        down(index, index)
    for step in range(1, n_q):
        send_share(step, 0)
    for rel in (1, 0):
        send_share(0, rel)
    for step in range(1, n_q):
        for rel in (1, 0):
            own_block(step, rel)
    add_d_hidden(0, 0)
    for r in range(1, n_y):
        add_d_hidden(0, r)
    for p in backward:
        add_d_hidden(p, 0)
        for r in range(1, n_y):
            add_d_hidden(p, r)

    d_tile = tile_of(piece, 128)

    @pl.loop(0, 2 * rows // d_tile)
    def _(i):
        at = rows_at(i * d_tile, d_tile)
        index = lax.div(i * d_tile, piece)
        group, index = lax.div(index, n_tp), lax.rem(index, n_tp)
        turn = lax.rem(lax.rem(index, n_x) + 2 * n_x - 1 - x, n_x)
        mine = lax.rem(lax.div(index, n_x) + c + 1, 2)
        to = group * rows + (2 * turn + mine) * piece + lax.rem(i * d_tile, piece)
        d = d_hid[at, :]
        d_gate[rows_at(to, d_tile), :] = (d * gate[at, :]).astype(BF16)
        d_up[rows_at(to, d_tile), :] = (d * up[at, :]).astype(BF16)

    c_copies = {}

    def owner_of(s):
        return lax.rem(x + s, n_x) * subs

    def partial(group, s):
        first = group * rows + (s - 1 if s else n_x - 1) * 2 * piece
        owner = owner_of(s)

        @pl.loop(0, n_z * n_y, unroll=8)
        def _(k):
            at, to = pl.ds(first, 2 * piece), cols_at(k * depth, depth)
            value = dot(d_gate[at, :], wg_t[k], ((1,), (0,))) + dot(d_up[at, :], wu_t[k], ((1,), (0,)))
            for u in range(subs):
                c_out[group, owner + u, :, to] = value[u * chunk:(u + 1) * chunk].astype(BF16)
                part[group, owner + u, :, to] = value[piece + u * chunk:piece + (u + 1) * chunk]

        for u in range(subs):
            j = owner + u
            c_copies[group, s, u] = send(
                c_out.at[group, j], c_in.at[group, j], c_recv.at[group, j], core
            )

    l_tile = tile_of(chunk, 32)

    def each(body):
        @pl.loop(0, chunk // l_tile)
        def _(i):
            body(rows_at(i * l_tile, l_tile))

    x_copies, m_copies = {}, {}

    def summed(group, j, at):
        return part[group, j, at, :] + c_in[group, j, at, :].astype(F32)

    def to_x(group):
        for u in range(subs):
            for s in range(1, n_x):
                c_copies[group, s, u].wait_recv()
                j = owner_of(s) + u

                def fold(at):
                    x_out[group, s, u, at, :] = summed(group, j, at).astype(BF16)

                each(fold)
                x_copies[group, s, u] = send(
                    x_out.at[group, s, u], x_in.at[group, s, u], x_recv.at[group, s - 1, u], at_x(s)
                )

    def total_of(group, u, at):
        total = summed(group, owner_of(0) + u, at)
        for s in range(1, n_x):
            total = total + x_in[group, s, u, at, :].astype(F32)
        return total

    for s in range(1, n_x):
        partial(1, s)
    pl.when(at_middle)(functools.partial(cross, 1))
    to_x(1)
    pl.when(at_end)(functools.partial(cross, 1))
    partial(1, 0)
    for s in range(1, n_x):
        partial(0, s)
    to_x(0)
    pl.when(at_middle)(functools.partial(cross, 0))
    partial(0, 0)
    for rel in (1, 0):
        own_block(0, rel)
    for u in range(subs):
        c_copies[1, 0, u].wait_recv()
        for s in range(1, n_x):
            x_copies[1, s, u].wait_recv()

        def fold(at):
            m_out[u, at, :] = total_of(1, u, at).astype(BF16)

        each(fold)
        m_copies[u] = send(m_out.at[u], m_in.at[u], m_recv.at[u], twin)
    pl.when(at_end)(functools.partial(cross, 0))
    for u in range(subs):
        c_copies[0, 0, u].wait_recv()
    gathered = {}

    def place_of(at_x_index, u):
        return o_grad.at[rows_at((c * n_x + at_x_index) * piece + u * chunk, chunk)]

    def finish(u):
        for s in range(1, n_x):
            x_copies[0, s, u].wait_recv()
        m_copies[u].wait_recv()
        first = (c * n_x + x) * piece + u * chunk

        @pl.loop(0, chunk // l_tile)
        def _(i):
            at = rows_at(i * l_tile, l_tile)
            to = rows_at(first + i * l_tile, l_tile)
            xf = tok[to, :].astype(F32)
            inv = lax.rsqrt(jnp.mean(xf * xf, axis=-1, keepdims=True) + EPS)
            scaled = xf * inv
            d_normed = total_of(0, u, at) + m_in[u, at, :].astype(F32)
            d_scaled = d_normed * gain[...]
            inner = jnp.mean(d_scaled * scaled, axis=-1, keepdims=True)
            o_grad[to, :] = (inv * (d_scaled - scaled * inner)).astype(BF16)

        out = place_of(x, u)
        for s in range(1, n_x):
            gathered[u, s] = send(out, out, a_recv.at[u, s - 1], at_x(s), 1)
        send(out, out, g_recv, core, 1)

    def relay(u):
        for s in range(1, n_x):
            gathered[u, s].wait_recv()
            out = place_of(lax.rem(x + n_x - s, n_x), u)
            send(out, out, g_recv, core, 1)

    def collect(rel, put):
        for part in range(parts):
            for r in range(1, n_y):
                y_copies[0, rel, r, part].wait_recv()
            for step in range(1, n_q):
                q_copies[step, rel, part].wait_recv()
        total = own_share[0, rel]
        for r in range(1, n_y):
            total = total + y_in[0, rel, r].astype(F32)
        for step in range(1, n_q):
            total = total + q_in[step, rel].astype(F32)
        put(0, pl.ds(0, half), total)

    n_tile = tile_of(half, 128)

    def squares(value):
        folded = sum(value[:, k * 128:(k + 1) * 128] * value[:, k * 128:(k + 1) * 128] for k in range(depth // 128))
        return jnp.concatenate(
            [jnp.sum(folded[i:i + n_tile].T, axis=0, keepdims=True) for i in range(0, half, n_tile)], axis=1
        )

    def put_twin(start, at, value):
        t_out[at, :] = value.astype(BF16)
        n_all[f] = squares(value)

    def put_kept(start, at, value):
        o_down[rows_at(h * half + start, half), :] = value
        n_all[f] = n_all[f] + squares(value)

    collect(1, put_twin)
    traded = copy_to(t_out, t_in, t_recv, twin, 1)
    pl.when(at_middle)(traded.start)
    for u in range(subs):
        finish(u)
    collect(0, put_kept)
    for s in range(1, n_fs):
        send(n_all.at[f], n_all.at[f], n_recv, {"fs": lax.rem(f + s, n_fs)}, 1)
    pl.when(at_end)(traded.start)
    for copy in started[0]:
        copy.wait_send()
    for u in range(subs):
        relay(u)
    all_of(n_all.at[pl.ds(0, n_fs - 1)], n_recv)
    for side_of in range(2):
        total = sum(n_all[k] for k in range(n_fs) if k // n_y % 2 == side_of)
        o_norms[:, side_of * half:(side_of + 1) * half] = total
    for copy in started[1]:
        copy.wait_send()
    traded.wait_recv()
    o_down[rows_at((1 - h) * half, half), :] = t_in[...].astype(F32)
    all_of(o_grad.at[rows_at((1 - c) * side, side)], g_recv)


def put_out(grad, down, norms, o_grad, o_down, o_norms, done):
    copies = [
        pltpu.make_async_copy(src, dst, done.at[i])
        for i, (src, dst) in enumerate(((grad, o_grad), (down, o_down), (norms, o_norms)))
    ]
    for copy in copies:
        copy.start()
    for copy in copies:
        copy.wait()


def fused(n_z, n_y, n_x, tokens, norm_gain, w_gate, w_up, w_down, cotangent):
    n_fs, n_tp, n_q = n_z * n_y, 2 * n_x, n_z // 2
    rows, d_model = tokens.shape
    depth, half = w_gate.shape[0], w_gate.shape[1] // 2
    piece = rows // n_tp
    cuts = 2 if piece % 32 == 0 else 1
    kinds, parts = 2 + 2, 2
    subs = max(n for n in (1, 2, 3) if piece % (16 * n) == 0)
    chunks = n_x * subs
    chunk = rows // 2 // chunks
    dma, vmem = pltpu.SemaphoreType.DMA, pltpu.VMEM
    outside = pl.BlockSpec(memory_space=pltpu.HBM)
    inside = pl.BlockSpec(memory_space=pltpu.VMEM)
    block = (half, depth)
    scratch = [
        vmem((1, d_model), F32),
        vmem((2 * rows, d_model), BF16), vmem((2 * rows, d_model), BF16), vmem((2 * rows, d_model), BF16),
        vmem((n_fs, depth, half), BF16), vmem((n_fs, depth, half), BF16), vmem((n_fs, half, depth), BF16),
        vmem((n_fs, half, depth), BF16), vmem((n_fs, half, depth), BF16),
        vmem((2 * rows, half), F32), vmem((2 * rows, half), F32), vmem((2 * rows, half), F32),
        vmem((half, 2 * rows), BF16), vmem((2 * rows, half), BF16), vmem((2 * rows, half), BF16),
        vmem((n_q, 2) + block, F32), vmem((n_q, 2, n_y) + block, BF16), vmem((n_q, 2, n_y) + block, BF16),
        vmem((n_q, 2) + block, BF16), vmem((n_q, 2) + block, BF16), vmem(block, BF16), vmem(block, BF16),
        vmem((n_fs, 1, half), F32),
        vmem((2, chunks, chunk, d_model), F32),
        vmem((2, chunks, chunk, d_model), BF16), vmem((2, chunks, chunk, d_model), BF16),
        vmem((subs, chunk, d_model), BF16), vmem((subs, chunk, d_model), BF16),
        vmem((2, n_x, subs, chunk, d_model), BF16), vmem((2, n_x, subs, chunk, d_model), BF16),
        dma((2,)), dma((kinds, n_z)), dma((3, n_z, n_y - 1)),
        dma((2, cuts)), dma((2, cuts, n_x - 1)), dma((2, n_x)),
        dma((n_q, 2, n_y - 1, parts)), dma((n_q, 2, parts)), dma, dma,
        dma((2, chunks)), dma((subs,)), dma((2, n_x - 1, subs)), dma((subs, n_x - 1)),
        dma, dma((6,)),
    ]
    grad, down, norms = pl.pallas_call(
        functools.partial(fused_kernel, n_z, n_y, n_x),
        out_shape=[
            jax.ShapeDtypeStruct((rows, d_model), BF16),
            jax.ShapeDtypeStruct((2 * half, depth), F32),
            jax.ShapeDtypeStruct((1, 2 * half), F32),
        ],
        in_specs=[outside] * 6,
        out_specs=[inside, inside, inside],
        scratch_shapes=scratch,
        compiler_params=pltpu.CompilerParams(
            collective_id=1, has_side_effects=True, vmem_limit_bytes=48 * 2**20
        ),
    )(*[
        pltpu.with_memory_space_constraint(a, pltpu.HBM)
        for a in (tokens, cotangent, norm_gain.reshape(1, d_model), w_gate, w_up, w_down)
    ])
    grad, down, norms = pl.pallas_call(
        put_out,
        out_shape=[jax.ShapeDtypeStruct(a.shape, a.dtype) for a in (grad, down, norms)],
        in_specs=[pl.BlockSpec(memory_space=pl.ANY)] * 3,
        out_specs=[outside] * 3,
        scratch_shapes=[dma((3,))],
        compiler_params=pltpu.CompilerParams(vmem_limit_bytes=2**20),
    )(grad, down, norms)
    return grad, down, norms.reshape(2 * half)


def shards(n_fs, n_tp, tokens, norm_gain, w_gate, w_up, w_down, cotangent):
    n_y = 2 ** ((n_fs.bit_length() - 1) // 2)
    n_z, n_x = n_fs // n_y, n_tp // 2
    n_q = n_z // 2
    f, t = lax.axis_index("fs"), lax.axis_index("tp")
    z, y, x, c = f // n_y, f % n_y, t // 2, t % 2
    q, h = z // 2, z % 2
    rows, d_model = tokens.shape
    depth, half = w_gate.shape[0], w_gate.shape[1] // 2
    piece = rows // n_tp

    if piece % 16 == 0 and depth % 128 == 0 and half % 128 == 0:
        return fused(n_z, n_y, n_x, tokens, norm_gain, w_gate, w_up, w_down, cotangent)

    def to_z(a, step):
        return lax.ppermute(a, "fs", [(i, (i + step * n_y) % n_fs) for i in range(n_fs)])

    def to_y(a, step):
        return lax.ppermute(
            a, "fs", [(i, i // n_y * n_y + (i + step) % n_y) for i in range(n_fs)]
        )

    def to_twin(a):
        return lax.ppermute(
            a, "fs", [(i, (i // n_y ^ 1) * n_y + i % n_y) for i in range(n_fs)]
        )

    def to_x(a, step):
        return lax.ppermute(a, "tp", [(i, (i + 2 * step) % n_tp) for i in range(n_tp)])

    def to_core(a):
        return lax.ppermute(a, "tp", [(i, i ^ 1) for i in range(n_tp)])

    mine = jnp.stack(
        [lax.dynamic_slice_in_dim(a, t * piece, piece, 0) for a in (tokens, cotangent)]
    )
    down_t = w_down.T

    def half_of(which):
        gate_up = jnp.concatenate(
            [lax.dynamic_slice_in_dim(w, which * half, half, 1) for w in (w_gate, w_up)], axis=1
        )
        return gate_up, lax.dynamic_slice_in_dim(down_t, which * half, half, 1)

    own, other = half_of(h), half_of(1 - h)

    w_gu, w_dn, got = gather_all(n_z, n_y, n_x, own, other, mine)
    w_gu, w_dn = w_gu.reshape(d_model, 2 * half), w_dn.reshape(d_model, half)
    got = got.reshape(2, rows, d_model)
    tokens2 = jnp.concatenate([tokens, got[0]], axis=0)
    cot2 = jnp.concatenate([cotangent, got[1]], axis=0)

    xf = tokens2.astype(F32)
    inv = lax.rsqrt(jnp.mean(xf * xf, axis=-1, keepdims=True) + EPS)
    normed = (xf * inv * norm_gain).astype(BF16)
    gate_up = jnp.dot(normed, w_gu, preferred_element_type=F32)
    gate, up = gate_up[:, :half], gate_up[:, half:]
    sig = jax.nn.sigmoid(gate)
    act = gate * sig
    hidden = (act * up).astype(BF16)

    share = 0.5 * lax.dot_general(
        cot2, hidden, (((0,), (0,)), ((), ())), preferred_element_type=F32
    )
    share = share.reshape(n_q, 2, n_y, depth, half)
    share, w_dn = lax.optimization_barrier((share, w_dn))

    def sent_over_y(pair):
        block = take(share, pair)
        return [to_y(take(block, (y + s) % n_y, 1).astype(BF16), s) for s in range(1, n_y)]

    def over_y(pair, came):
        return sum([a.astype(F32) for a in came], take(take(share, pair), y, 1))

    first = [sent_over_y((q + s) % n_q) for s in range(1, n_q)]

    d_hidden = 0.5 * jnp.dot(cot2, w_dn, preferred_element_type=F32)
    d_gate = (d_hidden * up * sig * (1.0 + gate * (1.0 - sig))).astype(BF16)
    d_up = (d_hidden * act).astype(BF16)
    d_both = jnp.concatenate([d_gate, d_up], axis=1)
    part = lax.dot_general(
        d_both, w_gu, (((1,), (1,)), ((), ())), preferred_element_type=F32
    )
    part, first = lax.optimization_barrier((part.astype(BF16), first))

    away = [
        to_z(over_y((q + s) % n_q, first[s - 1]).astype(BF16), 2 * s) for s in range(1, n_q)
    ]
    total = over_y(q, sent_over_y(q))
    total = sum([a.astype(F32) for a in away], total)
    kept = take(total, h)
    came = to_twin(take(total, 1 - h).astype(BF16)).astype(F32)
    grad_down = place([(h, kept.T), (1 - h, came.T)], 2).reshape(2 * half, depth)
    norms = jnp.sum(grad_down * grad_down, axis=1)
    norms = sum([to_y(norms, s) for s in range(1, n_y)], norms)
    down_norms = sum([to_z(norms, s) for s in range(1, n_z)], norms)

    part = part.reshape(2, n_x, 2, piece, d_model)
    part = take(part, c, 2).astype(F32) + to_core(take(part, 1 - c, 2)).astype(F32)
    total = take(part, x, 1)
    for s in range(1, n_x):
        total = total + to_x(take(part, (x + s) % n_x, 1).astype(BF16), s).astype(F32)
    d_normed = total[0] + to_twin(total[1].astype(BF16)).astype(F32)

    xp = lax.dynamic_slice_in_dim(tokens, t * piece, piece, 0).astype(F32)
    inv_p = lax.rsqrt(jnp.mean(xp * xp, axis=-1, keepdims=True) + EPS)
    scaled = xp * inv_p
    d_scaled = d_normed * norm_gain
    inner = jnp.mean(d_scaled * scaled, axis=-1, keepdims=True)
    grad = (inv_p * (d_scaled - scaled * inner)).astype(BF16)
    grad = place([(x, grad)] + [((x - s) % n_x, to_x(grad, s)) for s in range(1, n_x)], n_x)
    grad = place([(c, grad), (1 - c, to_core(grad))], 2)
    grad_tokens = grad.transpose(1, 0, 2, 3).reshape(rows, d_model)
    return (grad_tokens, grad_down, down_norms)


def solution(mesh):
    in_specs = (P("fs", None), P(), P("fs", "tp"), P("fs", "tp"), P("tp", "fs"), P("fs", None))
    out_specs = (P("fs", None), P("tp", "fs"), P("tp"))
    return jax.shard_map(
        functools.partial(shards, mesh.shape["fs"], mesh.shape["tp"]),
        mesh=mesh, in_specs=in_specs, out_specs=out_specs, check_vma=False,
    )
```
